32 devices in a mesh: sp: 8 (over z, y), tp: 4 (over x, core).
Axes of the slice: x: 2, y: 2, z: 4, core: 2. Of those that a mesh axis runs over, the one named last changes fastest.
Arguments:
- tokens: bfloat16 [1536, 2048], P(('sp', 'tp')), may hold values from -6 to 6
- norm_in: float32 [2048], replicated, may hold values from 0.1 to 1.9
- decay_log: float32 [128, 64], P('tp'), may hold values from -0.034 to -0.00016276042, as said below
- phase: float32 [128, 64], P('tp'), may hold values from -1 to 1
- b_real: float32 [128, 64, 16], P('tp'), may hold values from -1 to 1
- b_imag: float32 [128, 64, 16], P('tp'), may hold values from -1 to 1
- c_real: float32 [128, 16, 64], P('tp'), may hold values from -0.75 to 0.75
- c_imag: float32 [128, 16, 64], P('tp'), may hold values from -0.75 to 0.75
- skip_gain: float32 [2048], P('tp'), may hold values from -6 to 6
- w_value: bfloat16 [2048, 2048], P(None, 'tp'), as said below
- w_gate: bfloat16 [2048, 2048], P(None, 'tp'), may hold values from -0.125 to 0.125
- norm_out: float32 [2048], P('tp'), may hold values from 0.1 to 1.9
Outputs:
- mixed: bfloat16 [1536, 2048], P('sp', 'tp')
The draws below stay inside these ranges and needn't reach their ends.
Inputs may be any that keep to these rules, and one draw needn't show every extreme that they name: `decay_log`: negative real parts of the eigenvalues. `w_value`: weights of the value projection.
All inputs are finite; a program needn't handle non-finite values.
Results may differ from the reference program's by a relative error of at most 0.012.
The reference program's roundings to bfloat16 on the way count: a program that leaves them out, or rounds other values in their place, can miss the bound.
Values may be sent and summed in bfloat16 or wider, within the bound.
A program may use at most 64 MiB of HBM per device.

```python
import math
import jax
import jax.numpy as jnp
from jax import lax

D = 2048
GROUP = 16
STATE = 64
GROUPS = 128
TOK_DEV = 192
TOKENS = 1536
N_SP = 8


def draw_decay_log(key, part):
    first_key = jax.random.fold_in(key, 11)
    second_key = jax.random.fold_in(key, 12)
    third_key = jax.random.fold_in(key, 13)
    slow_share = 0.5
    slow_flag = jax.random.uniform(first_key, (GROUPS, 1), jnp.float32) < slow_share
    slow_rate = jnp.exp(jax.random.uniform(second_key, (GROUPS, STATE), jnp.float32, math.log(0.25), math.log(2.2))) / TOKENS
    fast_rate = jnp.exp(jax.random.uniform(third_key, (GROUPS, STATE), jnp.float32, math.log(0.0101), math.log(0.0333)))
    return -jnp.where(slow_flag, slow_rate, fast_rate)


def draw_w_value(key, part):
    top_scale = 10.0
    columns = jnp.arange(D, dtype=jnp.float32)
    column_scale = jnp.exp(math.log(top_scale) * columns / D)
    base = jax.random.normal(key, (D, D), jnp.float32) * D ** (-0.5)
    return (base * column_scale[None, :]).astype(jnp.bfloat16)


def block_levels(key, dims, shards, low, top_value):
    def one(dim, shards_of):
        steps = jax.random.uniform(jax.random.fold_in(jax.random.fold_in(key, 6), dim), (shards_of,), jnp.float32, low / len(shards), top_value / len(shards))
        return jnp.repeat(jnp.exp(steps), dims[dim] // shards_of).reshape((-1,) + (1,) * (len(dims) - dim - 1))

    level = one(*shards[0])
    for cut in shards[1:]:
        level = level * one(*cut)
    return level


def centred(rng, dims, spread, bound, cuts=(), kind=jnp.bfloat16):
    result = jax.random.normal(rng, dims, jnp.float32) * spread
    if len(cuts) > 0:
        result = block_levels(rng, dims, cuts, -0.22, 0.18) * result
    return jnp.clip(result, min=-bound, max=bound).astype(kind)


def setup_inputs(seed: int = 0) -> dict:
    splits = jax.random.split(jax.random.key(seed), 13)
    return {
        "tokens": centred(splits[0], (TOKENS, D), 1.0, 6.0, ((0, 32),)),
        "norm_in": jnp.clip(1.0 + 0.18 * jax.random.normal(splits[1], (D,), jnp.float32), 0.1, 1.9),
        "decay_log": draw_decay_log(jax.random.fold_in(splits[12], 71), 0),
        "phase": jnp.clip(jax.random.uniform(splits[3], (GROUPS, STATE), jnp.float32, -1.0, 1.0) * block_levels(splits[3], (GROUPS, STATE), ((0, 4),), -0.4, 0.0), -1.0, 1.0),
        "b_real": centred(splits[4], (GROUPS, STATE, GROUP), (2 * GROUP) ** -0.5, 1.0, ((0, 4),), jnp.float32),
        "b_imag": centred(splits[5], (GROUPS, STATE, GROUP), (2 * GROUP) ** -0.5, 1.0, ((0, 4),), jnp.float32),
        "c_real": centred(splits[6], (GROUPS, GROUP, STATE), STATE ** -0.5, 0.75, ((0, 4),), jnp.float32),
        "c_imag": centred(splits[7], (GROUPS, GROUP, STATE), STATE ** -0.5, 0.75, ((0, 4),), jnp.float32),
        "skip_gain": centred(splits[8], (D,), 1.0, 6.0, ((0, 4),), jnp.float32),
        "w_value": draw_w_value(jax.random.fold_in(splits[12], 71), 0),
        "w_gate": centred(splits[10], (D, D), D ** -0.5, 0.125, ((1, 4),)),
        "norm_out": jnp.clip(1.0 + 0.18 * jax.random.normal(splits[11], (D,), jnp.float32), 0.1, 1.9),
    }


NORM_EPS = 1e-06
HIGHEST_PREC = lax.Precision.HIGHEST

def coefficients(decay_log, phase, b_real, b_imag):
    magnitude = jnp.exp(decay_log)
    bar_re = magnitude * jnp.cos(phase)
    bar_im = magnitude * jnp.sin(phase)
    modulus = decay_log * decay_log + phase * phase
    coef_re = ((bar_re - 1.0) * decay_log + bar_im * phase) / modulus
    coef_im = (bar_im * decay_log - (bar_re - 1.0) * phase) / modulus
    in_re = coef_re[:, :, None] * b_real - coef_im[:, :, None] * b_imag
    in_im = coef_re[:, :, None] * b_imag + coef_im[:, :, None] * b_real
    return (bar_re, bar_im, in_re, in_im)

def prefix_states(drive_re, drive_im, rate_re, rate_im):
    length = drive_re.shape[0]
    stride = 1
    for level in range(max(length - 1, 1).bit_length()):
        padding = jnp.zeros((stride,) + drive_re.shape[1:], jnp.float32)
        moved_re = jnp.concatenate([padding, drive_re[:length - stride]], axis=0)
        moved_im = jnp.concatenate([padding, drive_im[:length - stride]], axis=0)
        drive_re, drive_im = (drive_re + rate_re * moved_re - rate_im * moved_im, drive_im + rate_re * moved_im + rate_im * moved_re)
        rate_re, rate_im = (rate_re * rate_re - rate_im * rate_im, 2.0 * rate_re * rate_im)
        stride = stride * 2
    return (drive_re, drive_im)

def readout(state_re, state_im, c_real, c_imag):
    first = jnp.einsum('tgp,ghp->tgh', state_re, c_real, precision=HIGHEST_PREC)
    second = jnp.einsum('tgp,ghp->tgh', state_im, c_imag, precision=HIGHEST_PREC)
    return first - second

def reference(tokens, norm_in, decay_log, phase, b_real, b_imag, c_real, c_imag, skip_gain, w_value, w_gate, norm_out):
    xf = tokens.astype(jnp.float32)
    normed = (xf * lax.rsqrt(lax.optimization_barrier(jnp.mean(xf * xf, axis=1, keepdims=True)) + NORM_EPS) * norm_in).astype(jnp.bfloat16)
    bar_re, bar_im, bb_re, bb_im = coefficients(decay_log, phase, b_real, b_imag)
    blocks = normed.reshape(N_SP, TOK_DEV, GROUPS, GROUP)
    skip_grid = skip_gain.reshape(GROUPS, GROUP)

    def block_step(carried, block):
        state_re, state_im = carried
        drive = block.astype(jnp.float32)
        in_re = jnp.einsum('tgh,gph->tgp', drive, bb_re, precision=HIGHEST_PREC)
        in_im = jnp.einsum('tgh,gph->tgp', drive, bb_im, precision=HIGHEST_PREC)
        in_re = in_re.at[0].add(bar_re * state_re - bar_im * state_im)
        in_im = in_im.at[0].add(bar_re * state_im + bar_im * state_re)
        all_re, all_im = prefix_states(in_re, in_im, bar_re, bar_im)
        mixed_pre = readout(all_re, all_im, c_real, c_imag) + skip_grid * drive
        z_block = jax.nn.gelu(mixed_pre).reshape(TOK_DEV, D).astype(jnp.bfloat16)
        return ((all_re[-1], all_im[-1]), z_block)
    start_state = (jnp.zeros((GROUPS, STATE), jnp.float32), jnp.zeros((GROUPS, STATE), jnp.float32))
    ignored, z_blocks = lax.scan(block_step, start_state, blocks)
    z_all = z_blocks.reshape(N_SP * TOK_DEV, D)
    projected_value = jnp.dot(z_all, w_value, preferred_element_type=jnp.float32)
    projected_gate = jnp.dot(z_all, w_gate, preferred_element_type=jnp.float32)
    gated = projected_value * jax.nn.sigmoid(projected_gate)
    scale = lax.rsqrt(lax.optimization_barrier(jnp.mean(gated * gated, axis=1, keepdims=True)) + NORM_EPS)
    return (gated * scale * norm_out).astype(jnp.bfloat16)
```

```python
import functools

import jax
import jax.numpy as jnp
from jax import lax
from jax.experimental import pallas as pl
from jax.experimental.pallas import tpu as pltpu
from jax.sharding import PartitionSpec as P

NORM_EPS = 1e-06
LANES = 128
F32 = jnp.float32
BF16 = jnp.bfloat16


def cmul(ar, ai, br, bi):
    return ar * br - ai * bi, ar * bi + ai * br


def cpow(r, i, n):
    outr, outi = None, None
    while n:
        if n % 2:
            outr, outi = (r, i) if outr is None else cmul(outr, outi, r, i)
        n //= 2
        if n:
            r, i = cmul(r, i, r, i)
    return outr, outi


def remote(src, dst, send, recv, target):
    return pltpu.make_async_remote_copy(
        src_ref=src,
        dst_ref=dst,
        send_sem=send,
        recv_sem=recv,
        device_id=target,
        device_id_type=pl.DeviceIdType.MESH,
    )


def layer(
    n_sp, n_tp, state, group,
    tok_h, nin_h, dlog_h, phase_h, bre_h, bim_h, cre_h, cim_h, skip_h, wv_h, wg_h, nout_h,
    out,
    nsend, urecv, rows_a, rows_p, t1r, t1i, t2r, t2i, bs, cs, wbuf, xbuf, wsum, ylocal,
    e_send, e_all, l_ref, zbuf, wv, wg, acc_v, acc_g, sq_all,
    bre, bim, cre, cim, tok, nin, dlog, phase, skip, nout,
    load_sem, a_send, a_recv, e_ssem, e_rsem, z_send, z_recv, f_send, q_send, q_recv, met,
):
    sp, tp = lax.axis_index("sp"), lax.axis_index("tp")
    mine, d_model = tok.shape
    rows, width = acc_v.shape
    n_blk = width // LANES
    per = LANES // group
    lanes = per * state
    core = lax.rem(tp, 2)
    chip = tp // 2
    partner = tp + 1 - 2 * core
    n_chip = n_tp // 2
    span = 2 * mine
    near = max(n_sp // 2, 1)

    loads = [
        pltpu.make_async_copy(src, dst, load_sem.at[i])
        for i, (src, dst) in enumerate(
            (
                (tok_h, tok), (nin_h, nin), (dlog_h, dlog), (phase_h, phase),
                (bre_h, bre), (bim_h, bim), (cre_h, cre), (cim_h, cim),
                (skip_h, skip), (nout_h, nout), (wv_h, wv), (wg_h, wg),
            )
        )
    ]
    for copy in loads[:4]:
        copy.start()

    barrier = pltpu.get_barrier_semaphore()
    for k in range(1, n_tp):
        pl.semaphore_signal(
            barrier, inc=1, device_id={"tp": lax.rem(tp + k, n_tp)},
            device_id_type=pl.DeviceIdType.MESH,
        )

    def greet(j, c):
        pl.semaphore_signal(barrier, inc=1, device_id={"sp": j}, device_id_type=pl.DeviceIdType.MESH)
        return c

    lax.fori_loop(sp + 1, n_sp, greet, 0)
    for copy in loads[4:10]:
        copy.start()
    for copy in loads[:2]:
        copy.wait()

    xf = tok[...].astype(F32)
    scale = lax.rsqrt(jnp.sum(xf * xf, axis=1, keepdims=True) / d_model + NORM_EPS)
    normed = (xf * scale * nin[...]).astype(BF16)
    for j in range(n_tp):
        for blk in range(n_blk):
            at = j * width + blk * LANES
            nsend[j, blk] = normed[:, at : at + LANES]

    pl.semaphore_wait(barrier, n_tp - 1 + sp)

    sends = []
    far_peers = []
    for k in range(1, n_chip):
        other = lax.rem(chip + n_chip - k, n_chip)
        far_peers += [2 * other + core, 2 * other + 1 - core]

    def scatter(i, j, blk):
        copy = remote(
            nsend.at[j, blk], urecv.at[tp, blk], a_send.at[i, blk], a_recv.at[tp, blk], {"tp": j}
        )
        copy.start()
        sends.append(copy)

    for blk in range(n_blk):
        for i, j in enumerate(far_peers):
            scatter(i, j, blk)
        if blk == 0:
            for b in range(n_blk):
                scatter(n_tp - 2, partner, b)

    def ready(j, c):
        pl.semaphore_signal(met.at[sp], inc=1, device_id={"sp": j}, device_id_type=pl.DeviceIdType.MESH)
        return c

    lax.fori_loop(0, sp, ready, 0)
    for copy in loads[10:]:
        copy.start()
    urecv[tp] = nsend[tp]

    for copy in loads[2:4]:
        copy.wait()
    side = LANES // state
    for i in range(width // group // side):
        cut = slice(i * LANES, (i + 1) * LANES)
        for src, dst in ((dlog, rows_a), (phase, rows_p)):
            row = jnp.concatenate([src[i * side + k : i * side + k + 1, :] for k in range(side)], axis=1)
            dst[:, cut] = jnp.broadcast_to(row, (8, LANES))

    for blk in range(n_blk):
        cut = slice(blk * lanes, (blk + 1) * lanes)
        a, p = rows_a[:, cut], rows_p[:, cut]
        mag, cos, sin = jnp.exp(a), jnp.cos(p), jnp.sin(p)
        lr, li = mag * cos, mag * sin
        inv = jnp.exp(-a)
        nr, ni = inv * cos, -inv * sin
        mod = a * a + p * p
        cr = ((lr - 1.0) * a + li * p) / mod
        ci = (li * a - (lr - 1.0) * p) / mod
        one, zero = jnp.ones_like(a), jnp.zeros_like(a)
        pr, pi, mr, mi = one, zero, cr, ci
        sr, si, qr, qi = lr, li, nr, ni
        row = lax.broadcasted_iota(jnp.int32, a.shape, 0)
        for bit in range(3):
            on = lax.rem(row // (1 << bit), 2) == 1
            ar, ai = cmul(pr, pi, sr, si)
            pr, pi = jnp.where(on, ar, pr), jnp.where(on, ai, pi)
            ar, ai = cmul(mr, mi, qr, qi)
            mr, mi = jnp.where(on, ar, mr), jnp.where(on, ai, mi)
            sr, si = cmul(sr, si, sr, si)
            qr, qi = cmul(qr, qi, qr, qi)
        t2r[0:8, cut], t2i[0:8, cut], t1r[0:8, cut], t1i[0:8, cut] = pr, pi, mr, mi
        done = 8
        while done < span:
            more = min(done, span - done)
            for off in range(0, more, 8):
                src, dst = slice(off, off + 8), slice(done + off, done + off + 8)
                t2r[dst, cut], t2i[dst, cut] = cmul(t2r[src, cut], t2i[src, cut], sr, si)
                t1r[dst, cut], t1i[dst, cut] = cmul(t1r[src, cut], t1i[src, cut], qr, qi)
            sr, si = cmul(sr, si, sr, si)
            qr, qi = cmul(qr, qi, qr, qi)
            done += more
        endr, endi = t2r[span - 1 : span, cut], t2i[span - 1 : span, cut]
        wholer, wholei = cmul(endr, endi, lr[0:1], li[0:1])
        allr, alli = cpow(wholer, wholei, n_chip)
        for k, value in enumerate((allr, alli, lr[0:1], li[0:1], wholer, wholei, endr, endi)):
            l_ref[blk, k : k + 1, :] = value

    for copy in loads[4:10]:
        copy.wait()
    keep_b = (
        lax.broadcasted_iota(jnp.int32, (LANES, lanes), 0) // group
        == lax.broadcasted_iota(jnp.int32, (LANES, lanes), 1) // state
    )
    of_col = lax.broadcasted_iota(jnp.int32, (state, LANES), 1) // group
    a, p = dlog[...], phase[...]
    mag = jnp.exp(a)
    stepr, stepi = cpow(mag * jnp.cos(p), mag * jnp.sin(p), span)
    for blk in range(n_blk):
        ch = slice(blk * LANES, (blk + 1) * LANES)
        for part, in_ref in ((0, bre), (1, bim)):
            b = in_ref[ch, :]
            b = jnp.concatenate([b] * side, axis=1)
            wide = jnp.where(keep_b, jnp.concatenate([b] * (lanes // LANES), axis=1), 0.0)
            bs[blk, :, part * lanes : (part + 1) * lanes] = wide.astype(BF16)
        c_r, c_i = cre[ch, :], cim[ch, :]
        if n_chip > 1:
            spread = [
                jnp.concatenate(
                    [jnp.broadcast_to(s[g : g + 1], (group, state)) for g in range(blk * per, (blk + 1) * per)],
                    axis=0,
                )
                for s in (stepr, stepi)
            ]
        for c in range(n_chip):
            if c:
                c_r, c_i = cmul(c_r, c_i, *spread)
            turned = jnp.concatenate([c_r, -c_i], axis=1).T
            for part in range(2):
                piece = turned[part * state : (part + 1) * state]
                for g in range(per):
                    at = part * lanes + g * state
                    cs[blk, at : at + state, c * LANES : (c + 1) * LANES] = jnp.where(
                        of_col == g, piece, 0.0
                    ).astype(BF16)
    lower = (
        lax.broadcasted_iota(jnp.int32, (span, span), 0)
        >= lax.broadcasted_iota(jnp.int32, (span, span), 1)
    ).astype(BF16)

    def taken(j, blk):
        remote(
            nsend.at[j, blk], urecv.at[j, blk], a_send.at[0, blk], a_recv.at[j, blk], {"tp": partner}
        ).wait_recv()

    def source(c, blk):
        return jnp.concatenate([urecv[2 * c + s, blk].astype(F32) for s in range(2)], axis=0)

    def drive(c, blk):
        cut = slice(blk * lanes, (blk + 1) * lanes)
        d = jnp.dot(source(c, blk).astype(BF16), bs[blk], preferred_element_type=F32)
        wr, wi = cmul(d[:, :lanes], d[:, lanes:], t1r[:, cut], t1i[:, cut])
        wbuf[c, blk, :, :lanes] = wr.astype(BF16)
        wbuf[c, blk, :, lanes:] = wi.astype(BF16)
        wsum[c, blk, 0:1, :] = jnp.sum(wr, axis=0, keepdims=True)
        wsum[c, blk, 1:2, :] = jnp.sum(wi, axis=0, keepdims=True)

    def seeds(blk):
        turn = l_ref[blk, 4:5], l_ref[blk, 5:6]
        held = [None]
        for c in range(n_chip):
            r, i = wsum[c, blk, 0:1], wsum[c, blk, 1:2]
            if c:
                r, i = r + held[c][0], i + held[c][1]
            held.append(cmul(r, i, *turn) if c < n_chip - 1 else cmul(r, i, l_ref[blk, 6:7], l_ref[blk, 7:8]))
        return held

    def end_copy(j, blk):
        return remote(
            e_send.at[blk], e_all.at[sp, blk], e_ssem.at[j, blk], e_rsem.at[sp, blk], {"sp": j}
        )

    def local(blk):
        cut = slice(blk * lanes, (blk + 1) * lanes)
        ch = slice(blk * LANES, (blk + 1) * LANES)
        held = seeds(blk)
        for c in range(n_chip):
            s = jnp.dot(lower, wbuf[c, blk], preferred_element_type=F32)
            sr, si = s[:, :lanes], s[:, lanes:]
            if c:
                sr, si = sr + held[c][0], si + held[c][1]
            xr, xi = cmul(sr, si, t2r[:, cut], t2i[:, cut])
            at = slice(c * span, (c + 1) * span)
            xbuf[blk, at, :lanes] = xr.astype(BF16)
            xbuf[blk, at, lanes:] = xi.astype(BF16)
        y = jnp.dot(xbuf[blk], cs[blk, :, :LANES], preferred_element_type=F32)
        for c in range(n_chip):
            at = slice(c * span, (c + 1) * span)
            ylocal[blk, at] = y[at] + skip[:, ch] * source(c, blk)

    for blk in range(n_blk):
        taken(partner, blk)
    for blk in range(n_blk):
        drive(chip, blk)

    def send_ends(blk, first, last):
        def go(j, c):
            end_copy(j, blk).start()
            return c

        lax.fori_loop(first, last, go, 0)

    def meet(first, last):
        def go(j, c):
            pl.semaphore_wait(met.at[j], 1)
            return c

        lax.fori_loop(first, last, go, 0)

    close = jnp.minimum(sp + 1 + near, n_sp)
    for blk in range(n_blk):
        for k in range(1, n_chip):
            c = lax.rem(chip + k, n_chip)
            taken(2 * c, blk)
            taken(2 * c + 1, blk)
        for k in range(1, n_chip):
            drive(lax.rem(chip + k, n_chip), blk)
        er, ei = seeds(blk)[n_chip]
        e_send[blk] = jnp.concatenate([er, ei], axis=0).astype(BF16)
        if blk:
            local(blk - 1)
        if blk == 0:
            meet(sp + 1, close)
        send_ends(blk, sp + 1, close)
    local(n_blk - 1)

    def send_far():
        meet(close, n_sp)
        for blk in range(n_blk):
            send_ends(blk, close, n_sp)

    pl.when(sp > 0)(send_far)

    for blk in range(n_blk):
        cut = slice(blk * lanes, (blk + 1) * lanes)
        lr, li = l_ref[blk, 0:1], l_ref[blk, 1:2]

        def join(j, held, blk=blk, lr=lr, li=li):
            remote(
                e_send.at[blk], e_all.at[j, blk], e_ssem.at[j, blk], e_rsem.at[j, blk], {"sp": j}
            ).wait_recv()
            e = e_all[j, blk].astype(F32)
            hr, hi = cmul(*held, lr, li)
            return hr + e[0:1], hi + e[1:2]

        nil = jnp.zeros((1, lanes), F32)
        hr, hi = lax.fori_loop(0, sp, join, (nil, nil))
        hr, hi = cmul(hr, hi, l_ref[blk, 2:3], l_ref[blk, 3:4])
        xr, xi = cmul(hr, hi, t2r[:, cut], t2i[:, cut])
        x = jnp.concatenate([xr.astype(BF16), xi.astype(BF16)], axis=1)
        y = jnp.dot(x, cs[blk], preferred_element_type=F32)
        for c in range(n_chip):
            at = slice(c * span, (c + 1) * span)
            zbuf[tp, blk, at] = jax.nn.gelu(y[:, c * LANES : (c + 1) * LANES] + ylocal[blk, at]).astype(BF16)
        for k in range(1, n_chip):
            j = lax.rem(tp + 2 * k, n_tp)
            copy = remote(
                zbuf.at[tp, blk], zbuf.at[tp, blk], z_send.at[k, blk], z_recv.at[tp, blk], {"tp": j}
            )
            copy.start()
            sends.append(copy)
        copy = remote(
            zbuf.at[tp, blk], zbuf.at[tp, blk], z_send.at[0, blk], z_recv.at[tp, blk], {"tp": partner}
        )
        copy.start()
        sends.append(copy)
    pl.when(sp == 0)(send_far)

    for copy in loads[10:]:
        copy.wait()

    def arrived(j, blk):
        remote(
            zbuf.at[j, blk], zbuf.at[j, blk], z_send.at[0, blk], z_recv.at[j, blk], {"tp": partner}
        ).wait_recv()

    def project(items):
        at = [pl.ds(pl.multiple_of(j * width + blk * LANES, LANES), LANES) for j, blk in items]
        z = jnp.concatenate([zbuf[j, blk] for j, blk in items], axis=1)
        return [
            jnp.dot(z, jnp.concatenate([w[a, :] for a in at], axis=0), preferred_element_type=F32)
            for w in (wv, wg)
        ]

    v, g = project([(tp, blk) for blk in range(n_blk)])
    acc_v[...], acc_g[...] = v, g
    for blk in range(n_blk):
        arrived(partner, blk)
    v, g = project([(partner, blk) for blk in range(n_blk)])
    acc_v[...] += v
    acc_g[...] += g
    late = []
    ripe = []

    def flush():
        v, g = project(ripe)
        ripe.clear()
        acc_v[...] += v
        acc_g[...] += g

    for blk in range(n_blk):
        for k in range(1, n_chip):
            j = lax.rem(tp + n_tp - 2 * k, n_tp)
            arrived(j, blk)
            copy = remote(
                zbuf.at[j, blk], zbuf.at[j, blk], f_send.at[k, blk], z_recv.at[j, blk], {"tp": partner}
            )
            copy.start()
            sends.append(copy)
            ripe.append((j, blk))
            if len(ripe) == 2:
                flush()
            late.append((lax.rem(partner + n_tp - 2 * k, n_tp), blk))
            if len(late) > 1:
                item = late.pop(0)
                arrived(*item)
                ripe.append(item)
                if len(ripe) == 2:
                    flush()
    if ripe:
        flush()
    for item in late:
        arrived(*item)
    if late:
        v, g = project(late)
        v, g = acc_v[...] + v, acc_g[...] + g
    else:
        v, g = acc_v[...], acc_g[...]

    gated = v * (0.5 + 0.5 * jnp.tanh(0.5 * g))
    acc_v[...] = gated
    square = gated * gated
    part = square[:, :LANES]
    for blk in range(1, n_blk):
        part = part + square[:, blk * LANES : (blk + 1) * LANES]
    sums = jnp.sum(part, axis=1, keepdims=True)
    lane = lax.broadcasted_iota(jnp.int32, (8, LANES), 1)
    total = jnp.zeros((8, LANES), F32)
    for k in range(rows // 8):
        total = jnp.where(lane == k, sums[8 * k : 8 * k + 8], total)
    sq_all[tp] = total
    for k in range(1, n_tp):
        j = lax.rem(tp + n_tp - k, n_tp)
        copy = remote(sq_all.at[tp], sq_all.at[tp], q_send.at[k], q_recv.at[tp], {"tp": j})
        copy.start()
        sends.append(copy)
    for k in range(1, n_tp):
        j = lax.rem(tp + k, n_tp)
        remote(sq_all.at[j], sq_all.at[j], q_send.at[k], q_recv.at[j], {"tp": j}).wait_recv()
        total = total + sq_all[j]
    scale = lax.rsqrt(total / d_model + NORM_EPS)
    for k in range(0, rows // 8, 2):
        two = range(k, min(k + 2, rows // 8))
        column = jnp.concatenate([scale[:, i : i + 1] for i in two], axis=0)
        at = slice(8 * k, 8 * k + 8 * len(two))
        out[at, :] = (acc_v[at, :] * column * nout[...]).astype(BF16)

    for copy in sends:
        copy.wait_send()

    def sent(j, c):
        for blk in range(n_blk):
            end_copy(j, blk).wait_send()
        return c

    lax.fori_loop(sp + 1, n_sp, sent, 0)


def solution(mesh):
    n_sp, n_tp = mesh.shape["sp"], mesh.shape["tp"]

    def on_device(
        tokens, norm_in, decay_log, phase, b_real, b_imag, c_real, c_imag, skip_gain, w_value, w_gate, norm_out
    ):
        mine, d_model = tokens.shape
        rows = mine * n_tp
        groups, state, group = b_real.shape
        width = groups * group
        n_blk = width // LANES
        lanes = LANES // group * state
        entries = groups * state
        n_chip = n_tp // 2
        span = 2 * mine
        vmem = pl.BlockSpec(memory_space=pltpu.VMEM)
        hbm = pl.BlockSpec(memory_space=pl.ANY)
        dma = pltpu.SemaphoreType.DMA
        return pl.pallas_call(
            functools.partial(layer, n_sp, n_tp, state, group),
            out_shape=pltpu.VMEM((rows, width), BF16),
            in_specs=[hbm] * 12,
            out_specs=vmem,
            scratch_shapes=[
                pltpu.VMEM((n_tp, n_blk, mine, LANES), BF16),
                pltpu.VMEM((n_tp, n_blk, mine, LANES), BF16),
                pltpu.VMEM((8, entries), F32),
                pltpu.VMEM((8, entries), F32),
                pltpu.VMEM((span, entries), F32),
                pltpu.VMEM((span, entries), F32),
                pltpu.VMEM((span, entries), F32),
                pltpu.VMEM((span, entries), F32),
                pltpu.VMEM((n_blk, LANES, 2 * lanes), BF16),
                pltpu.VMEM((n_blk, 2 * lanes, n_chip * LANES), BF16),
                pltpu.VMEM((n_chip, n_blk, span, 2 * lanes), BF16),
                pltpu.VMEM((n_blk, rows, 2 * lanes), BF16),
                pltpu.VMEM((n_chip, n_blk, 2, lanes), F32),
                pltpu.VMEM((n_blk, rows, LANES), F32),
                pltpu.VMEM((n_blk, 2, lanes), BF16),
                pltpu.VMEM((n_sp, n_blk, 2, lanes), BF16),
                pltpu.VMEM((n_blk, 8, lanes), F32),
                pltpu.VMEM((n_tp, n_blk, rows, LANES), BF16),
                pltpu.VMEM(w_value.shape, BF16),
                pltpu.VMEM(w_gate.shape, BF16),
                pltpu.VMEM((rows, width), F32),
                pltpu.VMEM((rows, width), F32),
                pltpu.VMEM((n_tp, 8, LANES), F32),
                pltpu.VMEM((width, state), F32),
                pltpu.VMEM((width, state), F32),
                pltpu.VMEM((width, state), F32),
                pltpu.VMEM((width, state), F32),
                pltpu.VMEM((mine, d_model), BF16),
                pltpu.VMEM((1, d_model), F32),
                pltpu.VMEM((groups, state), F32),
                pltpu.VMEM((groups, state), F32),
                pltpu.VMEM((1, width), F32),
                pltpu.VMEM((1, width), F32),
                dma((12,)),
                dma((n_tp - 1, n_blk)),
                dma((n_tp, n_blk)),
                dma((n_sp, n_blk)),
                dma((n_sp, n_blk)),
                dma((n_chip, n_blk)),
                dma((n_tp, n_blk)),
                dma((n_chip, n_blk)),
                dma((n_tp,)),
                dma((n_tp,)),
                pltpu.SemaphoreType.REGULAR((n_sp,)),
            ],
            compiler_params=pltpu.CompilerParams(collective_id=0, has_side_effects=True),
        )(
            tokens,
            norm_in.reshape(1, -1),
            decay_log,
            phase,
            b_real.transpose(0, 2, 1).reshape(width, state),
            b_imag.transpose(0, 2, 1).reshape(width, state),
            c_real.reshape(width, state),
            c_imag.reshape(width, state),
            skip_gain.reshape(1, -1),
            w_value,
            w_gate,
            norm_out.reshape(1, -1),
        )

    placed = (
        P(("sp", "tp"), None),
        P(),
        P("tp", None),
        P("tp", None),
        P("tp", None, None),
        P("tp", None, None),
        P("tp", None, None),
        P("tp", None, None),
        P("tp"),
        P(None, "tp"),
        P(None, "tp"),
        P("tp"),
    )
    return jax.shard_map(
        on_device, mesh=mesh, in_specs=placed, out_specs=P("sp", "tp"), check_vma=False
    )
```

```python
import functools

import jax
import jax.numpy as jnp
from jax import lax
from jax.experimental import pallas as pl
from jax.experimental.pallas import tpu as pltpu
from jax.sharding import PartitionSpec as P

NORM_EPS = 1e-06
LANES = 128
F32 = jnp.float32
BF16 = jnp.bfloat16


def cmul(ar, ai, br, bi):
    return ar * br - ai * bi, ar * bi + ai * br


def cpow(r, i, n):
    outr, outi = None, None
    while n:
        if n % 2:
            outr, outi = (r, i) if outr is None else cmul(outr, outi, r, i)
        n //= 2
        if n:
            r, i = cmul(r, i, r, i)
    return outr, outi


def remote(src, dst, send, recv, target):
    return pltpu.make_async_remote_copy(
        src_ref=src,
        dst_ref=dst,
        send_sem=send,
        recv_sem=recv,
        device_id=target,
        device_id_type=pl.DeviceIdType.MESH,
    )


def layer(
    n_sp, n_tp, state, group,
    tok_h, nin_h, dlog_h, phase_h, bre_h, bim_h, cre_h, cim_h, skip_h, wv_h, wg_h, nout_h,
    out,
    nsend, urecv, rows_a, rows_p, t1r, t1i, t2r, t2i, bs, cs, wbuf, xbuf, wsum, ylocal,
    e_send, e_all, l_ref, zbuf, wv, wg, acc_v, acc_g, sq_all,
    bre, bim, cre, cim, tok, nin, dlog, phase, skip, nout,
    load_sem, a_send, a_recv, e_ssem, e_rsem, z_send, z_recv, f_send, q_send, q_recv, met, met_tp,
):
    sp, tp = lax.axis_index("sp"), lax.axis_index("tp")
    mine, d_model = tok.shape
    rows, width = acc_v.shape
    n_blk = width // LANES
    per = LANES // group
    lanes = per * state
    core = lax.rem(tp, 2)
    chip = tp // 2
    partner = tp + 1 - 2 * core
    n_chip = n_tp // 2
    span = 2 * mine
    pair = 2 if n_sp % 2 == 0 else 1
    sp_b = lax.rem(sp, pair)

    loads = [
        pltpu.make_async_copy(src, dst, load_sem.at[i])
        for i, (src, dst) in enumerate(
            (
                (tok_h, tok), (nin_h, nin), (dlog_h, dlog), (phase_h, phase),
                (bre_h, bre), (bim_h, bim), (cre_h, cre), (cim_h, cim),
                (skip_h, skip), (nout_h, nout), (wv_h, wv), (wg_h, wg),
            )
        )
    ]
    for copy in loads[:4]:
        copy.start()

    barrier = pltpu.get_barrier_semaphore()

    def tell(sem, axis):
        def go(j, c):
            pl.semaphore_signal(sem, inc=1, device_id={axis: j}, device_id_type=pl.DeviceIdType.MESH)
            return c

        return go

    def above(go):
        for b in range(pair):
            first = sp // pair + jnp.where(b > sp_b, 0, 1)
            go_b = lambda a, c, b=b: go(a * pair + b, c)
            lax.fori_loop(jnp.where(b >= sp_b, first, n_sp // pair), n_sp // pair, go_b, 0)

    def below(go):
        for b in range(pair):
            last = sp // pair + jnp.where(b < sp_b, 1, 0)
            lax.fori_loop(0, jnp.where(b <= sp_b, last, 0), lambda a, c, b=b: go(a * pair + b, c), 0)

    lax.fori_loop(tp + 1, n_tp, tell(barrier, "tp"), 0)
    above(tell(barrier, "sp"))
    for copy in loads[4:10]:
        copy.start()
    pl.when(tp + sp > 0)(lambda: pl.semaphore_wait(barrier, tp + (sp // pair + 1) * (sp_b + 1) - 1))
    below(tell(met.at[sp], "sp"))
    lax.fori_loop(0, tp, tell(met_tp.at[tp], "tp"), 0)
    for copy in loads[:2]:
        copy.wait()

    xf = tok[...].astype(F32)
    scale = lax.rsqrt(jnp.sum(xf * xf, axis=1, keepdims=True) / d_model + NORM_EPS)
    normed = (xf * scale * nin[...]).astype(BF16)
    for j in range(n_tp):
        for blk in range(n_blk):
            at = j * width + blk * LANES
            nsend[j, blk] = normed[:, at : at + LANES]

    def meet(sem):
        def go(j, c):
            pl.semaphore_wait(sem.at[j], 1)
            return c

        return go

    lax.fori_loop(tp + 1, n_tp, meet(met_tp), 0)

    sends = []
    far_peers = []
    for k in range(1, n_chip):
        other = lax.rem(chip + n_chip - k, n_chip)
        far_peers += [2 * other + core, 2 * other + 1 - core]

    def scatter(i, j, blk):
        copy = remote(
            nsend.at[j, blk], urecv.at[tp, blk], a_send.at[i, blk], a_recv.at[tp, blk], {"tp": j}
        )
        copy.start()
        sends.append(copy)

    for blk in range(n_blk):
        for i, j in enumerate(far_peers):
            scatter(i, j, blk)
        if blk == 0:
            for b in range(n_blk):
                scatter(n_tp - 2, partner, b)

    for copy in loads[10:]:
        copy.start()
    urecv[tp] = nsend[tp]

    for copy in loads[2:4]:
        copy.wait()
    side = LANES // state
    for i in range(width // group // side):
        cut = slice(i * LANES, (i + 1) * LANES)
        for src, dst in ((dlog, rows_a), (phase, rows_p)):
            row = jnp.concatenate([src[i * side + k : i * side + k + 1, :] for k in range(side)], axis=1)
            dst[:, cut] = jnp.broadcast_to(row, (8, LANES))

    for blk in range(n_blk):
        cut = slice(blk * lanes, (blk + 1) * lanes)
        a, p = rows_a[:, cut], rows_p[:, cut]
        mag, cos, sin = jnp.exp(a), jnp.cos(p), jnp.sin(p)
        lr, li = mag * cos, mag * sin
        inv = jnp.exp(-a)
        nr, ni = inv * cos, -inv * sin
        mod = a * a + p * p
        cr = ((lr - 1.0) * a + li * p) / mod
        ci = (li * a - (lr - 1.0) * p) / mod
        one, zero = jnp.ones_like(a), jnp.zeros_like(a)
        pr, pi, mr, mi = one, zero, cr, ci
        sr, si, qr, qi = lr, li, nr, ni
        row = lax.broadcasted_iota(jnp.int32, a.shape, 0)
        for bit in range(3):
            on = lax.rem(row // (1 << bit), 2) == 1
            ar, ai = cmul(pr, pi, sr, si)
            pr, pi = jnp.where(on, ar, pr), jnp.where(on, ai, pi)
            ar, ai = cmul(mr, mi, qr, qi)
            mr, mi = jnp.where(on, ar, mr), jnp.where(on, ai, mi)
            sr, si = cmul(sr, si, sr, si)
            qr, qi = cmul(qr, qi, qr, qi)
        t2r[0:8, cut], t2i[0:8, cut], t1r[0:8, cut], t1i[0:8, cut] = pr, pi, mr, mi
        done = 8
        while done < span:
            more = min(done, span - done)
            for off in range(0, more, 8):
                src, dst = slice(off, off + 8), slice(done + off, done + off + 8)
                t2r[dst, cut], t2i[dst, cut] = cmul(t2r[src, cut], t2i[src, cut], sr, si)
                t1r[dst, cut], t1i[dst, cut] = cmul(t1r[src, cut], t1i[src, cut], qr, qi)
            sr, si = cmul(sr, si, sr, si)
            qr, qi = cmul(qr, qi, qr, qi)
            done += more
        endr, endi = t2r[span - 1 : span, cut], t2i[span - 1 : span, cut]
        wholer, wholei = cmul(endr, endi, lr[0:1], li[0:1])
        allr, alli = cpow(wholer, wholei, n_chip)
        for k, value in enumerate((allr, alli, lr[0:1], li[0:1], wholer, wholei, endr, endi)):
            l_ref[blk, k : k + 1, :] = value

    for copy in loads[4:10]:
        copy.wait()
    keep_b = (
        lax.broadcasted_iota(jnp.int32, (LANES, lanes), 0) // group
        == lax.broadcasted_iota(jnp.int32, (LANES, lanes), 1) // state
    )
    of_col = lax.broadcasted_iota(jnp.int32, (state, LANES), 1) // group
    a, p = dlog[...], phase[...]
    mag = jnp.exp(a)
    stepr, stepi = cpow(mag * jnp.cos(p), mag * jnp.sin(p), span)
    for blk in range(n_blk):
        ch = slice(blk * LANES, (blk + 1) * LANES)
        for part, in_ref in ((0, bre), (1, bim)):
            b = in_ref[ch, :]
            b = jnp.concatenate([b] * side, axis=1)
            wide = jnp.where(keep_b, jnp.concatenate([b] * (lanes // LANES), axis=1), 0.0)
            bs[blk, :, part * lanes : (part + 1) * lanes] = wide.astype(BF16)
        c_r, c_i = cre[ch, :], cim[ch, :]
        if n_chip > 1:
            spread = [
                jnp.concatenate(
                    [jnp.broadcast_to(s[g : g + 1], (group, state)) for g in range(blk * per, (blk + 1) * per)],
                    axis=0,
                )
                for s in (stepr, stepi)
            ]
        for c in range(n_chip):
            if c:
                c_r, c_i = cmul(c_r, c_i, *spread)
            turned = jnp.concatenate([c_r, -c_i], axis=1).T
            for part in range(2):
                piece = turned[part * state : (part + 1) * state]
                for g in range(per):
                    at = part * lanes + g * state
                    cs[blk, at : at + state, c * LANES : (c + 1) * LANES] = jnp.where(
                        of_col == g, piece, 0.0
                    ).astype(BF16)
    lower = (
        lax.broadcasted_iota(jnp.int32, (span, span), 0)
        >= lax.broadcasted_iota(jnp.int32, (span, span), 1)
    ).astype(BF16)

    def taken(j, blk):
        remote(
            nsend.at[j, blk], urecv.at[j, blk], a_send.at[0, blk], a_recv.at[j, blk], {"tp": partner}
        ).wait_recv()

    def source(c, blk):
        return jnp.concatenate([urecv[2 * c + s, blk].astype(F32) for s in range(2)], axis=0)

    def drive(c, blk):
        cut = slice(blk * lanes, (blk + 1) * lanes)
        d = jnp.dot(source(c, blk).astype(BF16), bs[blk], preferred_element_type=F32)
        wr, wi = cmul(d[:, :lanes], d[:, lanes:], t1r[:, cut], t1i[:, cut])
        wbuf[blk][c, :, :lanes] = wr.astype(BF16)
        wbuf[blk][c, :, lanes:] = wi.astype(BF16)
        wsum[blk][c, 0:1, :] = jnp.sum(wr, axis=0, keepdims=True)
        wsum[blk][c, 1:2, :] = jnp.sum(wi, axis=0, keepdims=True)

    def seeds(blk):
        turn = l_ref[blk, 4:5], l_ref[blk, 5:6]
        held = [None]
        for c in range(n_chip):
            r, i = wsum[blk][c, 0:1], wsum[blk][c, 1:2]
            if c:
                r, i = r + held[c][0], i + held[c][1]
            held.append(cmul(r, i, *turn) if c < n_chip - 1 else cmul(r, i, l_ref[blk, 6:7], l_ref[blk, 7:8]))
        return held

    def end_copy(j, blk):
        return remote(
            e_send.at[blk], e_all.at[sp, blk], e_ssem.at[j, blk], e_rsem.at[sp, blk], {"sp": j}
        )

    def scan(blk):
        cut = slice(blk * lanes, (blk + 1) * lanes)
        held = seeds(blk)
        for c in range(n_chip):
            s = jnp.dot(lower, wbuf[blk][c], preferred_element_type=F32)
            sr, si = s[:, :lanes], s[:, lanes:]
            if c:
                sr, si = sr + held[c][0], si + held[c][1]
            xr, xi = cmul(sr, si, t2r[:, cut], t2i[:, cut])
            at = slice(c * span, (c + 1) * span)
            xbuf[blk][at, :lanes] = xr.astype(BF16)
            xbuf[blk][at, lanes:] = xi.astype(BF16)

    def readout(blk):
        ch = slice(blk * LANES, (blk + 1) * LANES)
        y = jnp.dot(xbuf[blk][...], cs[blk, :, :LANES], preferred_element_type=F32)
        for c in range(n_chip):
            at = slice(c * span, (c + 1) * span)
            ylocal[blk][at] = y[at] + skip[:, ch] * source(c, blk)

    for blk in range(n_blk):
        taken(partner, blk)
    for blk in range(n_blk):
        drive(chip, blk)

    def send_ends(blks, first, last):
        def go(j, c):
            for blk in blks:
                end_copy(j, blk).start()
            return c

        lax.fori_loop(first, last, go, 0)

    def finish(blk, y):
        for c in range(n_chip):
            at = slice(c * span, (c + 1) * span)
            v = ylocal[blk][at]
            if y is not None:
                v = v + y[:, c * LANES : (c + 1) * LANES]
            zbuf[tp, blk, at] = jax.nn.gelu(v).astype(BF16)
        for copy in z_copies(blk):
            copy.start()

    def z_copies(blk):
        return [
            remote(
                zbuf.at[tp, blk], zbuf.at[tp, blk], z_send.at[k, blk], z_recv.at[tp, blk],
                {"tp": lax.rem(tp + 2 * k, n_tp) if k else partner},
            )
            for k in list(range(1, n_chip)) + [0]
        ]

    def reach(j, c):
        odd = lax.rem(j, pair)

        @pl.when((sp_b == 0) | (odd == 0))
        def _():
            pl.semaphore_wait(met.at[jnp.where(sp_b == 0, j, j - odd + pair - 1)], 1)

        return c

    old = sp + 1
    for blk in range(n_blk + 2):
        if blk < n_blk:
            for k in range(1, n_chip):
                c = lax.rem(chip + k, n_chip)
                taken(2 * c, blk)
                taken(2 * c + 1, blk)
            for k in range(1, n_chip):
                drive(lax.rem(chip + k, n_chip), blk)
        if 1 <= blk <= n_blk:
            scan(blk - 1)
        if 2 <= blk:
            readout(blk - 2)
        if blk < n_blk:
            er, ei = seeds(blk)[n_chip]
            e_send[blk] = jnp.concatenate([er, ei], axis=0).astype(BF16)
            new = jnp.minimum(sp + 1 + n_sp // 2, n_sp) if blk == 0 else n_sp
            lax.fori_loop(old, new, reach, 0)
            if blk:
                send_ends([blk], sp + 1, old)
            send_ends(range(blk + 1), old, new)
            old = new
        if 2 <= blk:
            pl.when(sp == 0)(functools.partial(finish, blk - 2, None))

    def after(blk):
        cut = slice(blk * lanes, (blk + 1) * lanes)
        lr, li = l_ref[blk, 0:1], l_ref[blk, 1:2]

        def join(j, held):
            remote(
                e_send.at[blk], e_all.at[j, blk], e_ssem.at[j, blk], e_rsem.at[j, blk], {"sp": j}
            ).wait_recv()
            e = e_all[j, blk].astype(F32)
            hr, hi = cmul(*held, lr, li)
            return hr + e[0:1], hi + e[1:2]

        nil = jnp.zeros((1, lanes), F32)
        hr, hi = lax.fori_loop(0, sp, join, (nil, nil))
        hr, hi = cmul(hr, hi, l_ref[blk, 2:3], l_ref[blk, 3:4])
        xr, xi = cmul(hr, hi, t2r[:, cut], t2i[:, cut])
        x = jnp.concatenate([xr.astype(BF16), xi.astype(BF16)], axis=1)
        finish(blk, jnp.dot(x, cs[blk], preferred_element_type=F32))


    @pl.when(sp > 0)
    def _():
        for blk in range(n_blk):
            after(blk)

    for copy in loads[10:]:
        copy.wait()

    def arrived(j, blk):
        remote(
            zbuf.at[j, blk], zbuf.at[j, blk], z_send.at[0, blk], z_recv.at[j, blk], {"tp": partner}
        ).wait_recv()

    def project(items):
        at = [pl.ds(pl.multiple_of(j * width + blk * LANES, LANES), LANES) for j, blk in items]
        z = jnp.concatenate([zbuf[j, blk] for j, blk in items], axis=1)
        return [
            jnp.dot(z, jnp.concatenate([w[a, :] for a in at], axis=0), preferred_element_type=F32)
            for w in (wv, wg)
        ]

    v, g = project([(tp, blk) for blk in range(n_blk)])
    acc_v[...], acc_g[...] = v, g
    for blk in range(n_blk):
        arrived(partner, blk)
    v, g = project([(partner, blk) for blk in range(n_blk)])
    acc_v[...] += v
    acc_g[...] += g
    late = []
    ripe = []

    def flush():
        v, g = project(ripe)
        ripe.clear()
        acc_v[...] += v
        acc_g[...] += g

    for blk in range(n_blk):
        for k in range(1, n_chip):
            j = lax.rem(tp + n_tp - 2 * k, n_tp)
            arrived(j, blk)
            copy = remote(
                zbuf.at[j, blk], zbuf.at[j, blk], f_send.at[k, blk], z_recv.at[j, blk], {"tp": partner}
            )
            copy.start()
            sends.append(copy)
            ripe.append((j, blk))
            if len(ripe) == 2:
                flush()
            late.append((lax.rem(partner + n_tp - 2 * k, n_tp), blk))
            if len(late) > 1:
                item = late.pop(0)
                arrived(*item)
                ripe.append(item)
                if len(ripe) == 2:
                    flush()
    if ripe:
        flush()
    for item in late:
        arrived(*item)
    if late:
        v, g = project(late)
        v, g = acc_v[...] + v, acc_g[...] + g
    else:
        v, g = acc_v[...], acc_g[...]

    gated = v * (0.5 + 0.5 * jnp.tanh(0.5 * g))
    acc_v[...] = gated
    square = gated * gated
    part = square[:, :LANES]
    for blk in range(1, n_blk):
        part = part + square[:, blk * LANES : (blk + 1) * LANES]
    sums = jnp.sum(part, axis=1, keepdims=True)
    lane = lax.broadcasted_iota(jnp.int32, (8, LANES), 1)
    total = jnp.zeros((8, LANES), F32)
    for k in range(rows // 8):
        total = jnp.where(lane == k, sums[8 * k : 8 * k + 8], total)
    sq_all[tp] = total
    sums_out = []
    for k in range(1, n_tp):
        j = lax.rem(tp + n_tp - k, n_tp)
        copy = remote(sq_all.at[tp], sq_all.at[tp], q_send.at[k], q_recv.at[tp], {"tp": j})
        copy.start()
        sums_out.append(copy)
    for blk in range(n_blk):
        sends += z_copies(blk)
    for copy in sends:
        copy.wait_send()

    def sent(j, c):
        for blk in range(n_blk):
            end_copy(j, blk).wait_send()
        return c

    lax.fori_loop(sp + 1, n_sp, sent, 0)
    for k in range(1, n_tp):
        j = lax.rem(tp + k, n_tp)
        remote(sq_all.at[j], sq_all.at[j], q_send.at[k], q_recv.at[j], {"tp": j}).wait_recv()
        total = total + sq_all[j]
    scale = lax.rsqrt(total / d_model + NORM_EPS)
    for k in range(0, rows // 8, 2):
        two = range(k, min(k + 2, rows // 8))
        column = jnp.concatenate([scale[:, i : i + 1] for i in two], axis=0)
        at = slice(8 * k, 8 * k + 8 * len(two))
        out[at, :] = (acc_v[at, :] * column * nout[...]).astype(BF16)

    for copy in sums_out:
        copy.wait_send()


def solution(mesh):
    n_sp, n_tp = mesh.shape["sp"], mesh.shape["tp"]

    def on_device(
        tokens, norm_in, decay_log, phase, b_real, b_imag, c_real, c_imag, skip_gain, w_value, w_gate, norm_out
    ):
        mine, d_model = tokens.shape
        rows = mine * n_tp
        groups, state, group = b_real.shape
        width = groups * group
        n_blk = width // LANES
        lanes = LANES // group * state
        entries = groups * state
        n_chip = n_tp // 2
        span = 2 * mine
        vmem = pl.BlockSpec(memory_space=pltpu.VMEM)
        hbm = pl.BlockSpec(memory_space=pl.ANY)
        dma = pltpu.SemaphoreType.DMA
        return pl.pallas_call(
            functools.partial(layer, n_sp, n_tp, state, group),
            out_shape=pltpu.VMEM((rows, width), BF16),
            in_specs=[hbm] * 12,
            out_specs=vmem,
            scratch_shapes=[
                pltpu.VMEM((n_tp, n_blk, mine, LANES), BF16),
                pltpu.VMEM((n_tp, n_blk, mine, LANES), BF16),
                pltpu.VMEM((8, entries), F32),
                pltpu.VMEM((8, entries), F32),
                pltpu.VMEM((span, entries), F32),
                pltpu.VMEM((span, entries), F32),
                pltpu.VMEM((span, entries), F32),
                pltpu.VMEM((span, entries), F32),
                pltpu.VMEM((n_blk, LANES, 2 * lanes), BF16),
                pltpu.VMEM((n_blk, 2 * lanes, n_chip * LANES), BF16),
                [pltpu.VMEM((n_chip, span, 2 * lanes), BF16)] * n_blk,
                [pltpu.VMEM((rows, 2 * lanes), BF16)] * n_blk,
                [pltpu.VMEM((n_chip, 2, lanes), F32)] * n_blk,
                [pltpu.VMEM((rows, LANES), F32)] * n_blk,
                pltpu.VMEM((n_blk, 2, lanes), BF16),
                pltpu.VMEM((n_sp, n_blk, 2, lanes), BF16),
                pltpu.VMEM((n_blk, 8, lanes), F32),
                pltpu.VMEM((n_tp, n_blk, rows, LANES), BF16),
                pltpu.VMEM(w_value.shape, BF16),
                pltpu.VMEM(w_gate.shape, BF16),
                pltpu.VMEM((rows, width), F32),
                pltpu.VMEM((rows, width), F32),
                pltpu.VMEM((n_tp, 8, LANES), F32),
                pltpu.VMEM((width, state), F32),
                pltpu.VMEM((width, state), F32),
                pltpu.VMEM((width, state), F32),
                pltpu.VMEM((width, state), F32),
                pltpu.VMEM((mine, d_model), BF16),
                pltpu.VMEM((1, d_model), F32),
                pltpu.VMEM((groups, state), F32),
                pltpu.VMEM((groups, state), F32),
                pltpu.VMEM((1, width), F32),
                pltpu.VMEM((1, width), F32),
                dma((12,)),
                dma((n_tp - 1, n_blk)),
                dma((n_tp, n_blk)),
                dma((n_sp, n_blk)),
                dma((n_sp, n_blk)),
                dma((n_chip, n_blk)),
                dma((n_tp, n_blk)),
                dma((n_chip, n_blk)),
                dma((n_tp,)),
                dma((n_tp,)),
                pltpu.SemaphoreType.REGULAR((n_sp,)),
                pltpu.SemaphoreType.REGULAR((n_tp,)),
            ],
            compiler_params=pltpu.CompilerParams(collective_id=0, has_side_effects=True),
        )(
            tokens,
            norm_in.reshape(1, -1),
            decay_log,
            phase,
            b_real.transpose(0, 2, 1).reshape(width, state),
            b_imag.transpose(0, 2, 1).reshape(width, state),
            c_real.reshape(width, state),
            c_imag.reshape(width, state),
            skip_gain.reshape(1, -1),
            w_value,
            w_gate,
            norm_out.reshape(1, -1),
        )

    placed = (
        P(("sp", "tp"), None),
        P(),
        P("tp", None),
        P("tp", None),
        P("tp", None, None),
        P("tp", None, None),
        P("tp", None, None),
        P("tp", None, None),
        P("tp"),
        P(None, "tp"),
        P(None, "tp"),
        P("tp"),
    )
    return jax.shard_map(
        on_device, mesh=mesh, in_specs=placed, out_specs=P("sp", "tp"), check_vma=False
    )
```

```python
import functools

import jax
import jax.numpy as jnp
from jax import lax
from jax.experimental import pallas as pl
from jax.experimental.pallas import tpu as pltpu
from jax.sharding import PartitionSpec as P

NORM_EPS = 1e-06
LANES = 128
F32 = jnp.float32
BF16 = jnp.bfloat16


def cmul(ar, ai, br, bi):
    return ar * br - ai * bi, ar * bi + ai * br


def cpow(r, i, n):
    outr, outi = None, None
    while n:
        if n % 2:
            outr, outi = (r, i) if outr is None else cmul(outr, outi, r, i)
        n //= 2
        if n:
            r, i = cmul(r, i, r, i)
    return outr, outi


def remote(src, dst, send, recv, target):
    return pltpu.make_async_remote_copy(
        src_ref=src,
        dst_ref=dst,
        send_sem=send,
        recv_sem=recv,
        device_id=target,
        device_id_type=pl.DeviceIdType.MESH,
    )


def layer(
    n_sp, n_tp, state, group,
    tok_h, nin_h, dlog_h, phase_h, bre_h, bim_h, cre_h, cim_h, skip_h, wv_h, wg_h, nout_h,
    out,
    nsend, urecv, rows_a, rows_p, t1r, t1i, t2r, t2i, bs, cs, wbuf, xbuf, wsum, ylocal,
    e_send, e_all, l_ref, zbuf, w, acc_v, acc_g, sq_all,
    bc, tok, nin, ap, sn,
    load_sem, a_send, a_recv, e_ssem, e_rsem, z_send, z_recv, f_send, q_sem, met,
):
    sp, tp = lax.axis_index("sp"), lax.axis_index("tp")
    mine, d_model = tok.shape
    rows, width = acc_v.shape
    n_blk = width // LANES
    per = LANES // group
    lanes = per * state
    core = lax.rem(tp, 2)
    chip = tp // 2
    partner = tp + 1 - 2 * core
    n_chip = n_tp // 2
    span = 2 * mine
    pair = 2 if n_sp % 2 == 0 else 1
    sp_b = lax.rem(sp, pair)

    def load(i, *pairs):
        return [pltpu.make_async_copy(src, dst, load_sem.at[i]) for src, dst in pairs]

    loads = [
        load(0, (tok_h, tok)),
        load(1, (nin_h, nin)),
        load(2, (dlog_h, ap.at[0]), (phase_h, ap.at[1])),
        load(3, *((src, bc.at[i]) for i, src in enumerate((bre_h, bim_h, cre_h, cim_h)))),
        load(4, (skip_h, sn.at[0]), (nout_h, sn.at[1])),
        load(5, (wv_h, w.at[0]), (wg_h, w.at[1])),
    ]

    def start(*which):
        for i in which:
            for copy in loads[i]:
                copy.start()

    def loaded(*which):
        for i in which:
            dst = (tok, nin, ap, bc, sn, w)[i]
            pltpu.make_async_copy(dst, dst, load_sem.at[i]).wait()

    start(0, 1, 2)

    barrier = pltpu.get_barrier_semaphore()

    def tell(sem, axis):
        def go(j, c):
            pl.semaphore_signal(sem, inc=1, device_id={axis: j}, device_id_type=pl.DeviceIdType.MESH)
            return c

        return go

    def above(go):
        for b in range(pair):
            first = sp // pair + jnp.where(b > sp_b, 0, 1)
            go_b = lambda a, c, b=b: go(a * pair + b, c)
            lax.fori_loop(jnp.where(b >= sp_b, first, n_sp // pair), n_sp // pair, go_b, 0)

    def below(go):
        for b in range(pair):
            last = sp // pair + jnp.where(b < sp_b, 1, 0)
            lax.fori_loop(0, jnp.where(b <= sp_b, last, 0), lambda a, c, b=b: go(a * pair + b, c), 0)

    lax.fori_loop(tp + 1, n_tp, tell(barrier, "tp"), 0)
    above(tell(barrier, "sp"))
    start(3, 4)
    pl.when(tp + sp > 0)(lambda: pl.semaphore_wait(barrier, tp + (sp // pair + 1) * (sp_b + 1) - 1))
    half = (n_sp // 2 + pair - 1) // pair * pair
    below(lambda j, c: tell(met.at[jnp.where(sp - j > half, 1, 0)], "sp")(j, c))
    lax.fori_loop(0, tp, tell(met.at[2], "tp"), 0)
    loaded(0, 1)

    xf = tok[...].astype(F32)
    scale = lax.rsqrt(jnp.sum(xf * xf, axis=1, keepdims=True) / d_model + NORM_EPS)
    normed = (xf * scale * nin[...]).astype(BF16)
    for j in range(n_tp):
        for blk in range(n_blk):
            at = j * width + blk * LANES
            nsend[j, blk] = normed[:, at : at + LANES]

    pl.when(tp < n_tp - 1)(lambda: pl.semaphore_wait(met.at[2], n_tp - 1 - tp))


    def scatter(j, blk, at):
        remote(nsend.at[j, blk], urecv.at[tp, blk], a_send.at[0], a_recv.at[at], {"tp": j}).start()

    for blk in range(n_blk):
        for k in range(1, n_chip):
            other = lax.rem(chip + n_chip - k, n_chip)
            for j in (2 * other + core, 2 * other + 1 - core):
                scatter(j, blk, 1 + (k - 1) * n_blk + blk)
        if blk == 0:
            for b in range(n_blk):
                scatter(partner, b, 0)
    start(5)
    urecv[tp] = nsend[tp]

    loaded(2)
    dlog, phase, skip, nout = ap.at[0], ap.at[1], sn.at[0], sn.at[1]
    bre, bim, cre, cim = (bc.at[i] for i in range(4))
    wv, wg = w.at[0], w.at[1]
    side = LANES // state
    for i in range(width // group // side):
        cut = slice(i * LANES, (i + 1) * LANES)
        for src, dst in ((dlog, rows_a), (phase, rows_p)):
            row = jnp.concatenate([src[i * side + k : i * side + k + 1, :] for k in range(side)], axis=1)
            dst[:, cut] = jnp.broadcast_to(row, (8, LANES))

    for blk in range(n_blk):
        cut = slice(blk * lanes, (blk + 1) * lanes)
        a, p = rows_a[:, cut], rows_p[:, cut]
        mag, cos, sin = jnp.exp(a), jnp.cos(p), jnp.sin(p)
        lr, li = mag * cos, mag * sin
        inv = jnp.exp(-a)
        nr, ni = inv * cos, -inv * sin
        mod = a * a + p * p
        cr = ((lr - 1.0) * a + li * p) / mod
        ci = (li * a - (lr - 1.0) * p) / mod
        one, zero = jnp.ones_like(a), jnp.zeros_like(a)
        pr, pi, mr, mi = one, zero, cr, ci
        sr, si, qr, qi = lr, li, nr, ni
        row = lax.broadcasted_iota(jnp.int32, a.shape, 0)
        for bit in range(3):
            on = lax.rem(row // (1 << bit), 2) == 1
            ar, ai = cmul(pr, pi, sr, si)
            pr, pi = jnp.where(on, ar, pr), jnp.where(on, ai, pi)
            ar, ai = cmul(mr, mi, qr, qi)
            mr, mi = jnp.where(on, ar, mr), jnp.where(on, ai, mi)
            sr, si = cmul(sr, si, sr, si)
            qr, qi = cmul(qr, qi, qr, qi)
        t2r[0:8, cut], t2i[0:8, cut], t1r[0:8, cut], t1i[0:8, cut] = pr, pi, mr, mi
        done = 8
        while done < span:
            more = min(done, span - done)
            for off in range(0, more, 8):
                src, dst = slice(off, off + 8), slice(done + off, done + off + 8)
                t2r[dst, cut], t2i[dst, cut] = cmul(t2r[src, cut], t2i[src, cut], sr, si)
                t1r[dst, cut], t1i[dst, cut] = cmul(t1r[src, cut], t1i[src, cut], qr, qi)
            sr, si = cmul(sr, si, sr, si)
            qr, qi = cmul(qr, qi, qr, qi)
            done += more
        endr, endi = t2r[span - 1 : span, cut], t2i[span - 1 : span, cut]
        wholer, wholei = cmul(endr, endi, lr[0:1], li[0:1])
        allr, alli = cpow(wholer, wholei, n_chip)
        for k, value in enumerate((allr, alli, lr[0:1], li[0:1], wholer, wholei, endr, endi)):
            l_ref[blk, k : k + 1, :] = value

    loaded(3, 4)
    keep_b = (
        lax.broadcasted_iota(jnp.int32, (LANES, lanes), 0) // group
        == lax.broadcasted_iota(jnp.int32, (LANES, lanes), 1) // state
    )
    of_col = lax.broadcasted_iota(jnp.int32, (state, LANES), 1) // group
    a, p = dlog[...], phase[...]
    mag = jnp.exp(a)
    stepr, stepi = cpow(mag * jnp.cos(p), mag * jnp.sin(p), span)
    for blk in range(n_blk):
        ch = slice(blk * LANES, (blk + 1) * LANES)
        for part, in_ref in ((0, bre), (1, bim)):
            b = in_ref[ch, :]
            b = jnp.concatenate([b] * side, axis=1)
            wide = jnp.where(keep_b, jnp.concatenate([b] * (lanes // LANES), axis=1), 0.0)
            bs[blk, :, part * lanes : (part + 1) * lanes] = wide.astype(BF16)
        c_r, c_i = cre[ch, :], cim[ch, :]
        if n_chip > 1:
            spread = [
                jnp.concatenate(
                    [jnp.broadcast_to(s[g : g + 1], (group, state)) for g in range(blk * per, (blk + 1) * per)],
                    axis=0,
                )
                for s in (stepr, stepi)
            ]
        for c in range(n_chip):
            if c:
                c_r, c_i = cmul(c_r, c_i, *spread)
            turned = jnp.concatenate([c_r, -c_i], axis=1).T
            for part in range(2):
                piece = turned[part * state : (part + 1) * state]
                for g in range(per):
                    at = part * lanes + g * state
                    cs[blk, at : at + state, c * LANES : (c + 1) * LANES] = jnp.where(
                        of_col == g, piece, 0.0
                    ).astype(BF16)
    lower = (
        lax.broadcasted_iota(jnp.int32, (span, span), 0)
        >= lax.broadcasted_iota(jnp.int32, (span, span), 1)
    ).astype(BF16)

    def landed(ref, sem):
        remote(ref, ref, a_send.at[0], sem, {"tp": partner}).wait_recv()

    def gone(ref, sem):
        remote(ref, ref, sem, a_recv.at[0], {"tp": partner}).wait_send()

    def source(c, blk):
        return jnp.concatenate([urecv[2 * c + s, blk].astype(F32) for s in range(2)], axis=0)

    def drive(c, blk):
        cut = slice(blk * lanes, (blk + 1) * lanes)
        d = jnp.dot(source(c, blk).astype(BF16), bs[blk], preferred_element_type=F32)
        wr, wi = cmul(d[:, :lanes], d[:, lanes:], t1r[:, cut], t1i[:, cut])
        wbuf[blk][c, :, :lanes] = wr.astype(BF16)
        wbuf[blk][c, :, lanes:] = wi.astype(BF16)
        wsum[blk][c, 0:1, :] = jnp.sum(wr, axis=0, keepdims=True)
        wsum[blk][c, 1:2, :] = jnp.sum(wi, axis=0, keepdims=True)

    def seeds(blk):
        turn = l_ref[blk, 4:5], l_ref[blk, 5:6]
        held = [None]
        for c in range(n_chip):
            r, i = wsum[blk][c, 0:1], wsum[blk][c, 1:2]
            if c:
                r, i = r + held[c][0], i + held[c][1]
            held.append(cmul(r, i, *turn) if c < n_chip - 1 else cmul(r, i, l_ref[blk, 6:7], l_ref[blk, 7:8]))
        return held

    def end_copy(j, blk):
        return remote(e_send.at[blk], e_all.at[blk, sp], e_ssem.at[0], e_rsem.at[blk], {"sp": j})

    def scan(blk):
        cut = slice(blk * lanes, (blk + 1) * lanes)
        held = seeds(blk)
        for c in range(n_chip):
            s = jnp.dot(lower, wbuf[blk][c], preferred_element_type=F32)
            sr, si = s[:, :lanes], s[:, lanes:]
            if c:
                sr, si = sr + held[c][0], si + held[c][1]
            xr, xi = cmul(sr, si, t2r[:, cut], t2i[:, cut])
            at = slice(c * span, (c + 1) * span)
            xbuf[blk][at, :lanes] = xr.astype(BF16)
            xbuf[blk][at, lanes:] = xi.astype(BF16)

    def readout(blk):
        ch = slice(blk * LANES, (blk + 1) * LANES)
        y = jnp.dot(xbuf[blk][...], cs[blk, :, :LANES], preferred_element_type=F32)
        for c in range(n_chip):
            at = slice(c * span, (c + 1) * span)
            ylocal[blk][at] = y[at] + skip[:, ch] * source(c, blk)

    landed(urecv.at[partner], a_recv.at[0])
    for blk in range(n_blk):
        drive(chip, blk)

    def send_ends(blks, first, last):
        def go(j, c):
            for blk in blks:
                end_copy(j, blk).start()
            return c

        lax.fori_loop(first, last, go, 0)

    def finish(blk, y):
        for c in range(n_chip):
            at = slice(c * span, (c + 1) * span)
            v = ylocal[blk][at]
            if y is not None:
                v = v + y[:, c * LANES : (c + 1) * LANES]
            zbuf[tp, blk, at] = jax.nn.gelu(v).astype(BF16)
        for copy in z_copies(blk):
            copy.start()

    def z_slot(k, blk, late):
        return 1 + ((k - 1) * n_blk + blk) * 2 + late if k else 0

    def z_copies(blk):
        return [
            remote(
                zbuf.at[tp, blk], zbuf.at[tp, blk], z_send.at[0], z_recv.at[z_slot(k, blk, 0)],
                {"tp": lax.rem(tp + 2 * k, n_tp) if k else partner},
            )
            for k in list(range(1, n_chip)) + [0]
        ]

    def reach(i, old, new):
        count = new - old if pair == 1 else jnp.where(sp_b == 0, new - old, (new - old) // pair)
        pl.when(count > 0)(lambda: pl.semaphore_wait(met.at[i], count))

    old = sp + 1
    for blk in range(n_blk + 2):
        if blk < n_blk:
            for k in range(1, n_chip):
                c = lax.rem(chip + k, n_chip)
                landed(urecv.at[pl.ds(2 * c, 2), blk], a_recv.at[1 + (k - 1) * n_blk + blk])
            for k in range(1, n_chip):
                drive(lax.rem(chip + k, n_chip), blk)
        if 1 <= blk <= n_blk:
            scan(blk - 1)
        if 2 <= blk:
            readout(blk - 2)
        if blk < n_blk:
            er, ei = seeds(blk)[n_chip]
            e_send[blk] = jnp.concatenate([er, ei], axis=0).astype(BF16)
            new = jnp.minimum(sp + 1 + half, n_sp) if blk == 0 else n_sp
            if blk < 2:
                reach(blk, old, new)
            if blk:
                send_ends([blk], sp + 1, old)
            send_ends(range(blk + 1), old, new)
            old = new
        if 2 <= blk:
            pl.when(sp == 0)(functools.partial(finish, blk - 2, None))

    def after(blk):
        cut = slice(blk * lanes, (blk + 1) * lanes)
        lr, li = l_ref[blk, 0:1], l_ref[blk, 1:2]

        def join(j, held):
            e = e_all[blk, j].astype(F32)
            hr, hi = cmul(*held, lr, li)
            return hr + e[0:1], hi + e[1:2]

        for s in range(1, n_sp):
            pl.when(sp == s)(functools.partial(landed, e_all.at[blk, pl.ds(0, s)], e_rsem.at[blk]))
        nil = jnp.zeros((1, lanes), F32)
        hr, hi = lax.fori_loop(0, sp, join, (nil, nil))
        hr, hi = cmul(hr, hi, l_ref[blk, 2:3], l_ref[blk, 3:4])
        xr, xi = cmul(hr, hi, t2r[:, cut], t2i[:, cut])
        x = jnp.concatenate([xr.astype(BF16), xi.astype(BF16)], axis=1)
        finish(blk, jnp.dot(x, cs[blk], preferred_element_type=F32))


    @pl.when(sp > 0)
    def _():
        for blk in range(n_blk):
            after(blk)

    loaded(5)

    def project(items):
        at = [pl.ds(pl.multiple_of(j * width + blk * LANES, LANES), LANES) for j, blk in items]
        z = jnp.concatenate([zbuf[j, blk] for j, blk in items], axis=1)
        return [
            jnp.dot(z, jnp.concatenate([w[a, :] for a in at], axis=0), preferred_element_type=F32)
            for w in (wv, wg)
        ]

    v, g = project([(tp, blk) for blk in range(n_blk)])
    acc_v[...], acc_g[...] = v, g
    landed(zbuf.at[partner], z_recv.at[0])
    v, g = project([(partner, blk) for blk in range(n_blk)])
    acc_v[...] += v
    acc_g[...] += g
    late = []
    ripe = []

    def flush():
        v, g = project(ripe)
        ripe.clear()
        acc_v[...] += v
        acc_g[...] += g

    for blk in range(n_blk):
        for k in range(1, n_chip):
            j = lax.rem(tp + n_tp - 2 * k, n_tp)
            landed(zbuf.at[j, blk], z_recv.at[z_slot(k, blk, 0)])
            remote(
                zbuf.at[j, blk], zbuf.at[j, blk], f_send.at[0], z_recv.at[z_slot(k, blk, 1)], {"tp": partner}
            ).start()
            ripe.append((j, blk))
            if len(ripe) == 2:
                flush()
            late.append((lax.rem(partner + n_tp - 2 * k, n_tp), blk, k))
            if len(late) > 1:
                item = late.pop(0)
                landed(zbuf.at[item[0], item[1]], z_recv.at[z_slot(item[2], item[1], 1)])
                ripe.append(item[:2])
                if len(ripe) == 2:
                    flush()
    if ripe:
        flush()
    for item in late:
        landed(zbuf.at[item[0], item[1]], z_recv.at[z_slot(item[2], item[1], 1)])
    if late:
        v, g = project([item[:2] for item in late])
        v, g = acc_v[...] + v, acc_g[...] + g
    else:
        v, g = acc_v[...], acc_g[...]

    gated = v * (0.5 + 0.5 * jnp.tanh(0.5 * g))
    acc_v[...] = gated
    square = gated * gated
    part = square[:, :LANES]
    for blk in range(1, n_blk):
        part = part + square[:, blk * LANES : (blk + 1) * LANES]
    sums = jnp.sum(part, axis=1, keepdims=True)
    lane = lax.broadcasted_iota(jnp.int32, (8, LANES), 1)
    total = jnp.zeros((8, LANES), F32)
    for k in range(rows // 8):
        total = jnp.where(lane == k, sums[8 * k : 8 * k + 8], total)
    sq_all[tp] = total
    for k in range(1, n_tp):
        j = lax.rem(tp + n_tp - k, n_tp)
        remote(sq_all.at[tp], sq_all.at[tp], q_sem.at[0], q_sem.at[1], {"tp": j}).start()
    gone(nsend.at[pl.ds(0, n_tp - 1)], a_send.at[0])
    gone(zbuf.at[pl.ds(0, n_chip)], z_send.at[0])
    if n_chip > 1:
        gone(zbuf.at[pl.ds(0, n_chip - 1)], f_send.at[0])
    for s in range(n_sp - 1):
        pl.when(sp == s)(functools.partial(gone, e_all.at[:, pl.ds(0, n_sp - 1 - s)], e_ssem.at[0]))
    landed(sq_all.at[pl.ds(0, n_tp - 1)], q_sem.at[1])
    for k in range(1, n_tp):
        total = total + sq_all[lax.rem(tp + k, n_tp)]
    scale = lax.rsqrt(total / d_model + NORM_EPS)
    for k in range(0, rows // 8, 2):
        two = range(k, min(k + 2, rows // 8))
        column = jnp.concatenate([scale[:, i : i + 1] for i in two], axis=0)
        at = slice(8 * k, 8 * k + 8 * len(two))
        out[at, :] = (acc_v[at, :] * column * nout[...]).astype(BF16)

    gone(sq_all.at[pl.ds(0, n_tp - 1)], q_sem.at[0])


def solution(mesh):
    n_sp, n_tp = mesh.shape["sp"], mesh.shape["tp"]

    def on_device(
        tokens, norm_in, decay_log, phase, b_real, b_imag, c_real, c_imag, skip_gain, w_value, w_gate, norm_out
    ):
        mine, d_model = tokens.shape
        rows = mine * n_tp
        groups, state, group = b_real.shape
        width = groups * group
        n_blk = width // LANES
        lanes = LANES // group * state
        entries = groups * state
        n_chip = n_tp // 2
        span = 2 * mine
        vmem = pl.BlockSpec(memory_space=pltpu.VMEM)
        hbm = pl.BlockSpec(memory_space=pl.ANY)
        dma = pltpu.SemaphoreType.DMA
        return pl.pallas_call(
            functools.partial(layer, n_sp, n_tp, state, group),
            out_shape=pltpu.VMEM((rows, width), BF16),
            in_specs=[hbm] * 12,
            out_specs=vmem,
            scratch_shapes=[
                pltpu.VMEM((n_tp, n_blk, mine, LANES), BF16),
                pltpu.VMEM((n_tp, n_blk, mine, LANES), BF16),
                pltpu.VMEM((8, entries), F32),
                pltpu.VMEM((8, entries), F32),
                pltpu.VMEM((span, entries), F32),
                pltpu.VMEM((span, entries), F32),
                pltpu.VMEM((span, entries), F32),
                pltpu.VMEM((span, entries), F32),
                pltpu.VMEM((n_blk, LANES, 2 * lanes), BF16),
                pltpu.VMEM((n_blk, 2 * lanes, n_chip * LANES), BF16),
                [pltpu.VMEM((n_chip, span, 2 * lanes), BF16)] * n_blk,
                [pltpu.VMEM((rows, 2 * lanes), BF16)] * n_blk,
                [pltpu.VMEM((n_chip, 2, lanes), F32)] * n_blk,
                [pltpu.VMEM((rows, LANES), F32)] * n_blk,
                pltpu.VMEM((n_blk, 2, lanes), BF16),
                pltpu.VMEM((n_blk, n_sp, 2, lanes), BF16),
                pltpu.VMEM((n_blk, 8, lanes), F32),
                pltpu.VMEM((n_tp, n_blk, rows, LANES), BF16),
                pltpu.VMEM((2,) + w_value.shape, BF16),
                pltpu.VMEM((rows, width), F32),
                pltpu.VMEM((rows, width), F32),
                pltpu.VMEM((n_tp, 8, LANES), F32),
                pltpu.VMEM((4, width, state), F32),
                pltpu.VMEM((mine, d_model), BF16),
                pltpu.VMEM((1, d_model), F32),
                pltpu.VMEM((2, groups, state), F32),
                pltpu.VMEM((2, 1, width), F32),
                dma((6,)),
                dma((1,)),
                dma((1 + (n_chip - 1) * n_blk,)),
                dma((1,)),
                dma((n_blk,)),
                dma((1,)),
                dma((1 + (n_chip - 1) * n_blk * 2,)),
                dma((1,)),
                dma((2,)),
                pltpu.SemaphoreType.REGULAR((3,)),
            ],
            compiler_params=pltpu.CompilerParams(collective_id=0, has_side_effects=True),
        )(
            tokens,
            norm_in.reshape(1, -1),
            decay_log,
            phase,
            b_real.transpose(0, 2, 1).reshape(width, state),
            b_imag.transpose(0, 2, 1).reshape(width, state),
            c_real.reshape(width, state),
            c_imag.reshape(width, state),
            skip_gain.reshape(1, -1),
            w_value,
            w_gate,
            norm_out.reshape(1, -1),
        )

    placed = (
        P(("sp", "tp"), None),
        P(),
        P("tp", None),
        P("tp", None),
        P("tp", None, None),
        P("tp", None, None),
        P("tp", None, None),
        P("tp", None, None),
        P("tp"),
        P(None, "tp"),
        P(None, "tp"),
        P("tp"),
    )
    return jax.shard_map(
        on_device, mesh=mesh, in_specs=placed, out_specs=P("sp", "tp"), check_vma=False
    )
```

```python
import functools

import jax
import jax.numpy as jnp
from jax import lax
from jax.experimental import pallas as pl
from jax.experimental.pallas import tpu as pltpu
from jax.sharding import PartitionSpec as P

NORM_EPS = 1e-06
LANES = 128
F32 = jnp.float32
BF16 = jnp.bfloat16


def cmul(ar, ai, br, bi):
    return ar * br - ai * bi, ar * bi + ai * br


def cpow(r, i, n):
    outr, outi = None, None
    while n:
        if n % 2:
            outr, outi = (r, i) if outr is None else cmul(outr, outi, r, i)
        n //= 2
        if n:
            r, i = cmul(r, i, r, i)
    return outr, outi


def remote(src, dst, send, recv, target):
    return pltpu.make_async_remote_copy(
        src_ref=src,
        dst_ref=dst,
        send_sem=send,
        recv_sem=recv,
        device_id=target,
        device_id_type=pl.DeviceIdType.MESH,
    )


def layer(
    n_sp, n_tp, state, group,
    tok_h, nin_h, dlog_h, phase_h, bre_h, bim_h, cre_h, cim_h, skip_h, wv_h, wg_h, nout_h,
    out,
    nsend, urecv, rows_a, rows_p, t1r, t1i, t2r, t2i, bs, cs, wbuf, xbuf, wsum, ylocal,
    e_send, e_all, l_ref, zst, zbuf, w, acc, both, swapped, sq_all,
    bc, tok, nin, ap, sn,
    load_sem, a_send, a_recv, e_ssem, e_rsem, z_send, z_recv, w_sem, q_sem, met,
):
    sp, tp = lax.axis_index("sp"), lax.axis_index("tp")
    mine, d_model = tok.shape
    rows, width = out.shape
    half_rows = rows // 2
    n_blk = width // LANES
    per = LANES // group
    lanes = per * state
    core = lax.rem(tp, 2)
    chip = tp // 2
    partner = tp + 1 - 2 * core
    n_chip = n_tp // 2
    span = 2 * mine
    pair = 2 if n_sp % 2 == 0 else 1
    sp_b = lax.rem(sp, pair)

    def load(i, *pairs):
        return [pltpu.make_async_copy(src, dst, load_sem.at[i]) for src, dst in pairs]

    loads = [
        load(0, (tok_h, tok)),
        load(1, (nin_h, nin)),
        load(2, (dlog_h, ap.at[0]), (phase_h, ap.at[1])),
        load(3, *((src, bc.at[i]) for i, src in enumerate((bre_h, bim_h, cre_h, cim_h)))),
        load(4, (skip_h, sn.at[0]), (nout_h, sn.at[1])),
        load(5, (wv_h, w.at[core, 0]), (wg_h, w.at[core, 1])),
    ]

    def start(*which):
        for i in which:
            for copy in loads[i]:
                copy.start()

    def loaded(*which):
        for i in which:
            dst = (tok, nin, ap, bc, sn, w.at[core])[i]
            pltpu.make_async_copy(dst, dst, load_sem.at[i]).wait()

    start(0, 1, 2)

    barrier = pltpu.get_barrier_semaphore()

    def tell(sem, axis):
        def go(j, c):
            pl.semaphore_signal(sem, inc=1, device_id={axis: j}, device_id_type=pl.DeviceIdType.MESH)
            return c

        return go

    def above(go):
        for b in range(pair):
            first = sp // pair + jnp.where(b > sp_b, 0, 1)
            go_b = lambda a, c, b=b: go(a * pair + b, c)
            lax.fori_loop(jnp.where(b >= sp_b, first, n_sp // pair), n_sp // pair, go_b, 0)

    def below(go):
        for b in range(pair):
            last = sp // pair + jnp.where(b < sp_b, 1, 0)
            lax.fori_loop(0, jnp.where(b <= sp_b, last, 0), lambda a, c, b=b: go(a * pair + b, c), 0)

    lax.fori_loop(tp + 1, n_tp, tell(barrier, "tp"), 0)
    above(tell(barrier, "sp"))
    start(3, 4)
    pl.when(tp + sp > 0)(lambda: pl.semaphore_wait(barrier, tp + (sp // pair + 1) * (sp_b + 1) - 1))
    half = (n_sp // 2 + pair - 1) // pair * pair
    below(lambda j, c: tell(met.at[jnp.where(sp - j > half, 1, 0)], "sp")(j, c))
    lax.fori_loop(0, tp, tell(met.at[2], "tp"), 0)
    loaded(0, 1)

    xf = tok[...].astype(F32)
    scale = lax.rsqrt(jnp.sum(xf * xf, axis=1, keepdims=True) / d_model + NORM_EPS)
    normed = (xf * scale * nin[...]).astype(BF16)
    for j in range(n_tp):
        for blk in range(n_blk):
            at = j * width + blk * LANES
            nsend[j, blk] = normed[:, at : at + LANES]

    pl.when(tp < n_tp - 1)(lambda: pl.semaphore_wait(met.at[2], n_tp - 1 - tp))


    def scatter(j, blk, at):
        remote(nsend.at[j, blk], urecv.at[tp, blk], a_send.at[0], a_recv.at[at], {"tp": j}).start()

    for blk in range(n_blk):
        for k in range(1, n_chip):
            other = lax.rem(chip + n_chip - k, n_chip)
            for j in (2 * other + core, 2 * other + 1 - core):
                scatter(j, blk, 1 + (k - 1) * n_blk + blk)
        if blk == 0:
            for b in range(n_blk):
                scatter(partner, b, 0)
    start(5)
    for i, src in enumerate((wv_h, wg_h)):
        remote(src, w.at[core, i], w_sem.at[0], w_sem.at[1], {"tp": partner}).start()
    urecv[tp] = nsend[tp]

    loaded(2)
    dlog, phase, skip, nout = ap.at[0], ap.at[1], sn.at[0], sn.at[1]
    bre, bim, cre, cim = (bc.at[i] for i in range(4))
    side = LANES // state
    for i in range(width // group // side):
        cut = slice(i * LANES, (i + 1) * LANES)
        for src, dst in ((dlog, rows_a), (phase, rows_p)):
            row = jnp.concatenate([src[i * side + k : i * side + k + 1, :] for k in range(side)], axis=1)
            dst[:, cut] = jnp.broadcast_to(row, (8, LANES))

    for blk in range(n_blk):
        cut = slice(blk * lanes, (blk + 1) * lanes)
        a, p = rows_a[:, cut], rows_p[:, cut]
        mag, cos, sin = jnp.exp(a), jnp.cos(p), jnp.sin(p)
        lr, li = mag * cos, mag * sin
        inv = jnp.exp(-a)
        nr, ni = inv * cos, -inv * sin
        mod = a * a + p * p
        cr = ((lr - 1.0) * a + li * p) / mod
        ci = (li * a - (lr - 1.0) * p) / mod
        one, zero = jnp.ones_like(a), jnp.zeros_like(a)
        pr, pi, mr, mi = one, zero, cr, ci
        sr, si, qr, qi = lr, li, nr, ni
        row = lax.broadcasted_iota(jnp.int32, a.shape, 0)
        for bit in range(3):
            on = lax.rem(row // (1 << bit), 2) == 1
            ar, ai = cmul(pr, pi, sr, si)
            pr, pi = jnp.where(on, ar, pr), jnp.where(on, ai, pi)
            ar, ai = cmul(mr, mi, qr, qi)
            mr, mi = jnp.where(on, ar, mr), jnp.where(on, ai, mi)
            sr, si = cmul(sr, si, sr, si)
            qr, qi = cmul(qr, qi, qr, qi)
        t2r[0:8, cut], t2i[0:8, cut], t1r[0:8, cut], t1i[0:8, cut] = pr, pi, mr, mi
        done = 8
        while done < span:
            more = min(done, span - done)
            for off in range(0, more, 8):
                src, dst = slice(off, off + 8), slice(done + off, done + off + 8)
                t2r[dst, cut], t2i[dst, cut] = cmul(t2r[src, cut], t2i[src, cut], sr, si)
                t1r[dst, cut], t1i[dst, cut] = cmul(t1r[src, cut], t1i[src, cut], qr, qi)
            sr, si = cmul(sr, si, sr, si)
            qr, qi = cmul(qr, qi, qr, qi)
            done += more
        endr, endi = t2r[span - 1 : span, cut], t2i[span - 1 : span, cut]
        wholer, wholei = cmul(endr, endi, lr[0:1], li[0:1])
        allr, alli = cpow(wholer, wholei, n_chip)
        for k, value in enumerate((allr, alli, lr[0:1], li[0:1], wholer, wholei, endr, endi)):
            l_ref[blk, k : k + 1, :] = value

    loaded(3, 4)
    keep_b = (
        lax.broadcasted_iota(jnp.int32, (LANES, lanes), 0) // group
        == lax.broadcasted_iota(jnp.int32, (LANES, lanes), 1) // state
    )
    of_col = lax.broadcasted_iota(jnp.int32, (state, LANES), 1) // group
    a, p = dlog[...], phase[...]
    mag = jnp.exp(a)
    stepr, stepi = cpow(mag * jnp.cos(p), mag * jnp.sin(p), span)
    for blk in range(n_blk):
        ch = slice(blk * LANES, (blk + 1) * LANES)
        for part, in_ref in ((0, bre), (1, bim)):
            b = in_ref[ch, :]
            b = jnp.concatenate([b] * side, axis=1)
            wide = jnp.where(keep_b, jnp.concatenate([b] * (lanes // LANES), axis=1), 0.0)
            bs[blk, :, part * lanes : (part + 1) * lanes] = wide.astype(BF16)
        c_r, c_i = cre[ch, :], cim[ch, :]
        if n_chip > 1:
            spread = [
                jnp.concatenate(
                    [jnp.broadcast_to(s[g : g + 1], (group, state)) for g in range(blk * per, (blk + 1) * per)],
                    axis=0,
                )
                for s in (stepr, stepi)
            ]
        for c in range(n_chip):
            if c:
                c_r, c_i = cmul(c_r, c_i, *spread)
            turned = jnp.concatenate([c_r, -c_i], axis=1).T
            for part in range(2):
                piece = turned[part * state : (part + 1) * state]
                for g in range(per):
                    at = part * lanes + g * state
                    cs[blk, at : at + state, c * LANES : (c + 1) * LANES] = jnp.where(
                        of_col == g, piece, 0.0
                    ).astype(BF16)
    lower = (
        lax.broadcasted_iota(jnp.int32, (span, span), 0)
        >= lax.broadcasted_iota(jnp.int32, (span, span), 1)
    ).astype(BF16)

    def landed(ref, sem):
        remote(ref, ref, a_send.at[0], sem, {"tp": partner}).wait_recv()

    def gone(ref, sem):
        remote(ref, ref, sem, a_recv.at[0], {"tp": partner}).wait_send()

    def source(c, blk):
        return jnp.concatenate([urecv[2 * c + s, blk].astype(F32) for s in range(2)], axis=0)

    def drive(c, blk):
        cut = slice(blk * lanes, (blk + 1) * lanes)
        d = jnp.dot(source(c, blk).astype(BF16), bs[blk], preferred_element_type=F32)
        wr, wi = cmul(d[:, :lanes], d[:, lanes:], t1r[:, cut], t1i[:, cut])
        wbuf[blk][c, :, :lanes] = wr.astype(BF16)
        wbuf[blk][c, :, lanes:] = wi.astype(BF16)
        wsum[blk][c, 0:1, :] = jnp.sum(wr, axis=0, keepdims=True)
        wsum[blk][c, 1:2, :] = jnp.sum(wi, axis=0, keepdims=True)

    def seeds(blk):
        turn = l_ref[blk, 4:5], l_ref[blk, 5:6]
        held = [None]
        for c in range(n_chip):
            r, i = wsum[blk][c, 0:1], wsum[blk][c, 1:2]
            if c:
                r, i = r + held[c][0], i + held[c][1]
            held.append(cmul(r, i, *turn) if c < n_chip - 1 else cmul(r, i, l_ref[blk, 6:7], l_ref[blk, 7:8]))
        return held

    def end_copy(j, blk):
        return remote(e_send.at[blk], e_all.at[blk, sp], e_ssem.at[0], e_rsem.at[blk], {"sp": j})

    def scan(blk):
        cut = slice(blk * lanes, (blk + 1) * lanes)
        held = seeds(blk)
        for c in range(n_chip):
            s = jnp.dot(lower, wbuf[blk][c], preferred_element_type=F32)
            sr, si = s[:, :lanes], s[:, lanes:]
            if c:
                sr, si = sr + held[c][0], si + held[c][1]
            xr, xi = cmul(sr, si, t2r[:, cut], t2i[:, cut])
            at = slice(c * span, (c + 1) * span)
            xbuf[blk][at, :lanes] = xr.astype(BF16)
            xbuf[blk][at, lanes:] = xi.astype(BF16)

    def readout(blk):
        ch = slice(blk * LANES, (blk + 1) * LANES)
        y = jnp.dot(xbuf[blk][...], cs[blk, :, :LANES], preferred_element_type=F32)
        for c in range(n_chip):
            at = slice(c * span, (c + 1) * span)
            ylocal[blk][at] = y[at] + skip[:, ch] * source(c, blk)

    landed(urecv.at[partner], a_recv.at[0])
    for blk in range(n_blk):
        drive(chip, blk)

    def send_ends(blks, first, last):
        def go(j, c):
            for blk in blks:
                end_copy(j, blk).start()
            return c

        lax.fori_loop(first, last, go, 0)

    def finish(blk, y):
        for c in range(n_chip):
            at = slice(c * span, (c + 1) * span)
            v = ylocal[blk][at]
            if y is not None:
                v = v + y[:, c * LANES : (c + 1) * LANES]
            top = c * span // half_rows
            to = slice(c * span - top * half_rows, (c + 1) * span - top * half_rows)
            zst[top, blk, to] = jax.nn.gelu(v).astype(BF16)
        for copy in z_copies(blk):
            copy.start()

    def z_copies(blk):
        targets = []
        for k in range(1, n_chip):
            other = 2 * lax.rem(chip + k, n_chip)
            targets += [(h, other + h, 1 + (k - 1) * n_blk + blk) for h in (core, 1 - core)]
        targets.append((1 - core, partner, 0))
        return [
            remote(zst.at[h, blk], zbuf.at[tp, blk], z_send.at[0], z_recv.at[slot], {"tp": j})
            for h, j, slot in targets
        ]

    def reach(i, old, new):
        count = new - old if pair == 1 else jnp.where(sp_b == 0, new - old, (new - old) // pair)
        pl.when(count > 0)(lambda: pl.semaphore_wait(met.at[i], count))

    old = sp + 1
    for blk in range(n_blk + 2):
        if blk < n_blk:
            for k in range(1, n_chip):
                c = lax.rem(chip + k, n_chip)
                landed(urecv.at[pl.ds(2 * c, 2), blk], a_recv.at[1 + (k - 1) * n_blk + blk])
            for k in range(1, n_chip):
                drive(lax.rem(chip + k, n_chip), blk)
        if 1 <= blk <= n_blk:
            scan(blk - 1)
        if 2 <= blk:
            readout(blk - 2)
        if blk < n_blk:
            er, ei = seeds(blk)[n_chip]
            e_send[blk] = jnp.concatenate([er, ei], axis=0).astype(BF16)
            new = jnp.minimum(sp + 1 + half, n_sp) if blk == 0 else n_sp
            if blk < 2:
                reach(blk, old, new)
            if blk:
                send_ends([blk], sp + 1, old)
            send_ends(range(blk + 1), old, new)
            old = new
        if 2 <= blk:
            pl.when(sp == 0)(functools.partial(finish, blk - 2, None))

    def after(blk):
        cut = slice(blk * lanes, (blk + 1) * lanes)
        lr, li = l_ref[blk, 0:1], l_ref[blk, 1:2]

        def join(j, held):
            e = e_all[blk, j].astype(F32)
            hr, hi = cmul(*held, lr, li)
            return hr + e[0:1], hi + e[1:2]

        for s in range(1, n_sp):
            pl.when(sp == s)(functools.partial(landed, e_all.at[blk, pl.ds(0, s)], e_rsem.at[blk]))
        nil = jnp.zeros((1, lanes), F32)
        hr, hi = lax.fori_loop(0, sp, join, (nil, nil))
        hr, hi = cmul(hr, hi, l_ref[blk, 2:3], l_ref[blk, 3:4])
        xr, xi = cmul(hr, hi, t2r[:, cut], t2i[:, cut])
        x = jnp.concatenate([xr.astype(BF16), xi.astype(BF16)], axis=1)
        finish(blk, jnp.dot(x, cs[blk], preferred_element_type=F32))


    @pl.when(sp > 0)
    def _():
        for blk in range(n_blk):
            after(blk)

    loaded(5)

    def project(ref, i, j, blks):
        at = pl.ds(pl.multiple_of(j * width + blks[0] * LANES, LANES), LANES * len(blks))
        z = jnp.concatenate([ref[i, blk] for blk in blks], axis=1)
        return z, at

    def products(*parts):
        z = jnp.concatenate([p[0] for p in parts], axis=1)
        return [
            [
                jnp.dot(
                    z, jnp.concatenate([w[q, i, p[1], :] for p in parts], axis=0), preferred_element_type=F32
                )
                for i in range(2)
            ]
            for q in range(2)
        ]

    def add(new):
        for q in range(2):
            for i in range(2):
                acc[q, i] += new[q][i]

    landed(w.at[1 - core], w_sem.at[1])
    every = range(n_blk)
    new = products(project(zst, core, tp, every))
    for q in range(2):
        for i in range(2):
            acc[q, i] = new[q][i]
    landed(zbuf.at[partner], z_recv.at[0])
    add(products(project(zbuf, partner, partner, every)))
    for blk in range(n_blk):
        for k in range(1, n_chip):
            c2 = 2 * lax.rem(chip + n_chip - k, n_chip)
            landed(zbuf.at[pl.ds(c2, 2), blk], z_recv.at[1 + (k - 1) * n_blk + blk])
            new = products(*(project(zbuf, c2 + h, c2 + h, [blk]) for h in range(2)))
            if blk < n_blk - 1 or k < n_chip - 1:
                add(new)
    part = None
    for q in range(2):
        v, g = (acc[q, i] + new[q][i] for i in range(2))
        gated = v * (0.5 + 0.5 * jnp.tanh(0.5 * g))
        both[q] = gated
        square = gated * gated
        for blk in range(n_blk):
            piece = square[:, blk * LANES : (blk + 1) * LANES]
            part = piece if part is None else part + piece
    remote(both.at[1 - core], swapped, q_sem.at[2], q_sem.at[3], {"tp": partner}).start()
    sums = jnp.sum(part, axis=1, keepdims=True)
    lane = lax.broadcasted_iota(jnp.int32, (8, LANES), 1)
    total = jnp.zeros((8, LANES), F32)
    for k in range(half_rows // 8):
        total = jnp.where(lane == k, sums[8 * k : 8 * k + 8], total)
    sq_all[tp] = total
    for k in range(1, n_tp):
        j = lax.rem(tp + n_tp - k, n_tp)
        remote(sq_all.at[tp], sq_all.at[tp], q_sem.at[0], q_sem.at[1], {"tp": j}).start()
    gone(nsend.at[pl.ds(0, n_tp - 1)], a_send.at[0])
    gone(zbuf.at[pl.ds(0, n_tp - 1)], z_send.at[0])
    gone(w.at[core], w_sem.at[0])
    for s in range(n_sp - 1):
        pl.when(sp == s)(functools.partial(gone, e_all.at[:, pl.ds(0, n_sp - 1 - s)], e_ssem.at[0]))
    landed(sq_all.at[pl.ds(0, n_tp - 1)], q_sem.at[1])
    landed(swapped, q_sem.at[3])
    for h in (core, 1 - core):
        total = sq_all[h]
        for c in range(1, n_chip):
            total = total + sq_all[2 * c + h]
        scale = lax.rsqrt(total / d_model + NORM_EPS)
        column = jnp.concatenate([scale[:, i : i + 1] for i in range(half_rows // 8)], axis=0)
        gated = both[core] if h is core else swapped[...]
        at = pl.ds(pl.multiple_of(h * half_rows, half_rows), half_rows)
        out[at, :] = (gated * column * nout[...]).astype(BF16)

    gone(sq_all.at[pl.ds(0, n_tp - 1)], q_sem.at[0])
    gone(swapped, q_sem.at[2])


def solution(mesh):
    n_sp, n_tp = mesh.shape["sp"], mesh.shape["tp"]

    def on_device(
        tokens, norm_in, decay_log, phase, b_real, b_imag, c_real, c_imag, skip_gain, w_value, w_gate, norm_out
    ):
        mine, d_model = tokens.shape
        rows = mine * n_tp
        groups, state, group = b_real.shape
        width = groups * group
        n_blk = width // LANES
        lanes = LANES // group * state
        entries = groups * state
        n_chip = n_tp // 2
        span = 2 * mine
        vmem = pl.BlockSpec(memory_space=pltpu.VMEM)
        hbm = pl.BlockSpec(memory_space=pl.ANY)
        dma = pltpu.SemaphoreType.DMA
        return pl.pallas_call(
            functools.partial(layer, n_sp, n_tp, state, group),
            out_shape=pltpu.VMEM((rows, width), BF16),
            in_specs=[hbm] * 12,
            out_specs=vmem,
            scratch_shapes=[
                pltpu.VMEM((n_tp, n_blk, mine, LANES), BF16),
                pltpu.VMEM((n_tp, n_blk, mine, LANES), BF16),
                pltpu.VMEM((8, entries), F32),
                pltpu.VMEM((8, entries), F32),
                pltpu.VMEM((span, entries), F32),
                pltpu.VMEM((span, entries), F32),
                pltpu.VMEM((span, entries), F32),
                pltpu.VMEM((span, entries), F32),
                pltpu.VMEM((n_blk, LANES, 2 * lanes), BF16),
                pltpu.VMEM((n_blk, 2 * lanes, n_chip * LANES), BF16),
                [pltpu.VMEM((n_chip, span, 2 * lanes), BF16)] * n_blk,
                [pltpu.VMEM((rows, 2 * lanes), BF16)] * n_blk,
                [pltpu.VMEM((n_chip, 2, lanes), F32)] * n_blk,
                [pltpu.VMEM((rows, LANES), F32)] * n_blk,
                pltpu.VMEM((n_blk, 2, lanes), BF16),
                pltpu.VMEM((n_blk, n_sp, 2, lanes), BF16),
                pltpu.VMEM((n_blk, 8, lanes), F32),
                pltpu.VMEM((2, n_blk, rows // 2, LANES), BF16),
                pltpu.VMEM((n_tp, n_blk, rows // 2, LANES), BF16),
                pltpu.VMEM((2, 2) + w_value.shape, BF16),
                pltpu.VMEM((2, 2, rows // 2, width), F32),
                pltpu.VMEM((2, rows // 2, width), F32),
                pltpu.VMEM((rows // 2, width), F32),
                pltpu.VMEM((n_tp, 8, LANES), F32),
                pltpu.VMEM((4, width, state), F32),
                pltpu.VMEM((mine, d_model), BF16),
                pltpu.VMEM((1, d_model), F32),
                pltpu.VMEM((2, groups, state), F32),
                pltpu.VMEM((2, 1, width), F32),
                dma((6,)),
                dma((1,)),
                dma((1 + (n_chip - 1) * n_blk,)),
                dma((1,)),
                dma((n_blk,)),
                dma((1,)),
                dma((1 + (n_chip - 1) * n_blk,)),
                dma((2,)),
                dma((4,)),
                pltpu.SemaphoreType.REGULAR((3,)),
            ],
            compiler_params=pltpu.CompilerParams(collective_id=0, has_side_effects=True),
        )(
            tokens,
            norm_in.reshape(1, -1),
            decay_log,
            phase,
            b_real.transpose(0, 2, 1).reshape(width, state),
            b_imag.transpose(0, 2, 1).reshape(width, state),
            c_real.reshape(width, state),
            c_imag.reshape(width, state),
            skip_gain.reshape(1, -1),
            w_value,
            w_gate,
            norm_out.reshape(1, -1),
        )

    placed = (
        P(("sp", "tp"), None),
        P(),
        P("tp", None),
        P("tp", None),
        P("tp", None, None),
        P("tp", None, None),
        P("tp", None, None),
        P("tp", None, None),
        P("tp"),
        P(None, "tp"),
        P(None, "tp"),
        P("tp"),
    )
    return jax.shard_map(
        on_device, mesh=mesh, in_specs=placed, out_specs=P("sp", "tp"), check_vma=False
    )
```

```python
import functools

import jax
import jax.numpy as jnp
from jax import lax
from jax.experimental import pallas as pl
from jax.experimental.pallas import tpu as pltpu
from jax.sharding import PartitionSpec as P

NORM_EPS = 1e-06
LANES = 128
F32 = jnp.float32
BF16 = jnp.bfloat16


def cmul(ar, ai, br, bi):
    return ar * br - ai * bi, ar * bi + ai * br


def cpow(r, i, n):
    outr, outi = None, None
    while n:
        if n % 2:
            outr, outi = (r, i) if outr is None else cmul(outr, outi, r, i)
        n //= 2
        if n:
            r, i = cmul(r, i, r, i)
    return outr, outi


def remote(src, dst, send, recv, target):
    return pltpu.make_async_remote_copy(
        src_ref=src,
        dst_ref=dst,
        send_sem=send,
        recv_sem=recv,
        device_id=target,
        device_id_type=pl.DeviceIdType.MESH,
    )


def layer(
    n_sp, n_tp, state, group,
    tok_h, nin_h, dlog_h, phase_h, bre_h, bim_h, cre_h, cim_h, skip_h, wv_h, wg_h, nout_h,
    out,
    nsend, urecv, rows_a, rows_p, t1r, t1i, t2r, t2i, bs, cs, wbuf, xbuf, wsum, ylocal,
    e_send, e_all, l_ref, zst, zbuf, w, acc, both, swapped, sq_all,
    bc, tok, nin, ap, sn,
    load_sem, a_send, a_recv, e_ssem, e_rsem, z_send, z_recv, w_sem, q_sem, met,
):
    sp, tp = lax.axis_index("sp"), lax.axis_index("tp")
    mine, d_model = tok.shape
    rows, width = out.shape
    half_rows = rows // 2
    n_blk = width // LANES
    per = LANES // group
    lanes = per * state
    core = lax.rem(tp, 2)
    chip = tp // 2
    partner = tp + 1 - 2 * core
    n_chip = n_tp // 2
    span = 2 * mine
    pair = 2 if n_sp % 2 == 0 else 1
    sp_b = lax.rem(sp, pair)

    parts = [pl.ds(i * width, width) for i in range(n_tp)]

    def load(i, *pairs):
        return [pltpu.make_async_copy(src, dst, load_sem.at[i]) for src, dst in pairs]

    loads = [
        load(0, *((tok_h.at[:, part], tok.at[:, part]) for part in parts)),
        load(1, (nin_h, nin)),
        load(2, (dlog_h, ap.at[0]), (phase_h, ap.at[1])),
        load(3, *((src, bc.at[i]) for i, src in enumerate((bre_h, bim_h, cre_h, cim_h)))),
        load(4, (skip_h, sn.at[0]), (nout_h, sn.at[1])),
        load(5, (wv_h, w.at[core, 0]), (wg_h, w.at[core, 1])),
    ]

    def start(*which):
        for i in which:
            for copy in loads[i]:
                copy.start()

    def loaded(*which):
        for i in which:
            dst = (tok, nin, ap, bc, sn, w.at[core])[i]
            pltpu.make_async_copy(dst, dst, load_sem.at[i]).wait()

    start(0, 1, 2)

    barrier = pltpu.get_barrier_semaphore()

    def tell(sem, axis):
        def go(j, c):
            pl.semaphore_signal(sem, inc=1, device_id={axis: j}, device_id_type=pl.DeviceIdType.MESH)
            return c

        return go

    def above(go):
        for b in range(pair):
            first = sp // pair + jnp.where(b > sp_b, 0, 1)
            go_b = lambda a, c, b=b: go(a * pair + b, c)
            lax.fori_loop(jnp.where(b >= sp_b, first, n_sp // pair), n_sp // pair, go_b, 0)

    def below(go):
        for b in range(pair):
            last = sp // pair + jnp.where(b < sp_b, 1, 0)
            lax.fori_loop(0, jnp.where(b <= sp_b, last, 0), lambda a, c, b=b: go(a * pair + b, c), 0)

    last = sp == n_sp - 1
    lax.fori_loop(jnp.where(last, tp + 1, 0), jnp.where(last, tp + 1, tp), tell(barrier, "tp"), 0)
    lax.fori_loop(tp + 1, n_tp, tell(barrier, "tp"), 0)
    above(tell(barrier, "sp"))
    start(3, 4)
    known = (sp // pair + 1) * (sp_b + 1) - 1 + jnp.where(last, tp, n_tp - 1)
    half = (n_sp // 2 + pair - 1) // pair * pair

    def enter():
        pl.when(known > 0)(lambda: pl.semaphore_wait(barrier, known))
        below(lambda j, c: tell(met.at[jnp.where(sp - j > half, 1, 0)], "sp")(j, c))
        lax.fori_loop(0, jnp.where(last, tp, 0), tell(met.at[2], "tp"), 0)

    pl.when(last)(enter)
    loaded(0, 1)

    xf = tok[...].astype(F32)
    scale = lax.rsqrt(jnp.sum(xf * xf, axis=1, keepdims=True) / d_model + NORM_EPS)
    normed = (xf * scale * nin[...]).astype(BF16)
    for j in range(n_tp):
        for blk in range(n_blk):
            at = j * width + blk * LANES
            nsend[j, blk] = normed[:, at : at + LANES]

    pl.when(jnp.logical_not(last))(enter)
    pl.when(last & (tp < n_tp - 1))(lambda: pl.semaphore_wait(met.at[2], n_tp - 1 - tp))


    def scatter(j, blk, at):
        remote(nsend.at[j, blk], urecv.at[tp, blk], a_send.at[0], a_recv.at[at], {"tp": j}).start()

    for blk in range(n_blk):
        for k in range(1, n_chip):
            other = lax.rem(chip + n_chip - k, n_chip)
            for j in (2 * other + core, 2 * other + 1 - core):
                scatter(j, blk, 1 + (k - 1) * n_blk + blk)
        if blk == 0:
            for b in range(n_blk):
                scatter(partner, b, 0)
    start(5)
    for i, src in enumerate((wv_h, wg_h)):
        remote(src, w.at[core, i], w_sem.at[0], w_sem.at[1], {"tp": partner}).start()
    urecv[tp] = nsend[tp]

    loaded(2)
    dlog, phase, skip, nout = ap.at[0], ap.at[1], sn.at[0], sn.at[1]
    bre, bim, cre, cim = (bc.at[i] for i in range(4))
    side = LANES // state
    for i in range(width // group // side):
        cut = slice(i * LANES, (i + 1) * LANES)
        for src, dst in ((dlog, rows_a), (phase, rows_p)):
            row = jnp.concatenate([src[i * side + k : i * side + k + 1, :] for k in range(side)], axis=1)
            dst[:, cut] = jnp.broadcast_to(row, (8, LANES))

    for blk in range(n_blk):
        cut = slice(blk * lanes, (blk + 1) * lanes)
        a, p = rows_a[:, cut], rows_p[:, cut]
        mag, cos, sin = jnp.exp(a), jnp.cos(p), jnp.sin(p)
        lr, li = mag * cos, mag * sin
        inv = jnp.exp(-a)
        nr, ni = inv * cos, -inv * sin
        mod = a * a + p * p
        cr = ((lr - 1.0) * a + li * p) / mod
        ci = (li * a - (lr - 1.0) * p) / mod
        one, zero = jnp.ones_like(a), jnp.zeros_like(a)
        pr, pi, mr, mi = one, zero, cr, ci
        sr, si, qr, qi = lr, li, nr, ni
        row = lax.broadcasted_iota(jnp.int32, a.shape, 0)
        for bit in range(3):
            on = lax.rem(row // (1 << bit), 2) == 1
            ar, ai = cmul(pr, pi, sr, si)
            pr, pi = jnp.where(on, ar, pr), jnp.where(on, ai, pi)
            ar, ai = cmul(mr, mi, qr, qi)
            mr, mi = jnp.where(on, ar, mr), jnp.where(on, ai, mi)
            sr, si = cmul(sr, si, sr, si)
            qr, qi = cmul(qr, qi, qr, qi)
        t2r[0:8, cut], t2i[0:8, cut], t1r[0:8, cut], t1i[0:8, cut] = pr, pi, mr, mi
        done = 8
        while done < span:
            more = min(done, span - done)
            for off in range(0, more, 8):
                src, dst = slice(off, off + 8), slice(done + off, done + off + 8)
                t2r[dst, cut], t2i[dst, cut] = cmul(t2r[src, cut], t2i[src, cut], sr, si)
                t1r[dst, cut], t1i[dst, cut] = cmul(t1r[src, cut], t1i[src, cut], qr, qi)
            sr, si = cmul(sr, si, sr, si)
            qr, qi = cmul(qr, qi, qr, qi)
            done += more
        endr, endi = t2r[span - 1 : span, cut], t2i[span - 1 : span, cut]
        wholer, wholei = cmul(endr, endi, lr[0:1], li[0:1])
        allr, alli = cpow(wholer, wholei, n_chip)
        for k, value in enumerate((allr, alli, lr[0:1], li[0:1], wholer, wholei, endr, endi)):
            l_ref[blk, k : k + 1, :] = value

    loaded(3, 4)
    keep_b = (
        lax.broadcasted_iota(jnp.int32, (LANES, lanes), 0) // group
        == lax.broadcasted_iota(jnp.int32, (LANES, lanes), 1) // state
    )
    of_col = lax.broadcasted_iota(jnp.int32, (state, LANES), 1) // group
    a, p = dlog[...], phase[...]
    mag = jnp.exp(a)
    stepr, stepi = cpow(mag * jnp.cos(p), mag * jnp.sin(p), span)
    for blk in range(n_blk):
        ch = slice(blk * LANES, (blk + 1) * LANES)
        for part, in_ref in ((0, bre), (1, bim)):
            b = in_ref[ch, :]
            b = jnp.concatenate([b] * side, axis=1)
            wide = jnp.where(keep_b, jnp.concatenate([b] * (lanes // LANES), axis=1), 0.0)
            bs[blk, :, part * lanes : (part + 1) * lanes] = wide.astype(BF16)
        c_r, c_i = cre[ch, :], cim[ch, :]
        if n_chip > 1:
            spread = [
                jnp.concatenate(
                    [jnp.broadcast_to(s[g : g + 1], (group, state)) for g in range(blk * per, (blk + 1) * per)],
                    axis=0,
                )
                for s in (stepr, stepi)
            ]
        for c in range(n_chip):
            if c:
                c_r, c_i = cmul(c_r, c_i, *spread)
            turned = jnp.concatenate([c_r, -c_i], axis=1).T
            for part in range(2):
                piece = turned[part * state : (part + 1) * state]
                for g in range(per):
                    at = part * lanes + g * state
                    cs[blk, at : at + state, c * LANES : (c + 1) * LANES] = jnp.where(
                        of_col == g, piece, 0.0
                    ).astype(BF16)
    lower = (
        lax.broadcasted_iota(jnp.int32, (span, span), 0)
        >= lax.broadcasted_iota(jnp.int32, (span, span), 1)
    ).astype(BF16)

    def landed(ref, sem):
        remote(ref, ref, a_send.at[0], sem, {"tp": partner}).wait_recv()

    def gone(ref, sem):
        remote(ref, ref, sem, a_recv.at[0], {"tp": partner}).wait_send()

    def source(c, blk):
        return jnp.concatenate([urecv[2 * c + s, blk].astype(F32) for s in range(2)], axis=0)

    def drive(c, blk):
        cut = slice(blk * lanes, (blk + 1) * lanes)
        d = jnp.dot(source(c, blk).astype(BF16), bs[blk], preferred_element_type=F32)
        wr, wi = cmul(d[:, :lanes], d[:, lanes:], t1r[:, cut], t1i[:, cut])
        wbuf[blk][c, :, :lanes] = wr.astype(BF16)
        wbuf[blk][c, :, lanes:] = wi.astype(BF16)
        wsum[blk][c, 0:1, :] = jnp.sum(wr, axis=0, keepdims=True)
        wsum[blk][c, 1:2, :] = jnp.sum(wi, axis=0, keepdims=True)

    def seeds(blk):
        turn = l_ref[blk, 4:5], l_ref[blk, 5:6]
        held = [None]
        for c in range(n_chip):
            r, i = wsum[blk][c, 0:1], wsum[blk][c, 1:2]
            if c:
                r, i = r + held[c][0], i + held[c][1]
            held.append(cmul(r, i, *turn) if c < n_chip - 1 else cmul(r, i, l_ref[blk, 6:7], l_ref[blk, 7:8]))
        return held

    def end_copy(j, blk):
        return remote(e_send.at[blk], e_all.at[blk, sp], e_ssem.at[0], e_rsem.at[blk], {"sp": j})

    def scan(blk):
        cut = slice(blk * lanes, (blk + 1) * lanes)
        held = seeds(blk)
        for c in range(n_chip):
            s = jnp.dot(lower, wbuf[blk][c], preferred_element_type=F32)
            sr, si = s[:, :lanes], s[:, lanes:]
            if c:
                sr, si = sr + held[c][0], si + held[c][1]
            xr, xi = cmul(sr, si, t2r[:, cut], t2i[:, cut])
            at = slice(c * span, (c + 1) * span)
            xbuf[blk][at, :lanes] = xr.astype(BF16)
            xbuf[blk][at, lanes:] = xi.astype(BF16)

    def readout(blk):
        ch = slice(blk * LANES, (blk + 1) * LANES)
        y = jnp.dot(xbuf[blk][...], cs[blk, :, :LANES], preferred_element_type=F32)
        for c in range(n_chip):
            at = slice(c * span, (c + 1) * span)
            ylocal[blk][at] = y[at] + skip[:, ch] * source(c, blk)

    landed(urecv.at[partner], a_recv.at[0])
    for blk in range(n_blk):
        drive(chip, blk)

    def send_ends(blks, first, last):
        def go(j, c):
            for blk in blks:
                end_copy(j, blk).start()
            return c

        lax.fori_loop(first, last, go, 0)

    def finish(blk, y):
        for c in range(n_chip):
            at = slice(c * span, (c + 1) * span)
            v = ylocal[blk][at]
            if y is not None:
                v = v + y[:, c * LANES : (c + 1) * LANES]
            top = c * span // half_rows
            to = slice(c * span - top * half_rows, (c + 1) * span - top * half_rows)
            zst[top, blk, to] = jax.nn.gelu(v).astype(BF16)
        for copy in z_copies(blk):
            copy.start()

    def z_copies(blk):
        targets = []
        for k in range(1, n_chip):
            other = 2 * lax.rem(chip + k, n_chip)
            targets += [(h, other + h, 1 + (k - 1) * n_blk + blk) for h in (core, 1 - core)]
        targets.append((1 - core, partner, 0))
        return [
            remote(zst.at[h, blk], zbuf.at[tp, blk], z_send.at[0], z_recv.at[slot], {"tp": j})
            for h, j, slot in targets
        ]

    def reach(i, old, new):
        count = new - old if pair == 1 else jnp.where(sp_b == 0, new - old, (new - old) // pair)
        pl.when(count > 0)(lambda: pl.semaphore_wait(met.at[i], count))

    old = sp + 1
    for blk in range(n_blk + 2):
        if blk < n_blk:
            for k in range(1, n_chip):
                c = lax.rem(chip + k, n_chip)
                landed(urecv.at[pl.ds(2 * c, 2), blk], a_recv.at[1 + (k - 1) * n_blk + blk])
            for k in range(1, n_chip):
                drive(lax.rem(chip + k, n_chip), blk)
        if 1 <= blk <= n_blk:
            scan(blk - 1)
        if 2 <= blk:
            readout(blk - 2)
        if blk < n_blk:
            er, ei = seeds(blk)[n_chip]
            e_send[blk] = jnp.concatenate([er, ei], axis=0).astype(BF16)
            new = jnp.minimum(sp + 1 + half, n_sp) if blk == 0 else n_sp
            if blk < 2:
                reach(blk, old, new)
            if blk:
                send_ends([blk], sp + 1, old)
            send_ends(range(blk + 1), old, new)
            old = new
        if blk == 0:

            @pl.when(sp == 0)
            def _():
                scan(0)
                readout(0)
                finish(0, None)

        if 3 <= blk:
            pl.when(sp == 0)(functools.partial(finish, blk - 2, None))

    def after(blk):
        cut = slice(blk * lanes, (blk + 1) * lanes)
        lr, li = l_ref[blk, 0:1], l_ref[blk, 1:2]

        def join(j, held):
            e = e_all[blk, j].astype(F32)
            hr, hi = cmul(*held, lr, li)
            return hr + e[0:1], hi + e[1:2]

        for s in range(1, n_sp):
            pl.when(sp == s)(functools.partial(landed, e_all.at[blk, pl.ds(0, s)], e_rsem.at[blk]))
        nil = jnp.zeros((1, lanes), F32)
        hr, hi = lax.fori_loop(0, sp, join, (nil, nil))
        hr, hi = cmul(hr, hi, l_ref[blk, 2:3], l_ref[blk, 3:4])
        xr, xi = cmul(hr, hi, t2r[:, cut], t2i[:, cut])
        x = jnp.concatenate([xr.astype(BF16), xi.astype(BF16)], axis=1)
        finish(blk, jnp.dot(x, cs[blk], preferred_element_type=F32))


    @pl.when(sp > 0)
    def _():
        for blk in range(n_blk):
            after(blk)

    loaded(5)

    def project(ref, i, j, blks):
        at = pl.ds(pl.multiple_of(j * width + blks[0] * LANES, LANES), LANES * len(blks))
        z = jnp.concatenate([ref[i, blk] for blk in blks], axis=1)
        return z, at

    def products(*parts):
        z = jnp.concatenate([p[0] for p in parts], axis=1)
        return [
            [
                jnp.dot(
                    z, jnp.concatenate([w[q, i, p[1], :] for p in parts], axis=0), preferred_element_type=F32
                )
                for i in range(2)
            ]
            for q in range(2)
        ]

    def add(new):
        for q in range(2):
            for i in range(2):
                acc[q, i] += new[q][i]

    landed(w.at[1 - core], w_sem.at[1])
    every = range(n_blk)
    new = products(project(zst, core, tp, every))
    for q in range(2):
        for i in range(2):
            acc[q, i] = new[q][i]
    landed(zbuf.at[partner], z_recv.at[0])
    add(products(project(zbuf, partner, partner, every)))
    for blk in range(n_blk):
        for k in range(1, n_chip):
            c2 = 2 * lax.rem(chip + n_chip - k, n_chip)
            landed(zbuf.at[pl.ds(c2, 2), blk], z_recv.at[1 + (k - 1) * n_blk + blk])
            new = products(*(project(zbuf, c2 + h, c2 + h, [blk]) for h in range(2)))
            if blk < n_blk - 1 or k < n_chip - 1:
                add(new)
    part = None
    for q in range(2):
        v, g = (acc[q, i] + new[q][i] for i in range(2))
        gated = v * (0.5 + 0.5 * jnp.tanh(0.5 * g))
        both[q] = gated
        square = gated * gated
        for blk in range(n_blk):
            piece = square[:, blk * LANES : (blk + 1) * LANES]
            part = piece if part is None else part + piece
    remote(both.at[1 - core], swapped, q_sem.at[2], q_sem.at[3], {"tp": partner}).start()
    sums = jnp.sum(part, axis=1, keepdims=True)
    lane = lax.broadcasted_iota(jnp.int32, (8, LANES), 1)
    total = jnp.zeros((8, LANES), F32)
    for k in range(half_rows // 8):
        total = jnp.where(lane == k, sums[8 * k : 8 * k + 8], total)
    sq_all[tp] = total
    for k in range(1, n_tp):
        j = lax.rem(tp + n_tp - k, n_tp)
        remote(sq_all.at[tp], sq_all.at[tp], q_sem.at[0], q_sem.at[1], {"tp": j}).start()
    gone(nsend.at[pl.ds(0, n_tp - 1)], a_send.at[0])
    gone(zbuf.at[pl.ds(0, n_tp - 1)], z_send.at[0])
    gone(w.at[core], w_sem.at[0])
    for s in range(n_sp - 1):
        pl.when(sp == s)(functools.partial(gone, e_all.at[:, pl.ds(0, n_sp - 1 - s)], e_ssem.at[0]))
    both[core] = both[core] * nout[...]
    landed(swapped, q_sem.at[3])
    swapped[...] = swapped[...] * nout[...]
    landed(sq_all.at[pl.ds(0, n_tp - 1)], q_sem.at[1])
    for h in (core, 1 - core):
        total = sq_all[h]
        for c in range(1, n_chip):
            total = total + sq_all[2 * c + h]
        scale = lax.rsqrt(total / d_model + NORM_EPS)
        column = jnp.concatenate([scale[:, i : i + 1] for i in range(half_rows // 8)], axis=0)
        gated = both[core] if h is core else swapped[...]
        at = pl.ds(pl.multiple_of(h * half_rows, half_rows), half_rows)
        out[at, :] = (gated * column).astype(BF16)

    gone(sq_all.at[pl.ds(0, n_tp - 1)], q_sem.at[0])
    gone(swapped, q_sem.at[2])


def solution(mesh):
    n_sp, n_tp = mesh.shape["sp"], mesh.shape["tp"]

    def on_device(
        tokens, norm_in, decay_log, phase, b_real, b_imag, c_real, c_imag, skip_gain, w_value, w_gate, norm_out
    ):
        mine, d_model = tokens.shape
        rows = mine * n_tp
        groups, state, group = b_real.shape
        width = groups * group
        n_blk = width // LANES
        lanes = LANES // group * state
        entries = groups * state
        n_chip = n_tp // 2
        span = 2 * mine
        vmem = pl.BlockSpec(memory_space=pltpu.VMEM)
        hbm = pl.BlockSpec(memory_space=pl.ANY)
        dma = pltpu.SemaphoreType.DMA
        return pl.pallas_call(
            functools.partial(layer, n_sp, n_tp, state, group),
            out_shape=pltpu.VMEM((rows, width), BF16),
            in_specs=[hbm] * 12,
            out_specs=vmem,
            scratch_shapes=[
                pltpu.VMEM((n_tp, n_blk, mine, LANES), BF16),
                pltpu.VMEM((n_tp, n_blk, mine, LANES), BF16),
                pltpu.VMEM((8, entries), F32),
                pltpu.VMEM((8, entries), F32),
                pltpu.VMEM((span, entries), F32),
                pltpu.VMEM((span, entries), F32),
                pltpu.VMEM((span, entries), F32),
                pltpu.VMEM((span, entries), F32),
                pltpu.VMEM((n_blk, LANES, 2 * lanes), BF16),
                pltpu.VMEM((n_blk, 2 * lanes, n_chip * LANES), BF16),
                [pltpu.VMEM((n_chip, span, 2 * lanes), BF16)] * n_blk,
                [pltpu.VMEM((rows, 2 * lanes), BF16)] * n_blk,
                [pltpu.VMEM((n_chip, 2, lanes), F32)] * n_blk,
                [pltpu.VMEM((rows, LANES), F32)] * n_blk,
                pltpu.VMEM((n_blk, 2, lanes), BF16),
                pltpu.VMEM((n_blk, n_sp, 2, lanes), BF16),
                pltpu.VMEM((n_blk, 8, lanes), F32),
                pltpu.VMEM((2, n_blk, rows // 2, LANES), BF16),
                pltpu.VMEM((n_tp, n_blk, rows // 2, LANES), BF16),
                pltpu.VMEM((2, 2) + w_value.shape, BF16),
                pltpu.VMEM((2, 2, rows // 2, width), F32),
                pltpu.VMEM((2, rows // 2, width), F32),
                pltpu.VMEM((rows // 2, width), F32),
                pltpu.VMEM((n_tp, 8, LANES), F32),
                pltpu.VMEM((4, width, state), F32),
                pltpu.VMEM((mine, d_model), BF16),
                pltpu.VMEM((1, d_model), F32),
                pltpu.VMEM((2, groups, state), F32),
                pltpu.VMEM((2, 1, width), F32),
                dma((6,)),
                dma((1,)),
                dma((1 + (n_chip - 1) * n_blk,)),
                dma((1,)),
                dma((n_blk,)),
                dma((1,)),
                dma((1 + (n_chip - 1) * n_blk,)),
                dma((2,)),
                dma((4,)),
                pltpu.SemaphoreType.REGULAR((3,)),
            ],
            compiler_params=pltpu.CompilerParams(collective_id=0, has_side_effects=True),
        )(
            tokens,
            norm_in.reshape(1, -1),
            decay_log,
            phase,
            b_real.transpose(0, 2, 1).reshape(width, state),
            b_imag.transpose(0, 2, 1).reshape(width, state),
            c_real.reshape(width, state),
            c_imag.reshape(width, state),
            skip_gain.reshape(1, -1),
            w_value,
            w_gate,
            norm_out.reshape(1, -1),
        )

    placed = (
        P(("sp", "tp"), None),
        P(),
        P("tp", None),
        P("tp", None),
        P("tp", None, None),
        P("tp", None, None),
        P("tp", None, None),
        P("tp", None, None),
        P("tp"),
        P(None, "tp"),
        P(None, "tp"),
        P("tp"),
    )
    return jax.shard_map(
        on_device, mesh=mesh, in_specs=placed, out_specs=P("sp", "tp"), check_vma=False
    )
```

```python
import functools

import jax
import jax.numpy as jnp
from jax import lax
from jax.experimental import pallas as pl
from jax.experimental.pallas import tpu as pltpu
from jax.sharding import PartitionSpec as P

NORM_EPS = 1e-06
LANES = 128
F32 = jnp.float32
BF16 = jnp.bfloat16


def cmul(ar, ai, br, bi):
    return ar * br - ai * bi, ar * bi + ai * br


def cpow(r, i, n):
    outr, outi = None, None
    while n:
        if n % 2:
            outr, outi = (r, i) if outr is None else cmul(outr, outi, r, i)
        n //= 2
        if n:
            r, i = cmul(r, i, r, i)
    return outr, outi


def remote(src, dst, send, recv, target):
    return pltpu.make_async_remote_copy(
        src_ref=src,
        dst_ref=dst,
        send_sem=send,
        recv_sem=recv,
        device_id=target,
        device_id_type=pl.DeviceIdType.MESH,
    )


def layer(
    n_sp, n_tp, state, group,
    tok_h, nin_h, dlog_h, phase_h, bre_h, bim_h, cre_h, cim_h, skip_h, wv_h, wg_h, nout_h,
    out,
    nsend, urecv, rows_a, rows_p, t1r, t1i, t2r, t2i, bs, cs, wbuf, xbuf, wsum, ylocal,
    e_send, e_all, l_ref, zst, zbuf, w, acc, both, swapped, sq_all, ct, xct, xcs, yst, lh, xlh,
    bc, tok, nin, ap, sn,
    load_sem, a_send, a_recv, e_ssem, e_rsem, z_send, z_recv, w_sem, q_sem, c_sem, h_sem, met,
):
    sp, tp = lax.axis_index("sp"), lax.axis_index("tp")
    mine, d_model = tok.shape
    rows, width = out.shape
    half_rows = rows // 2
    n_blk = width // LANES
    per = LANES // group
    lanes = per * state
    core = lax.rem(tp, 2)
    chip = tp // 2
    partner = tp + 1 - 2 * core
    n_chip = n_tp // 2
    span = 2 * mine
    pair = 2 if n_sp % 2 == 0 else 1
    sp_b = lax.rem(sp, pair)
    early = 0
    half_chips = n_chip // 2

    parts = [pl.ds(i * width, width) for i in range(n_tp)]

    def load(i, *pairs):
        return [pltpu.make_async_copy(src, dst, load_sem.at[i]) for src, dst in pairs]

    loads = [
        load(0, *((tok_h.at[:, part], tok.at[:, part]) for part in parts)),
        load(1, (nin_h, nin)),
        load(2, (dlog_h, ap.at[0]), (phase_h, ap.at[1])),
        load(3, *((src, bc.at[i]) for i, src in enumerate((bre_h, bim_h, cre_h, cim_h)))),
        load(4, (skip_h, sn.at[0]), (nout_h, sn.at[1])),
        load(5, (wv_h, w.at[core, 0]), (wg_h, w.at[core, 1])),
    ]

    def start(*which):
        for i in which:
            for copy in loads[i]:
                copy.start()

    def loaded(*which):
        for i in which:
            dst = (tok, nin, ap, bc, sn, w.at[core])[i]
            pltpu.make_async_copy(dst, dst, load_sem.at[i]).wait()

    start(0, 1, 2)

    barrier = pltpu.get_barrier_semaphore()

    def tell(sem, axis):
        def go(j, c):
            pl.semaphore_signal(sem, inc=1, device_id={axis: j}, device_id_type=pl.DeviceIdType.MESH)
            return c

        return go

    def above(go):
        for b in range(pair):
            first = sp // pair + jnp.where(b > sp_b, 0, 1)
            go_b = lambda a, c, b=b: go(a * pair + b, c)
            lax.fori_loop(jnp.where(b >= sp_b, first, n_sp // pair), n_sp // pair, go_b, 0)

    def below(go):
        for b in range(pair):
            last = sp // pair + jnp.where(b < sp_b, 1, 0)
            lax.fori_loop(0, jnp.where(b <= sp_b, last, 0), lambda a, c, b=b: go(a * pair + b, c), 0)

    last = sp == n_sp - 1
    lax.fori_loop(jnp.where(last, tp + 1, 0), jnp.where(last, tp + 1, tp), tell(barrier, "tp"), 0)
    lax.fori_loop(tp + 1, n_tp, tell(barrier, "tp"), 0)
    above(tell(barrier, "sp"))
    start(3, 4)
    known = (sp // pair + 1) * (sp_b + 1) - 1 + jnp.where(last, tp, n_tp - 1)
    half = (n_sp // 2 + pair - 1) // pair * pair

    def enter():
        pl.when(known > 0)(lambda: pl.semaphore_wait(barrier, known))
        below(lambda j, c: tell(met.at[jnp.where(sp - j > half, 1, 0)], "sp")(j, c))
        lax.fori_loop(0, jnp.where(last, tp, 0), tell(met.at[2], "tp"), 0)

    pl.when(last)(enter)
    loaded(0, 1)

    xf = tok[...].astype(F32)
    scale = lax.rsqrt(jnp.sum(xf * xf, axis=1, keepdims=True) / d_model + NORM_EPS)
    normed = (xf * scale * nin[...]).astype(BF16)
    for j in range(n_tp):
        for blk in range(n_blk):
            at = j * width + blk * LANES
            nsend[j, blk] = normed[:, at : at + LANES]

    pl.when(jnp.logical_not(last))(enter)
    pl.when(last & (tp < n_tp - 1))(lambda: pl.semaphore_wait(met.at[2], n_tp - 1 - tp))


    def scatter(j, blk, at):
        remote(nsend.at[j, blk], urecv.at[tp, blk], a_send.at[0], a_recv.at[at], {"tp": j}).start()

    for blk in range(n_blk):
        for k in range(1, n_chip):
            other = lax.rem(chip + n_chip - k, n_chip)
            for j in (2 * other + core, 2 * other + 1 - core):
                scatter(j, blk, 1 + (k - 1) * n_blk + blk)
        if blk == 0:
            for b in range(n_blk):
                scatter(partner, b, 0)
    start(5)
    for i, src in enumerate((wv_h, wg_h)):
        remote(src, w.at[core, i], w_sem.at[0], w_sem.at[1], {"tp": partner}).start()
    urecv[tp] = nsend[tp]

    loaded(2)
    dlog, phase, skip, nout = ap.at[0], ap.at[1], sn.at[0], sn.at[1]
    bre, bim, cre, cim = (bc.at[i] for i in range(4))
    side = LANES // state
    for i in range(width // group // side):
        cut = slice(i * LANES, (i + 1) * LANES)
        for src, dst in ((dlog, rows_a), (phase, rows_p)):
            row = jnp.concatenate([src[i * side + k : i * side + k + 1, :] for k in range(side)], axis=1)
            dst[:, cut] = jnp.broadcast_to(row, (8, LANES))

    for blk in range(n_blk):
        cut = slice(blk * lanes, (blk + 1) * lanes)
        a, p = rows_a[:, cut], rows_p[:, cut]
        mag, cos, sin = jnp.exp(a), jnp.cos(p), jnp.sin(p)
        lr, li = mag * cos, mag * sin
        inv = jnp.exp(-a)
        nr, ni = inv * cos, -inv * sin
        mod = a * a + p * p
        cr = ((lr - 1.0) * a + li * p) / mod
        ci = (li * a - (lr - 1.0) * p) / mod
        one, zero = jnp.ones_like(a), jnp.zeros_like(a)
        pr, pi, mr, mi = one, zero, cr, ci
        sr, si, qr, qi = lr, li, nr, ni
        row = lax.broadcasted_iota(jnp.int32, a.shape, 0)
        for bit in range(3):
            on = lax.rem(row // (1 << bit), 2) == 1
            ar, ai = cmul(pr, pi, sr, si)
            pr, pi = jnp.where(on, ar, pr), jnp.where(on, ai, pi)
            ar, ai = cmul(mr, mi, qr, qi)
            mr, mi = jnp.where(on, ar, mr), jnp.where(on, ai, mi)
            sr, si = cmul(sr, si, sr, si)
            qr, qi = cmul(qr, qi, qr, qi)
        t2r[0:8, cut], t2i[0:8, cut], t1r[0:8, cut], t1i[0:8, cut] = pr, pi, mr, mi
        done = 8
        while done < span:
            more = min(done, span - done)
            for off in range(0, more, 8):
                src, dst = slice(off, off + 8), slice(done + off, done + off + 8)
                t2r[dst, cut], t2i[dst, cut] = cmul(t2r[src, cut], t2i[src, cut], sr, si)
                t1r[dst, cut], t1i[dst, cut] = cmul(t1r[src, cut], t1i[src, cut], qr, qi)
            sr, si = cmul(sr, si, sr, si)
            qr, qi = cmul(qr, qi, qr, qi)
            done += more
        endr, endi = t2r[span - 1 : span, cut], t2i[span - 1 : span, cut]
        wholer, wholei = cmul(endr, endi, lr[0:1], li[0:1])
        allr, alli = cpow(wholer, wholei, n_chip)
        for k, value in enumerate((allr, alli, lr[0:1], li[0:1], wholer, wholei, endr, endi)):
            l_ref[blk, k : k + 1, :] = value

    loaded(3, 4)
    keep_b = (
        lax.broadcasted_iota(jnp.int32, (LANES, lanes), 0) // group
        == lax.broadcasted_iota(jnp.int32, (LANES, lanes), 1) // state
    )
    of_col = lax.broadcasted_iota(jnp.int32, (state, LANES), 1) // group
    a, p = dlog[...], phase[...]
    mag = jnp.exp(a)
    stepr, stepi = cpow(mag * jnp.cos(p), mag * jnp.sin(p), span)

    def widen(dst, turned, c):
        for part in range(2):
            piece = turned[part * state : (part + 1) * state]
            for g in range(per):
                at = part * lanes + g * state
                dst[at : at + state, c * LANES : (c + 1) * LANES] = jnp.where(of_col == g, piece, 0.0).astype(BF16)

    for blk in range(n_blk):
        ch = slice(blk * LANES, (blk + 1) * LANES)
        for part, in_ref in ((0, bre), (1, bim)):
            b = in_ref[ch, :]
            b = jnp.concatenate([b] * side, axis=1)
            wide = jnp.where(keep_b, jnp.concatenate([b] * (lanes // LANES), axis=1), 0.0)
            bs[blk, :, part * lanes : (part + 1) * lanes] = wide.astype(BF16)
        c_r, c_i = cre[ch, :], cim[ch, :]
        if n_chip > 1:
            spread = [
                jnp.concatenate(
                    [jnp.broadcast_to(s[g : g + 1], (group, state)) for g in range(blk * per, (blk + 1) * per)],
                    axis=0,
                )
                for s in (stepr, stepi)
            ]
        for c in range(n_chip):
            if c:
                c_r, c_i = cmul(c_r, c_i, *spread)
            turned = jnp.concatenate([c_r, -c_i], axis=1).T
            if blk == early:
                ct[c] = turned.astype(BF16)
            widen(cs.at[blk], turned, c)
    def across(start):
        for k in range(1, n_chip):
            for h in range(2):
                start(h, 2 * lax.rem(chip + k, n_chip) + h)

    @pl.when(sp > 0)
    def _():
        across(
            lambda h, j: remote(
                ct.at[pl.ds(h * half_chips, half_chips)], xct.at[tp], c_sem.at[0], c_sem.at[1], {"tp": j}
            ).start()
        )

    lower = (
        lax.broadcasted_iota(jnp.int32, (span, span), 0)
        >= lax.broadcasted_iota(jnp.int32, (span, span), 1)
    ).astype(BF16)

    def landed(ref, sem):
        remote(ref, ref, a_send.at[0], sem, {"tp": partner}).wait_recv()

    def gone(ref, sem):
        remote(ref, ref, sem, a_recv.at[0], {"tp": partner}).wait_send()

    def source(c, blk):
        return jnp.concatenate([urecv[2 * c + s, blk].astype(F32) for s in range(2)], axis=0)

    def drive(c, blk):
        cut = slice(blk * lanes, (blk + 1) * lanes)
        d = jnp.dot(source(c, blk).astype(BF16), bs[blk], preferred_element_type=F32)
        wr, wi = cmul(d[:, :lanes], d[:, lanes:], t1r[:, cut], t1i[:, cut])
        wbuf[blk][c, :, :lanes] = wr.astype(BF16)
        wbuf[blk][c, :, lanes:] = wi.astype(BF16)
        wsum[blk][c, 0:1, :] = jnp.sum(wr, axis=0, keepdims=True)
        wsum[blk][c, 1:2, :] = jnp.sum(wi, axis=0, keepdims=True)

    def seeds(blk):
        turn = l_ref[blk, 4:5], l_ref[blk, 5:6]
        held = [None]
        for c in range(n_chip):
            r, i = wsum[blk][c, 0:1], wsum[blk][c, 1:2]
            if c:
                r, i = r + held[c][0], i + held[c][1]
            held.append(cmul(r, i, *turn) if c < n_chip - 1 else cmul(r, i, l_ref[blk, 6:7], l_ref[blk, 7:8]))
        return held

    def end_copy(j, blk):
        return remote(e_send.at[blk], e_all.at[blk, sp], e_ssem.at[0], e_rsem.at[blk], {"sp": j})

    def scan(blk):
        cut = slice(blk * lanes, (blk + 1) * lanes)
        held = seeds(blk)
        for c in range(n_chip):
            s = jnp.dot(lower, wbuf[blk][c], preferred_element_type=F32)
            sr, si = s[:, :lanes], s[:, lanes:]
            if c:
                sr, si = sr + held[c][0], si + held[c][1]
            xr, xi = cmul(sr, si, t2r[:, cut], t2i[:, cut])
            at = slice(c * span, (c + 1) * span)
            xbuf[blk][at, :lanes] = xr.astype(BF16)
            xbuf[blk][at, lanes:] = xi.astype(BF16)

    def readout(blk):
        ch = slice(blk * LANES, (blk + 1) * LANES)
        y = jnp.dot(xbuf[blk][...], cs[blk, :, :LANES], preferred_element_type=F32)
        for c in range(n_chip):
            at = slice(c * span, (c + 1) * span)
            ylocal[blk][at] = y[at] + skip[:, ch] * source(c, blk)

    landed(urecv.at[partner], a_recv.at[0])
    for blk in range(n_blk):
        drive(chip, blk)

    def send_ends(blks, first, last):
        def go(j, c):
            for blk in blks:
                end_copy(j, blk).start()
            return c

        lax.fori_loop(first, last, go, 0)

    def finish(blk, y):
        for c in range(n_chip):
            at = slice(c * span, (c + 1) * span)
            v = ylocal[blk][at]
            if y is not None:
                v = v + y[:, c * LANES : (c + 1) * LANES]
            top, to = half_of(c)
            zst[top, blk, to] = jax.nn.gelu(v).astype(BF16)
        if y is None or blk != early:
            cross(blk, zst.at[:, blk])
        remote(
            zst.at[1 - core, blk], zbuf.at[tp, blk], z_send.at[0], z_recv.at[0], {"tp": partner}
        ).start()

    def half_of(c):
        top = c * span // half_rows
        return top, slice(c * span - top * half_rows, (c + 1) * span - top * half_rows)

    def cross(blk, src):
        for k in range(1, n_chip):
            for h in (core, 1 - core):
                remote(
                    src.at[h], zbuf.at[tp, blk], z_send.at[0], z_recv.at[1 + (k - 1) * n_blk + blk],
                    {"tp": 2 * lax.rem(chip + k, n_chip) + h},
                ).start()

    def reach(i, old, new):
        count = new - old if pair == 1 else jnp.where(sp_b == 0, new - old, (new - old) // pair)
        pl.when(count > 0)(lambda: pl.semaphore_wait(met.at[i], count))

    def take(blk):
        for k in range(1, n_chip):
            c = lax.rem(chip + k, n_chip)
            landed(urecv.at[pl.ds(2 * c, 2), blk], a_recv.at[1 + (k - 1) * n_blk + blk])
        for k in range(1, n_chip):
            drive(lax.rem(chip + k, n_chip), blk)

    close = jnp.minimum(sp + 1 + half, n_sp)

    def give(blk):
        er, ei = seeds(blk)[n_chip]
        e_send[blk] = jnp.concatenate([er, ei], axis=0).astype(BF16)

    def post(blk):
        if blk == 0:
            reach(0, sp + 1, close)
            send_ends([0], sp + 1, close)
            return
        if blk == 1:
            reach(1, close, n_sp)
        send_ends([blk], sp + 1, close)
        send_ends(range(2) if blk == 1 else [blk], close, n_sp)

    @pl.when(sp == 0)
    def _():
        for blk in range(n_blk):
            take(blk)
            give(blk)
            if blk != 1:
                post(blk)
            else:
                send_ends([1], sp + 1, close)
            scan(blk)
            readout(blk)
            finish(blk, None)
            if blk == 1:
                reach(1, close, n_sp)
                send_ends(range(2), close, n_sp)

    @pl.when(sp > 0)
    def _():
        for blk in range(n_blk + 2):
            if blk < n_blk:
                take(blk)
            if 1 <= blk <= n_blk:
                scan(blk - 1)
            if 2 <= blk:
                readout(blk - 2)
            if blk < n_blk:
                give(blk)
                post(blk)
            if blk - 2 == early:
                for c in range(n_chip):
                    top, to = half_of(c)
                    yst[top, to] = ylocal[early][c * span : (c + 1) * span].astype(BF16)
                cross(early, yst)

    def after(blk):
        cut = slice(blk * lanes, (blk + 1) * lanes)
        lr, li = l_ref[blk, 0:1], l_ref[blk, 1:2]

        def join(j, held):
            e = e_all[blk, j].astype(F32)
            hr, hi = cmul(*held, lr, li)
            return hr + e[0:1], hi + e[1:2]

        for s in range(1, n_sp):
            pl.when(sp == s)(functools.partial(landed, e_all.at[blk, pl.ds(0, s)], e_rsem.at[blk]))
        nil = jnp.zeros((1, lanes), F32)
        hr, hi = lax.fori_loop(0, sp, join, (nil, nil))
        hr, hi = cmul(hr, hi, l_ref[blk, 2:3], l_ref[blk, 3:4])
        if blk == early:
            lh[...] = jnp.concatenate([l_ref[blk, 2:4], hr, hi], axis=0)
            across(lambda h, j: remote(lh, xlh.at[tp], h_sem.at[0], h_sem.at[1], {"tp": j}).start())
        xr, xi = cmul(hr, hi, t2r[:, cut], t2i[:, cut])
        x = jnp.concatenate([xr.astype(BF16), xi.astype(BF16)], axis=1)
        finish(blk, jnp.dot(x, cs[blk], preferred_element_type=F32))


    @pl.when(sp > 0)
    def _():
        for blk in range(n_blk):
            after(blk)

    @pl.when(sp > 0)
    def _():
        landed(xct.at[pl.ds(0, n_tp - 2)], c_sem.at[1])
        for k in range(1, n_chip):
            for h in range(2):
                j = 2 * lax.rem(chip + n_chip - k, n_chip) + h
                for c in range(half_chips):
                    widen(xcs.at[2 * (k - 1) + h], xct[j, c].astype(F32), c)

    def correct(k, c2):
        if k == 1:
            landed(xlh.at[pl.ds(0, n_tp - 2)], h_sem.at[1])
        fixed = []
        for h in range(2):
            j = c2 + h
            lr, li, pr, pi = (jnp.broadcast_to(xlh[j, i : i + 1], (8, lanes)) for i in range(4))
            row = lax.broadcasted_iota(jnp.int32, (8, lanes), 0)
            for bit in range(3):
                on = lax.rem(row // (1 << bit), 2) == 1
                ar, ai = cmul(pr, pi, lr, li)
                pr, pi = jnp.where(on, ar, pr), jnp.where(on, ai, pi)
                lr, li = cmul(lr, li, lr, li)
            pieces = [(pr, pi)]
            while len(pieces) < span // 8:
                pieces += [cmul(*p, lr, li) for p in pieces[: span // 8 - len(pieces)]]
                lr, li = cmul(lr, li, lr, li)
            x = jnp.concatenate(
                [jnp.concatenate([p[i] for p in pieces], axis=0).astype(BF16) for i in range(2)], axis=1
            )
            fixed.append(jnp.dot(x, xcs[2 * (k - 1) + h], preferred_element_type=F32))
        held = [zbuf[c2 + h, early].astype(F32) for h in range(2)]
        for h in range(2):
            y = jnp.concatenate([fixed[h][:, c * LANES : (c + 1) * LANES] for c in range(half_chips)], axis=0)
            held[h] = jax.nn.gelu(held[h] + y).astype(BF16)
        for h in range(2):
            zbuf[c2 + h, early] = held[h]

    loaded(5)

    def project(ref, i, j, blks):
        at = pl.ds(pl.multiple_of(j * width + blks[0] * LANES, LANES), LANES * len(blks))
        z = jnp.concatenate([ref[i, blk] for blk in blks], axis=1)
        return z, at

    def products(*parts):
        z = jnp.concatenate([p[0] for p in parts], axis=1)
        return [
            [
                jnp.dot(
                    z, jnp.concatenate([w[q, i, p[1], :] for p in parts], axis=0), preferred_element_type=F32
                )
                for i in range(2)
            ]
            for q in range(2)
        ]

    def add(new):
        for q in range(2):
            for i in range(2):
                acc[q, i] += new[q][i]

    landed(w.at[1 - core], w_sem.at[1])
    every = range(n_blk)
    new = products(project(zst, core, tp, every))
    for q in range(2):
        for i in range(2):
            acc[q, i] = new[q][i]
    landed(zbuf.at[partner], z_recv.at[0])
    add(products(project(zbuf, partner, partner, every)))
    for blk in range(n_blk):
        for k in range(1, n_chip):
            c2 = 2 * lax.rem(chip + n_chip - k, n_chip)
            landed(zbuf.at[pl.ds(c2, 2), blk], z_recv.at[1 + (k - 1) * n_blk + blk])
            if blk == early:
                pl.when(sp > 0)(functools.partial(correct, k, c2))
            new = products(*(project(zbuf, c2 + h, c2 + h, [blk]) for h in range(2)))
            if blk < n_blk - 1 or k < n_chip - 1:
                add(new)
    part = None
    for q in range(2):
        v, g = (acc[q, i] + new[q][i] for i in range(2))
        gated = v * (0.5 + 0.5 * jnp.tanh(0.5 * g))
        both[q] = gated
        square = gated * gated
        for blk in range(n_blk):
            piece = square[:, blk * LANES : (blk + 1) * LANES]
            part = piece if part is None else part + piece
    remote(both.at[1 - core], swapped, q_sem.at[2], q_sem.at[3], {"tp": partner}).start()
    sums = jnp.sum(part, axis=1, keepdims=True)
    lane = lax.broadcasted_iota(jnp.int32, (8, LANES), 1)
    total = jnp.zeros((8, LANES), F32)
    for k in range(half_rows // 8):
        total = jnp.where(lane == k, sums[8 * k : 8 * k + 8], total)
    sq_all[tp] = total
    for k in range(1, n_tp):
        j = lax.rem(tp + n_tp - k, n_tp)
        remote(sq_all.at[tp], sq_all.at[tp], q_sem.at[0], q_sem.at[1], {"tp": j}).start()
    gone(nsend.at[pl.ds(0, n_tp - 1)], a_send.at[0])
    gone(zbuf.at[pl.ds(0, n_tp - 1)], z_send.at[0])
    gone(w.at[core], w_sem.at[0])

    @pl.when(sp > 0)
    def _():
        gone(xct.at[pl.ds(0, n_tp - 2)], c_sem.at[0])
        gone(xlh.at[pl.ds(0, n_tp - 2)], h_sem.at[0])

    for s in range(n_sp - 1):
        pl.when(sp == s)(functools.partial(gone, e_all.at[:, pl.ds(0, n_sp - 1 - s)], e_ssem.at[0]))
    both[core] = both[core] * nout[...]
    landed(swapped, q_sem.at[3])
    swapped[...] = swapped[...] * nout[...]
    landed(sq_all.at[pl.ds(0, n_tp - 1)], q_sem.at[1])
    for h in (core, 1 - core):
        total = sq_all[h]
        for c in range(1, n_chip):
            total = total + sq_all[2 * c + h]
        scale = lax.rsqrt(total / d_model + NORM_EPS)
        column = jnp.concatenate([scale[:, i : i + 1] for i in range(half_rows // 8)], axis=0)
        gated = both[core] if h is core else swapped[...]
        at = pl.ds(pl.multiple_of(h * half_rows, half_rows), half_rows)
        out[at, :] = (gated * column).astype(BF16)

    gone(sq_all.at[pl.ds(0, n_tp - 1)], q_sem.at[0])
    gone(swapped, q_sem.at[2])


def solution(mesh):
    n_sp, n_tp = mesh.shape["sp"], mesh.shape["tp"]

    def on_device(
        tokens, norm_in, decay_log, phase, b_real, b_imag, c_real, c_imag, skip_gain, w_value, w_gate, norm_out
    ):
        mine, d_model = tokens.shape
        rows = mine * n_tp
        groups, state, group = b_real.shape
        width = groups * group
        n_blk = width // LANES
        lanes = LANES // group * state
        entries = groups * state
        n_chip = n_tp // 2
        span = 2 * mine
        vmem = pl.BlockSpec(memory_space=pltpu.VMEM)
        hbm = pl.BlockSpec(memory_space=pl.ANY)
        dma = pltpu.SemaphoreType.DMA
        return pl.pallas_call(
            functools.partial(layer, n_sp, n_tp, state, group),
            out_shape=pltpu.VMEM((rows, width), BF16),
            in_specs=[hbm] * 12,
            out_specs=vmem,
            scratch_shapes=[
                pltpu.VMEM((n_tp, n_blk, mine, LANES), BF16),
                pltpu.VMEM((n_tp, n_blk, mine, LANES), BF16),
                pltpu.VMEM((8, entries), F32),
                pltpu.VMEM((8, entries), F32),
                pltpu.VMEM((span, entries), F32),
                pltpu.VMEM((span, entries), F32),
                pltpu.VMEM((span, entries), F32),
                pltpu.VMEM((span, entries), F32),
                pltpu.VMEM((n_blk, LANES, 2 * lanes), BF16),
                pltpu.VMEM((n_blk, 2 * lanes, n_chip * LANES), BF16),
                [pltpu.VMEM((n_chip, span, 2 * lanes), BF16)] * n_blk,
                [pltpu.VMEM((rows, 2 * lanes), BF16)] * n_blk,
                [pltpu.VMEM((n_chip, 2, lanes), F32)] * n_blk,
                [pltpu.VMEM((rows, LANES), F32)] * n_blk,
                pltpu.VMEM((n_blk, 2, lanes), BF16),
                pltpu.VMEM((n_blk, n_sp, 2, lanes), BF16),
                pltpu.VMEM((n_blk, 8, lanes), F32),
                pltpu.VMEM((2, n_blk, rows // 2, LANES), BF16),
                pltpu.VMEM((n_tp, n_blk, rows // 2, LANES), BF16),
                pltpu.VMEM((2, 2) + w_value.shape, BF16),
                pltpu.VMEM((2, 2, rows // 2, width), F32),
                pltpu.VMEM((2, rows // 2, width), F32),
                pltpu.VMEM((rows // 2, width), F32),
                pltpu.VMEM((n_tp, 8, LANES), F32),
                pltpu.VMEM((n_chip, 2 * state, LANES), BF16),
                pltpu.VMEM((n_tp, n_chip // 2, 2 * state, LANES), BF16),
                pltpu.VMEM((n_tp - 2, 2 * lanes, n_chip // 2 * LANES), BF16),
                pltpu.VMEM((2, rows // 2, LANES), BF16),
                pltpu.VMEM((4, lanes), F32),
                pltpu.VMEM((n_tp, 4, lanes), F32),
                pltpu.VMEM((4, width, state), F32),
                pltpu.VMEM((mine, d_model), BF16),
                pltpu.VMEM((1, d_model), F32),
                pltpu.VMEM((2, groups, state), F32),
                pltpu.VMEM((2, 1, width), F32),
                dma((6,)),
                dma((1,)),
                dma((1 + (n_chip - 1) * n_blk,)),
                dma((1,)),
                dma((n_blk,)),
                dma((1,)),
                dma((1 + (n_chip - 1) * n_blk,)),
                dma((2,)),
                dma((4,)),
                dma((2,)),
                dma((2,)),
                pltpu.SemaphoreType.REGULAR((3,)),
            ],
            compiler_params=pltpu.CompilerParams(collective_id=0, has_side_effects=True),
        )(
            tokens,
            norm_in.reshape(1, -1),
            decay_log,
            phase,
            b_real.transpose(0, 2, 1).reshape(width, state),
            b_imag.transpose(0, 2, 1).reshape(width, state),
            c_real.reshape(width, state),
            c_imag.reshape(width, state),
            skip_gain.reshape(1, -1),
            w_value,
            w_gate,
            norm_out.reshape(1, -1),
        )

    placed = (
        P(("sp", "tp"), None),
        P(),
        P("tp", None),
        P("tp", None),
        P("tp", None, None),
        P("tp", None, None),
        P("tp", None, None),
        P("tp", None, None),
        P("tp"),
        P(None, "tp"),
        P(None, "tp"),
        P("tp"),
    )
    return jax.shard_map(
        on_device, mesh=mesh, in_specs=placed, out_specs=P("sp", "tp"), check_vma=False
    )
```

```python
import functools

import jax
import jax.numpy as jnp
from jax import lax
from jax.experimental import pallas as pl
from jax.experimental.pallas import tpu as pltpu
from jax.sharding import PartitionSpec as P

NORM_EPS = 1e-06
LANES = 128
F32 = jnp.float32
BF16 = jnp.bfloat16


def cmul(ar, ai, br, bi):
    return ar * br - ai * bi, ar * bi + ai * br


def cpow(r, i, n):
    outr, outi = None, None
    while n:
        if n % 2:
            outr, outi = (r, i) if outr is None else cmul(outr, outi, r, i)
        n //= 2
        if n:
            r, i = cmul(r, i, r, i)
    return outr, outi


def remote(src, dst, send, recv, target):
    return pltpu.make_async_remote_copy(
        src_ref=src,
        dst_ref=dst,
        send_sem=send,
        recv_sem=recv,
        device_id=target,
        device_id_type=pl.DeviceIdType.MESH,
    )


def layer(
    n_sp, n_tp, state, group,
    tok_h, nin_h, dlog_h, phase_h, bre_h, bim_h, cre_h, cim_h, skip_h, wv_h, wg_h, nout_h,
    out,
    nsend, urecv, rows_a, rows_p, t1r, t1i, t2r, t2i, bs, cs, wbuf, xbuf, wsum, ylocal,
    e_send, e_all, l_ref, zst, zbuf, w, acc, both, swapped, sq_all, ct, xct, xcs, yst, lam, xlam, begin, xbegin,
    bc, tok, nin, ap, sn,
    load_sem, a_recv, e_ssem, e_rsem, z_recv, w_sem, q_sem, x_sem, met,
):
    sp, tp = lax.axis_index("sp"), lax.axis_index("tp")
    mine, d_model = tok.shape
    rows, width = out.shape
    half_rows = rows // 2
    n_blk = width // LANES
    per = LANES // group
    lanes = per * state
    core = lax.rem(tp, 2)
    chip = tp // 2
    partner = tp + 1 - 2 * core
    n_chip = n_tp // 2
    span = 2 * mine
    pair = 2 if n_sp % 2 == 0 else 1
    sp_b = lax.rem(sp, pair)
    early = 0
    half_chips = n_chip // 2

    parts = [pl.ds(i * width, width) for i in range(n_tp)]

    def load(i, *pairs):
        return [pltpu.make_async_copy(src, dst, load_sem.at[i]) for src, dst in pairs]

    loads = [
        load(0, *((tok_h.at[:, part], tok.at[:, part]) for part in parts)),
        load(1, (nin_h, nin)),
        load(2, (dlog_h, ap.at[0]), (phase_h, ap.at[1])),
        load(3, *((src, bc.at[i]) for i, src in enumerate((bre_h, bim_h, cre_h, cim_h)))),
        load(4, (skip_h, sn.at[0]), (nout_h, sn.at[1])),
        load(5, (wv_h, w.at[core, 0]), (wg_h, w.at[core, 1])),
    ]

    def start(*which):
        for i in which:
            for copy in loads[i]:
                copy.start()

    def loaded(*which):
        for i in which:
            dst = (tok, nin, ap, bc, sn, w.at[core])[i]
            pltpu.make_async_copy(dst, dst, load_sem.at[i]).wait()

    start(0, 1, 2)

    barrier = pltpu.get_barrier_semaphore()

    def tell(sem, axis):
        def go(j, c):
            pl.semaphore_signal(sem, inc=1, device_id={axis: j}, device_id_type=pl.DeviceIdType.MESH)
            return c

        return go

    def above(go):
        for b in range(pair):
            first = sp // pair + jnp.where(b > sp_b, 0, 1)
            go_b = lambda a, c, b=b: go(a * pair + b, c)
            lax.fori_loop(jnp.where(b >= sp_b, first, n_sp // pair), n_sp // pair, go_b, 0)

    def below(go):
        for b in range(pair):
            last = sp // pair + jnp.where(b < sp_b, 1, 0)
            lax.fori_loop(0, jnp.where(b <= sp_b, last, 0), lambda a, c, b=b: go(a * pair + b, c), 0)

    last = sp == n_sp - 1
    lax.fori_loop(jnp.where(last, tp + 1, 0), jnp.where(last, tp + 1, tp), tell(barrier, "tp"), 0)
    lax.fori_loop(tp + 1, n_tp, tell(barrier, "tp"), 0)
    above(tell(barrier, "sp"))
    start(3, 4)
    known = (sp // pair + 1) * (sp_b + 1) - 1 + jnp.where(last, tp, n_tp - 1)
    half = (n_sp // 2 + pair - 1) // pair * pair

    def enter():
        pl.when(known > 0)(lambda: pl.semaphore_wait(barrier, known))
        below(lambda j, c: tell(met.at[jnp.where(sp - j > half, 1, 0)], "sp")(j, c))
        lax.fori_loop(0, jnp.where(last, tp, 0), tell(met.at[0], "tp"), 0)

    pl.when(last)(enter)
    loaded(0, 1)

    xf = tok[...].astype(F32)
    scale = lax.rsqrt(jnp.sum(xf * xf, axis=1, keepdims=True) / d_model + NORM_EPS)
    normed = (xf * scale * nin[...]).astype(BF16)
    for j in range(n_tp):
        for blk in range(n_blk):
            at = j * width + blk * LANES
            nsend[j, blk] = normed[:, at : at + LANES]

    pl.when(jnp.logical_not(last))(enter)
    pl.when(last & (tp < n_tp - 1))(lambda: pl.semaphore_wait(met.at[0], n_tp - 1 - tp))


    def scatter(j, blk, at):
        remote(nsend.at[j, blk], urecv.at[tp, blk], load_sem.at[0], a_recv.at[at], {"tp": j}).start()

    for blk in range(n_blk):
        for k in range(1, n_chip):
            other = lax.rem(chip + n_chip - k, n_chip)
            for j in (2 * other + core, 2 * other + 1 - core):
                scatter(j, blk, 1 + (k - 1) * n_blk + blk)
        if blk == 0:
            for b in range(n_blk):
                scatter(partner, b, 0)
    start(5)
    for i, src in enumerate((wv_h, wg_h)):
        remote(src, w.at[core, i], w_sem.at[0], w_sem.at[1], {"tp": partner}).start()
    urecv[tp] = nsend[tp]

    loaded(2)
    dlog, phase, skip, nout = ap.at[0], ap.at[1], sn.at[0], sn.at[1]
    bre, bim, cre, cim = (bc.at[i] for i in range(4))
    side = LANES // state
    for i in range(width // group // side):
        cut = slice(i * LANES, (i + 1) * LANES)
        for src, dst in ((dlog, rows_a), (phase, rows_p)):
            row = jnp.concatenate([src[i * side + k : i * side + k + 1, :] for k in range(side)], axis=1)
            dst[:, cut] = jnp.broadcast_to(row, (8, LANES))

    for blk in range(n_blk):
        cut = slice(blk * lanes, (blk + 1) * lanes)
        a, p = rows_a[:, cut], rows_p[:, cut]
        mag, cos, sin = jnp.exp(a), jnp.cos(p), jnp.sin(p)
        lr, li = mag * cos, mag * sin
        inv = jnp.exp(-a)
        nr, ni = inv * cos, -inv * sin
        mod = a * a + p * p
        cr = ((lr - 1.0) * a + li * p) / mod
        ci = (li * a - (lr - 1.0) * p) / mod
        one, zero = jnp.ones_like(a), jnp.zeros_like(a)
        pr, pi, mr, mi = one, zero, cr, ci
        sr, si, qr, qi = lr, li, nr, ni
        row = lax.broadcasted_iota(jnp.int32, a.shape, 0)
        for bit in range(3):
            on = lax.rem(row // (1 << bit), 2) == 1
            ar, ai = cmul(pr, pi, sr, si)
            pr, pi = jnp.where(on, ar, pr), jnp.where(on, ai, pi)
            ar, ai = cmul(mr, mi, qr, qi)
            mr, mi = jnp.where(on, ar, mr), jnp.where(on, ai, mi)
            sr, si = cmul(sr, si, sr, si)
            qr, qi = cmul(qr, qi, qr, qi)
        t2r[0:8, cut], t2i[0:8, cut], t1r[0:8, cut], t1i[0:8, cut] = pr, pi, mr, mi
        done = 8
        while done < span:
            more = min(done, span - done)
            for off in range(0, more, 8):
                src, dst = slice(off, off + 8), slice(done + off, done + off + 8)
                t2r[dst, cut], t2i[dst, cut] = cmul(t2r[src, cut], t2i[src, cut], sr, si)
                t1r[dst, cut], t1i[dst, cut] = cmul(t1r[src, cut], t1i[src, cut], qr, qi)
            sr, si = cmul(sr, si, sr, si)
            qr, qi = cmul(qr, qi, qr, qi)
            done += more
        endr, endi = t2r[span - 1 : span, cut], t2i[span - 1 : span, cut]
        wholer, wholei = cmul(endr, endi, lr[0:1], li[0:1])
        allr, alli = cpow(wholer, wholei, n_chip)
        for k, value in enumerate((allr, alli, lr[0:1], li[0:1], wholer, wholei, endr, endi)):
            l_ref[blk, k : k + 1, :] = value

    loaded(3, 4)
    keep_b = (
        lax.broadcasted_iota(jnp.int32, (LANES, lanes), 0) // group
        == lax.broadcasted_iota(jnp.int32, (LANES, lanes), 1) // state
    )
    of_col = lax.broadcasted_iota(jnp.int32, (state, LANES), 1) // group
    a, p = dlog[...], phase[...]
    mag = jnp.exp(a)
    stepr, stepi = cpow(mag * jnp.cos(p), mag * jnp.sin(p), span)

    def widen(dst, turned, c):
        for part in range(2):
            piece = turned[part * state : (part + 1) * state]
            for g in range(per):
                at = part * lanes + g * state
                dst[at : at + state, c * LANES : (c + 1) * LANES] = jnp.where(of_col == g, piece, 0.0).astype(BF16)

    for blk in range(n_blk):
        ch = slice(blk * LANES, (blk + 1) * LANES)
        for part, in_ref in ((0, bre), (1, bim)):
            b = in_ref[ch, :]
            b = jnp.concatenate([b] * side, axis=1)
            wide = jnp.where(keep_b, jnp.concatenate([b] * (lanes // LANES), axis=1), 0.0)
            bs[blk, :, part * lanes : (part + 1) * lanes] = wide.astype(BF16)
        c_r, c_i = cre[ch, :], cim[ch, :]
        if n_chip > 1:
            spread = [
                jnp.concatenate(
                    [jnp.broadcast_to(s[g : g + 1], (group, state)) for g in range(blk * per, (blk + 1) * per)],
                    axis=0,
                )
                for s in (stepr, stepi)
            ]
        for c in range(n_chip):
            if c:
                c_r, c_i = cmul(c_r, c_i, *spread)
            turned = jnp.concatenate([c_r, -c_i], axis=1).T
            if blk == early:
                ct[c] = turned.astype(BF16)
            widen(cs.at[blk], turned, c)
    def across(start):
        for k in range(1, n_chip):
            for h in range(2):
                start(h, 2 * lax.rem(chip + k, n_chip) + h)

    @pl.when(sp > 0)
    def _():
        lam[...] = l_ref[early, 2:4]
        across(
            lambda h, j: remote(
                ct.at[pl.ds(h * half_chips, half_chips)], xct.at[tp], load_sem.at[2], x_sem.at[0], {"tp": j}
            ).start()
        )
        across(lambda h, j: remote(lam, xlam.at[tp], load_sem.at[3], x_sem.at[1], {"tp": j}).start())

    lower = (
        lax.broadcasted_iota(jnp.int32, (span, span), 0)
        >= lax.broadcasted_iota(jnp.int32, (span, span), 1)
    ).astype(BF16)

    def landed(ref, sem):
        remote(ref, ref, load_sem.at[0], sem, {"tp": partner}).wait_recv()

    def gone(ref, sem):
        remote(ref, ref, sem, a_recv.at[0], {"tp": partner}).wait_send()

    def source(c, blk):
        return jnp.concatenate([urecv[2 * c + s, blk].astype(F32) for s in range(2)], axis=0)

    def drive(c, blk):
        cut = slice(blk * lanes, (blk + 1) * lanes)
        d = jnp.dot(source(c, blk).astype(BF16), bs[blk], preferred_element_type=F32)
        wr, wi = cmul(d[:, :lanes], d[:, lanes:], t1r[:, cut], t1i[:, cut])
        wbuf[blk][c, :, :lanes] = wr.astype(BF16)
        wbuf[blk][c, :, lanes:] = wi.astype(BF16)
        wsum[blk][c, 0:1, :] = jnp.sum(wr, axis=0, keepdims=True)
        wsum[blk][c, 1:2, :] = jnp.sum(wi, axis=0, keepdims=True)

    def seeds(blk):
        turn = l_ref[blk, 4:5], l_ref[blk, 5:6]
        held = [None]
        for c in range(n_chip):
            r, i = wsum[blk][c, 0:1], wsum[blk][c, 1:2]
            if c:
                r, i = r + held[c][0], i + held[c][1]
            held.append(cmul(r, i, *turn) if c < n_chip - 1 else cmul(r, i, l_ref[blk, 6:7], l_ref[blk, 7:8]))
        return held

    def end_copy(j, blk):
        return remote(e_send.at[blk], e_all.at[blk, sp], e_ssem.at[0], e_rsem.at[blk], {"sp": j})

    def scan(blk):
        cut = slice(blk * lanes, (blk + 1) * lanes)
        held = seeds(blk)
        for c in range(n_chip):
            s = jnp.dot(lower, wbuf[blk][c], preferred_element_type=F32)
            sr, si = s[:, :lanes], s[:, lanes:]
            if c:
                sr, si = sr + held[c][0], si + held[c][1]
            xr, xi = cmul(sr, si, t2r[:, cut], t2i[:, cut])
            at = slice(c * span, (c + 1) * span)
            xbuf[blk][at, :lanes] = xr.astype(BF16)
            xbuf[blk][at, lanes:] = xi.astype(BF16)

    def readout(blk):
        ch = slice(blk * LANES, (blk + 1) * LANES)
        y = jnp.dot(xbuf[blk][...], cs[blk, :, :LANES], preferred_element_type=F32)
        for c in range(n_chip):
            at = slice(c * span, (c + 1) * span)
            ylocal[blk][at] = y[at] + skip[:, ch] * source(c, blk)

    landed(urecv.at[partner], a_recv.at[0])
    for blk in range(n_blk):
        drive(chip, blk)

    def send_ends(blks, first, last):
        def go(j, c):
            for blk in blks:
                end_copy(j, blk).start()
            return c

        lax.fori_loop(first, last, go, 0)

    def finish(blk, y):
        for c in range(n_chip):
            at = slice(c * span, (c + 1) * span)
            v = ylocal[blk][at]
            if y is not None:
                v = v + y[:, c * LANES : (c + 1) * LANES]
            top, to = half_of(c)
            zst[top, blk, to] = jax.nn.gelu(v).astype(BF16)
        if y is None or blk != early:
            cross(blk, zst.at[:, blk])
        remote(
            zst.at[1 - core, blk], zbuf.at[tp, blk], load_sem.at[1], z_recv.at[0], {"tp": partner}
        ).start()

    def half_of(c):
        top = c * span // half_rows
        return top, slice(c * span - top * half_rows, (c + 1) * span - top * half_rows)

    def cross(blk, src):
        for k in range(1, n_chip):
            for h in (core, 1 - core):
                remote(
                    src.at[h], zbuf.at[tp, blk], load_sem.at[1], z_recv.at[1 + (k - 1) * n_blk + blk],
                    {"tp": 2 * lax.rem(chip + k, n_chip) + h},
                ).start()

    def reach(i, old, new):
        count = new - old if pair == 1 else jnp.where(sp_b == 0, new - old, (new - old) // pair)
        pl.when(count > 0)(lambda: pl.semaphore_wait(met.at[i], count))

    def take(blk):
        for k in range(1, n_chip):
            c = lax.rem(chip + k, n_chip)
            landed(urecv.at[pl.ds(2 * c, 2), blk], a_recv.at[1 + (k - 1) * n_blk + blk])
        for k in range(1, n_chip):
            drive(lax.rem(chip + k, n_chip), blk)

    close = jnp.minimum(sp + 1 + half, n_sp)

    def give(blk):
        er, ei = seeds(blk)[n_chip]
        e_send[blk] = jnp.concatenate([er, ei], axis=0).astype(BF16)

    def post(blk):
        if blk == 0:
            reach(0, sp + 1, close)
            send_ends([0], sp + 1, close)
            return
        if blk == 1:
            reach(1, close, n_sp)
        send_ends([blk], sp + 1, close)
        send_ends(range(2) if blk == 1 else [blk], close, n_sp)

    @pl.when(sp == 0)
    def _():
        for blk in range(n_blk):
            take(blk)
            give(blk)
            if blk != 1:
                post(blk)
            else:
                send_ends([1], sp + 1, close)
            scan(blk)
            readout(blk)
            finish(blk, None)
            if blk == 1:
                reach(1, close, n_sp)
                send_ends(range(2), close, n_sp)

    @pl.when(sp > 0)
    def _():
        for blk in range(n_blk + 2):
            if blk < n_blk:
                take(blk)
            if blk == n_blk - 1:
                give(blk)
                post(blk)
            if 1 <= blk <= n_blk:
                scan(blk - 1)
            if 2 <= blk:
                readout(blk - 2)
            if blk < n_blk - 1:
                give(blk)
                post(blk)
            if blk - 2 == early:
                for c in range(n_chip):
                    top, to = half_of(c)
                    yst[top, to] = ylocal[early][c * span : (c + 1) * span].astype(BF16)
                cross(early, yst)

    def after(blk):
        cut = slice(blk * lanes, (blk + 1) * lanes)
        lr, li = l_ref[blk, 0:1], l_ref[blk, 1:2]

        def join(j, held):
            e = e_all[blk, j].astype(F32)
            hr, hi = cmul(*held, lr, li)
            return hr + e[0:1], hi + e[1:2]

        for s in range(1, n_sp):
            pl.when(sp == s)(functools.partial(landed, e_all.at[blk, pl.ds(0, s)], e_rsem.at[blk]))
        nil = jnp.zeros((1, lanes), F32)
        hr, hi = lax.fori_loop(0, sp, join, (nil, nil))
        hr, hi = cmul(hr, hi, l_ref[blk, 2:3], l_ref[blk, 3:4])
        if blk == early:
            begin[...] = jnp.concatenate([hr, hi], axis=0).astype(BF16)
            across(lambda h, j: remote(begin, xbegin.at[tp], load_sem.at[4], x_sem.at[2], {"tp": j}).start())
        xr, xi = cmul(hr, hi, t2r[:, cut], t2i[:, cut])
        x = jnp.concatenate([xr.astype(BF16), xi.astype(BF16)], axis=1)
        finish(blk, jnp.dot(x, cs[blk], preferred_element_type=F32))


    @pl.when(sp > 0)
    def _():
        for blk in range(n_blk):
            after(blk)

    @pl.when(sp > 0)
    def _():
        landed(xct.at[pl.ds(0, n_tp - 2)], x_sem.at[0])
        landed(xlam.at[pl.ds(0, n_tp - 2)], x_sem.at[1])
        for k in range(1, n_chip):
            for h in range(2):
                j = 2 * lax.rem(chip + n_chip - k, n_chip) + h
                for c in range(half_chips):
                    widen(xcs.at[2 * (k - 1) + h], xct[j, c].astype(F32), c)

    def correct(k, c2):
        if k == 1:
            landed(xbegin.at[pl.ds(0, n_tp - 2)], x_sem.at[2])
        fixed = []
        for h in range(2):
            j = c2 + h
            first = xbegin[j].astype(F32)
            lr, li, pr, pi = (
                jnp.broadcast_to(part[i : i + 1], (8, lanes)) for part in (xlam[j], first) for i in range(2)
            )
            row = lax.broadcasted_iota(jnp.int32, (8, lanes), 0)
            for bit in range(3):
                on = lax.rem(row // (1 << bit), 2) == 1
                ar, ai = cmul(pr, pi, lr, li)
                pr, pi = jnp.where(on, ar, pr), jnp.where(on, ai, pi)
                lr, li = cmul(lr, li, lr, li)
            pieces = [(pr, pi)]
            while len(pieces) < span // 8:
                pieces += [cmul(*p, lr, li) for p in pieces[: span // 8 - len(pieces)]]
                lr, li = cmul(lr, li, lr, li)
            x = jnp.concatenate(
                [jnp.concatenate([p[i] for p in pieces], axis=0).astype(BF16) for i in range(2)], axis=1
            )
            fixed.append(jnp.dot(x, xcs[2 * (k - 1) + h], preferred_element_type=F32))
        held = [zbuf[c2 + h, early].astype(F32) for h in range(2)]
        for h in range(2):
            y = jnp.concatenate([fixed[h][:, c * LANES : (c + 1) * LANES] for c in range(half_chips)], axis=0)
            held[h] = jax.nn.gelu(held[h] + y).astype(BF16)
        for h in range(2):
            zbuf[c2 + h, early] = held[h]

    loaded(5)

    def project(ref, i, j, blks):
        at = pl.ds(pl.multiple_of(j * width + blks[0] * LANES, LANES), LANES * len(blks))
        z = jnp.concatenate([ref[i, blk] for blk in blks], axis=1)
        return z, at

    def products(*parts):
        z = jnp.concatenate([p[0] for p in parts], axis=1)
        return [
            [
                jnp.dot(
                    z, jnp.concatenate([w[q, i, p[1], :] for p in parts], axis=0), preferred_element_type=F32
                )
                for i in range(2)
            ]
            for q in range(2)
        ]

    def add(new):
        for q in range(2):
            for i in range(2):
                acc[q, i] += new[q][i]

    landed(w.at[1 - core], w_sem.at[1])
    every = range(n_blk)
    new = products(project(zst, core, tp, every))
    for q in range(2):
        for i in range(2):
            acc[q, i] = new[q][i]
    landed(zbuf.at[partner], z_recv.at[0])
    add(products(project(zbuf, partner, partner, every)))
    for blk in range(n_blk):
        for k in range(1, n_chip):
            c2 = 2 * lax.rem(chip + n_chip - k, n_chip)
            landed(zbuf.at[pl.ds(c2, 2), blk], z_recv.at[1 + (k - 1) * n_blk + blk])
            if blk == early:
                pl.when(sp > 0)(functools.partial(correct, k, c2))
            new = products(*(project(zbuf, c2 + h, c2 + h, [blk]) for h in range(2)))
            if blk < n_blk - 1 or k < n_chip - 1:
                add(new)
    part = None
    for q in range(2):
        v, g = (acc[q, i] + new[q][i] for i in range(2))
        gated = v * (0.5 + 0.5 * jnp.tanh(0.5 * g))
        both[q] = gated
        square = gated * gated
        for blk in range(n_blk):
            piece = square[:, blk * LANES : (blk + 1) * LANES]
            part = piece if part is None else part + piece
    remote(both.at[1 - core], swapped, q_sem.at[1], q_sem.at[2], {"tp": partner}).start()
    sums = jnp.sum(part, axis=1, keepdims=True)
    lane = lax.broadcasted_iota(jnp.int32, (8, LANES), 1)
    total = jnp.zeros((8, LANES), F32)
    for k in range(half_rows // 8):
        total = jnp.where(lane == k, sums[8 * k : 8 * k + 8], total)
    sq_all[tp] = total
    for k in range(1, n_tp):
        j = lax.rem(tp + n_tp - k, n_tp)
        remote(sq_all.at[tp], sq_all.at[tp], load_sem.at[5], q_sem.at[0], {"tp": j}).start()
    gone(nsend.at[pl.ds(0, n_tp - 1)], load_sem.at[0])
    gone(zbuf.at[pl.ds(0, n_tp - 1)], load_sem.at[1])
    gone(w.at[core], w_sem.at[0])

    @pl.when(sp > 0)
    def _():
        gone(xct.at[pl.ds(0, n_tp - 2)], load_sem.at[2])
        gone(xlam.at[pl.ds(0, n_tp - 2)], load_sem.at[3])
        gone(xbegin.at[pl.ds(0, n_tp - 2)], load_sem.at[4])

    for s in range(n_sp - 1):
        pl.when(sp == s)(functools.partial(gone, e_all.at[:, pl.ds(0, n_sp - 1 - s)], e_ssem.at[0]))
    both[core] = both[core] * nout[...]
    landed(swapped, q_sem.at[2])
    swapped[...] = swapped[...] * nout[...]
    landed(sq_all.at[pl.ds(0, n_tp - 1)], q_sem.at[0])
    for h in (core, 1 - core):
        total = sq_all[h]
        for c in range(1, n_chip):
            total = total + sq_all[2 * c + h]
        scale = lax.rsqrt(total / d_model + NORM_EPS)
        column = jnp.concatenate([scale[:, i : i + 1] for i in range(half_rows // 8)], axis=0)
        gated = both[core] if h is core else swapped[...]
        at = pl.ds(pl.multiple_of(h * half_rows, half_rows), half_rows)
        out[at, :] = (gated * column).astype(BF16)

    gone(sq_all.at[pl.ds(0, n_tp - 1)], load_sem.at[5])
    gone(swapped, q_sem.at[1])


def solution(mesh):
    n_sp, n_tp = mesh.shape["sp"], mesh.shape["tp"]

    def on_device(
        tokens, norm_in, decay_log, phase, b_real, b_imag, c_real, c_imag, skip_gain, w_value, w_gate, norm_out
    ):
        mine, d_model = tokens.shape
        rows = mine * n_tp
        groups, state, group = b_real.shape
        width = groups * group
        n_blk = width // LANES
        lanes = LANES // group * state
        entries = groups * state
        n_chip = n_tp // 2
        span = 2 * mine
        vmem = pl.BlockSpec(memory_space=pltpu.VMEM)
        hbm = pl.BlockSpec(memory_space=pl.ANY)
        dma = pltpu.SemaphoreType.DMA
        return pl.pallas_call(
            functools.partial(layer, n_sp, n_tp, state, group),
            out_shape=pltpu.VMEM((rows, width), BF16),
            in_specs=[hbm] * 12,
            out_specs=vmem,
            scratch_shapes=[
                pltpu.VMEM((n_tp, n_blk, mine, LANES), BF16),
                pltpu.VMEM((n_tp, n_blk, mine, LANES), BF16),
                pltpu.VMEM((8, entries), F32),
                pltpu.VMEM((8, entries), F32),
                pltpu.VMEM((span, entries), F32),
                pltpu.VMEM((span, entries), F32),
                pltpu.VMEM((span, entries), F32),
                pltpu.VMEM((span, entries), F32),
                pltpu.VMEM((n_blk, LANES, 2 * lanes), BF16),
                pltpu.VMEM((n_blk, 2 * lanes, n_chip * LANES), BF16),
                [pltpu.VMEM((n_chip, span, 2 * lanes), BF16)] * n_blk,
                [pltpu.VMEM((rows, 2 * lanes), BF16)] * n_blk,
                [pltpu.VMEM((n_chip, 2, lanes), F32)] * n_blk,
                [pltpu.VMEM((rows, LANES), F32)] * n_blk,
                pltpu.VMEM((n_blk, 2, lanes), BF16),
                pltpu.VMEM((n_blk, n_sp, 2, lanes), BF16),
                pltpu.VMEM((n_blk, 8, lanes), F32),
                pltpu.VMEM((2, n_blk, rows // 2, LANES), BF16),
                pltpu.VMEM((n_tp, n_blk, rows // 2, LANES), BF16),
                pltpu.VMEM((2, 2) + w_value.shape, BF16),
                pltpu.VMEM((2, 2, rows // 2, width), F32),
                pltpu.VMEM((2, rows // 2, width), F32),
                pltpu.VMEM((rows // 2, width), F32),
                pltpu.VMEM((n_tp, 8, LANES), F32),
                pltpu.VMEM((n_chip, 2 * state, LANES), BF16),
                pltpu.VMEM((n_tp, n_chip // 2, 2 * state, LANES), BF16),
                pltpu.VMEM((n_tp - 2, 2 * lanes, n_chip // 2 * LANES), BF16),
                pltpu.VMEM((2, rows // 2, LANES), BF16),
                pltpu.VMEM((2, lanes), F32),
                pltpu.VMEM((n_tp, 2, lanes), F32),
                pltpu.VMEM((2, lanes), BF16),
                pltpu.VMEM((n_tp, 2, lanes), BF16),
                pltpu.VMEM((4, width, state), F32),
                pltpu.VMEM((mine, d_model), BF16),
                pltpu.VMEM((1, d_model), F32),
                pltpu.VMEM((2, groups, state), F32),
                pltpu.VMEM((2, 1, width), F32),
                dma((6,)),
                dma((1 + (n_chip - 1) * n_blk,)),
                dma((1,)),
                dma((n_blk,)),
                dma((1 + (n_chip - 1) * n_blk,)),
                dma((2,)),
                dma((3,)),
                dma((3,)),
                pltpu.SemaphoreType.REGULAR((2,)),
            ],
            compiler_params=pltpu.CompilerParams(collective_id=0, has_side_effects=True),
        )(
            tokens,
            norm_in.reshape(1, -1),
            decay_log,
            phase,
            b_real.transpose(0, 2, 1).reshape(width, state),
            b_imag.transpose(0, 2, 1).reshape(width, state),
            c_real.reshape(width, state),
            c_imag.reshape(width, state),
            skip_gain.reshape(1, -1),
            w_value,
            w_gate,
            norm_out.reshape(1, -1),
        )

    placed = (
        P(("sp", "tp"), None),
        P(),
        P("tp", None),
        P("tp", None),
        P("tp", None, None),
        P("tp", None, None),
        P("tp", None, None),
        P("tp", None, None),
        P("tp"),
        P(None, "tp"),
        P(None, "tp"),
        P("tp"),
    )
    return jax.shard_map(
        on_device, mesh=mesh, in_specs=placed, out_specs=P("sp", "tp"), check_vma=False
    )
```

```python
import functools

import jax
import jax.numpy as jnp
from jax import lax
from jax.experimental import pallas as pl
from jax.experimental.pallas import tpu as pltpu
from jax.sharding import PartitionSpec as P

NORM_EPS = 1e-06
LANES = 128
F32 = jnp.float32
BF16 = jnp.bfloat16


def cmul(ar, ai, br, bi):
    return ar * br - ai * bi, ar * bi + ai * br


def cpow(r, i, n):
    outr, outi = None, None
    while n:
        if n % 2:
            outr, outi = (r, i) if outr is None else cmul(outr, outi, r, i)
        n //= 2
        if n:
            r, i = cmul(r, i, r, i)
    return outr, outi


def remote(src, dst, send, recv, target):
    return pltpu.make_async_remote_copy(
        src_ref=src,
        dst_ref=dst,
        send_sem=send,
        recv_sem=recv,
        device_id=target,
        device_id_type=pl.DeviceIdType.MESH,
    )


def layer(
    n_sp, n_tp, state, group,
    tok_h, nin_h, dlog_h, phase_h, bre_h, bim_h, cre_h, cim_h, skip_h, wv_h, wg_h, nout_h,
    out,
    nsend, urecv, rows_a, rows_p, t1r, t1i, t2r, t2i, bs, cs, wbuf, xbuf, wsum, ylocal,
    e_send, e_all, l_ref, zst, zbuf, w, acc, both, swapped, sq_all, ct, xct, xcs, yst, lam, xlam, begin, xbegin,
    bc, tok, nin, ap, sn,
    load_sem, a_recv, e_ssem, e_rsem, z_recv, w_sem, q_sem, x_sem, met,
):
    sp, tp = lax.axis_index("sp"), lax.axis_index("tp")
    mine, d_model = tok.shape
    rows, width = out.shape
    half_rows = rows // 2
    n_blk = width // LANES
    per = LANES // group
    lanes = per * state
    core = lax.rem(tp, 2)
    chip = tp // 2
    partner = tp + 1 - 2 * core
    n_chip = n_tp // 2
    span = 2 * mine
    pair = 2 if n_sp % 2 == 0 else 1
    sp_b = lax.rem(sp, pair)
    n_early = min(2, n_blk)
    half_chips = n_chip // 2

    parts = [pl.ds(i * width, width) for i in range(n_tp)]

    def load(i, *pairs):
        return [pltpu.make_async_copy(src, dst, load_sem.at[i]) for src, dst in pairs]

    loads = [
        load(0, *((tok_h.at[:, part], tok.at[:, part]) for part in parts)),
        load(1, (nin_h, nin)),
        load(2, (dlog_h, ap.at[0]), (phase_h, ap.at[1])),
        load(3, *((src, bc.at[i]) for i, src in enumerate((bre_h, bim_h, cre_h, cim_h)))),
        load(4, (skip_h, sn.at[0]), (nout_h, sn.at[1])),
        load(5, (wv_h, w.at[core, 0]), (wg_h, w.at[core, 1])),
    ]

    def start(*which):
        for i in which:
            for copy in loads[i]:
                copy.start()

    def loaded(*which):
        for i in which:
            dst = (tok, nin, ap, bc, sn, w.at[core])[i]
            pltpu.make_async_copy(dst, dst, load_sem.at[i]).wait()

    start(0, 1, 2)

    barrier = pltpu.get_barrier_semaphore()

    def tell(sem, axis):
        def go(j, c):
            pl.semaphore_signal(sem, inc=1, device_id={axis: j}, device_id_type=pl.DeviceIdType.MESH)
            return c

        return go

    def above(go):
        for b in range(pair):
            first = sp // pair + jnp.where(b > sp_b, 0, 1)
            go_b = lambda a, c, b=b: go(a * pair + b, c)
            lax.fori_loop(jnp.where(b >= sp_b, first, n_sp // pair), n_sp // pair, go_b, 0)

    def below(go):
        for b in range(pair):
            last = sp // pair + jnp.where(b < sp_b, 1, 0)
            lax.fori_loop(0, jnp.where(b <= sp_b, last, 0), lambda a, c, b=b: go(a * pair + b, c), 0)

    last = sp == n_sp - 1
    lax.fori_loop(jnp.where(last, tp + 1, 0), jnp.where(last, tp + 1, tp), tell(barrier, "tp"), 0)
    lax.fori_loop(tp + 1, n_tp, tell(barrier, "tp"), 0)
    above(tell(barrier, "sp"))
    start(3, 4)
    known = (sp // pair + 1) * (sp_b + 1) - 1 + jnp.where(last, tp, n_tp - 1)
    half = (n_sp // 2 + pair - 1) // pair * pair

    def enter():
        pl.when(known > 0)(lambda: pl.semaphore_wait(barrier, known))
        below(lambda j, c: tell(met.at[jnp.where(sp - j > half, 1, 0)], "sp")(j, c))
        lax.fori_loop(0, jnp.where(last, tp, 0), tell(met.at[0], "tp"), 0)

    pl.when(last)(enter)
    loaded(0, 1)

    xf = tok[...].astype(F32)
    scale = lax.rsqrt(jnp.sum(xf * xf, axis=1, keepdims=True) / d_model + NORM_EPS)
    normed = (xf * scale * nin[...]).astype(BF16)
    for j in range(n_tp):
        for blk in range(n_blk):
            at = j * width + blk * LANES
            nsend[j, blk] = normed[:, at : at + LANES]

    pl.when(jnp.logical_not(last))(enter)
    pl.when(last & (tp < n_tp - 1))(lambda: pl.semaphore_wait(met.at[0], n_tp - 1 - tp))


    def scatter(j, blk, at):
        remote(nsend.at[j, blk], urecv.at[tp, blk], load_sem.at[0], a_recv.at[at], {"tp": j}).start()

    for blk in range(n_blk):
        for k in range(1, n_chip):
            other = lax.rem(chip + n_chip - k, n_chip)
            for j in (2 * other + core, 2 * other + 1 - core):
                scatter(j, blk, 1 + (k - 1) * n_blk + blk)
        if blk == 0:
            for b in range(n_blk):
                scatter(partner, b, 0)
    start(5)
    for i, src in enumerate((wv_h, wg_h)):
        remote(src, w.at[core, i], w_sem.at[0], w_sem.at[1], {"tp": partner}).start()
    urecv[tp] = nsend[tp]

    loaded(2)
    dlog, phase, skip, nout = ap.at[0], ap.at[1], sn.at[0], sn.at[1]
    bre, bim, cre, cim = (bc.at[i] for i in range(4))
    side = LANES // state
    for i in range(width // group // side):
        cut = slice(i * LANES, (i + 1) * LANES)
        for src, dst in ((dlog, rows_a), (phase, rows_p)):
            row = jnp.concatenate([src[i * side + k : i * side + k + 1, :] for k in range(side)], axis=1)
            dst[:, cut] = jnp.broadcast_to(row, (8, LANES))

    for blk in range(n_blk):
        cut = slice(blk * lanes, (blk + 1) * lanes)
        a, p = rows_a[:, cut], rows_p[:, cut]
        mag, cos, sin = jnp.exp(a), jnp.cos(p), jnp.sin(p)
        lr, li = mag * cos, mag * sin
        inv = jnp.exp(-a)
        nr, ni = inv * cos, -inv * sin
        mod = a * a + p * p
        cr = ((lr - 1.0) * a + li * p) / mod
        ci = (li * a - (lr - 1.0) * p) / mod
        one, zero = jnp.ones_like(a), jnp.zeros_like(a)
        pr, pi, mr, mi = one, zero, cr, ci
        sr, si, qr, qi = lr, li, nr, ni
        row = lax.broadcasted_iota(jnp.int32, a.shape, 0)
        for bit in range(3):
            on = lax.rem(row // (1 << bit), 2) == 1
            ar, ai = cmul(pr, pi, sr, si)
            pr, pi = jnp.where(on, ar, pr), jnp.where(on, ai, pi)
            ar, ai = cmul(mr, mi, qr, qi)
            mr, mi = jnp.where(on, ar, mr), jnp.where(on, ai, mi)
            sr, si = cmul(sr, si, sr, si)
            qr, qi = cmul(qr, qi, qr, qi)
        t2r[0:8, cut], t2i[0:8, cut], t1r[0:8, cut], t1i[0:8, cut] = pr, pi, mr, mi
        done = 8
        while done < span:
            more = min(done, span - done)
            for off in range(0, more, 8):
                src, dst = slice(off, off + 8), slice(done + off, done + off + 8)
                t2r[dst, cut], t2i[dst, cut] = cmul(t2r[src, cut], t2i[src, cut], sr, si)
                t1r[dst, cut], t1i[dst, cut] = cmul(t1r[src, cut], t1i[src, cut], qr, qi)
            sr, si = cmul(sr, si, sr, si)
            qr, qi = cmul(qr, qi, qr, qi)
            done += more
        endr, endi = t2r[span - 1 : span, cut], t2i[span - 1 : span, cut]
        wholer, wholei = cmul(endr, endi, lr[0:1], li[0:1])
        allr, alli = cpow(wholer, wholei, n_chip)
        for k, value in enumerate((allr, alli, lr[0:1], li[0:1], wholer, wholei, endr, endi)):
            l_ref[blk, k : k + 1, :] = value

    loaded(3, 4)
    keep_b = (
        lax.broadcasted_iota(jnp.int32, (LANES, lanes), 0) // group
        == lax.broadcasted_iota(jnp.int32, (LANES, lanes), 1) // state
    )
    of_col = lax.broadcasted_iota(jnp.int32, (state, LANES), 1) // group
    a, p = dlog[...], phase[...]
    mag = jnp.exp(a)
    stepr, stepi = cpow(mag * jnp.cos(p), mag * jnp.sin(p), span)

    def widen(dst, turned, c):
        for part in range(2):
            piece = turned[part * state : (part + 1) * state]
            for g in range(per):
                at = part * lanes + g * state
                dst[at : at + state, c * LANES : (c + 1) * LANES] = jnp.where(of_col == g, piece, 0.0).astype(BF16)

    for blk in range(n_blk):
        ch = slice(blk * LANES, (blk + 1) * LANES)
        for part, in_ref in ((0, bre), (1, bim)):
            b = in_ref[ch, :]
            b = jnp.concatenate([b] * side, axis=1)
            wide = jnp.where(keep_b, jnp.concatenate([b] * (lanes // LANES), axis=1), 0.0)
            bs[blk, :, part * lanes : (part + 1) * lanes] = wide.astype(BF16)
        c_r, c_i = cre[ch, :], cim[ch, :]
        if n_chip > 1:
            spread = [
                jnp.concatenate(
                    [jnp.broadcast_to(s[g : g + 1], (group, state)) for g in range(blk * per, (blk + 1) * per)],
                    axis=0,
                )
                for s in (stepr, stepi)
            ]
        for c in range(n_chip):
            if c:
                c_r, c_i = cmul(c_r, c_i, *spread)
            turned = jnp.concatenate([c_r, -c_i], axis=1).T
            if blk < n_early:
                ct[blk, c] = turned.astype(BF16)
            widen(cs.at[blk], turned, c)
    def across(start):
        for k in range(1, n_chip):
            for h in range(2):
                start(h, 2 * lax.rem(chip + k, n_chip) + h)

    def slot(k, h, b):
        return (k - 1) * (1 + n_early) + (n_early if h else b)

    def share(b):
        lam[b] = l_ref[b, 2:4]
        across(
            lambda h, j: remote(
                ct.at[b, pl.ds(h * half_chips, half_chips)], xct.at[tp * n_early + b], load_sem.at[2], x_sem.at[0],
                {"tp": j},
            ).start()
        )
        across(
            lambda h, j: remote(
                lam.at[b], xlam.at[tp * n_early + b], load_sem.at[3], x_sem.at[1], {"tp": j}
            ).start()
        )

    @pl.when(sp > 0)
    def _():
        share(0)
        for b in range(1, n_early):
            pl.when(core == 0)(functools.partial(share, b))

    lower = (
        lax.broadcasted_iota(jnp.int32, (span, span), 0)
        >= lax.broadcasted_iota(jnp.int32, (span, span), 1)
    ).astype(BF16)

    def landed(ref, sem):
        remote(ref, ref, load_sem.at[0], sem, {"tp": partner}).wait_recv()

    def gone(ref, sem):
        remote(ref, ref, sem, a_recv.at[0], {"tp": partner}).wait_send()

    def source(c, blk):
        return jnp.concatenate([urecv[2 * c + s, blk].astype(F32) for s in range(2)], axis=0)

    def drive(c, blk):
        cut = slice(blk * lanes, (blk + 1) * lanes)
        d = jnp.dot(source(c, blk).astype(BF16), bs[blk], preferred_element_type=F32)
        wr, wi = cmul(d[:, :lanes], d[:, lanes:], t1r[:, cut], t1i[:, cut])
        wbuf[blk][c, :, :lanes] = wr.astype(BF16)
        wbuf[blk][c, :, lanes:] = wi.astype(BF16)
        wsum[blk][c, 0:1, :] = jnp.sum(wr, axis=0, keepdims=True)
        wsum[blk][c, 1:2, :] = jnp.sum(wi, axis=0, keepdims=True)

    def seeds(blk):
        turn = l_ref[blk, 4:5], l_ref[blk, 5:6]
        held = [None]
        for c in range(n_chip):
            r, i = wsum[blk][c, 0:1], wsum[blk][c, 1:2]
            if c:
                r, i = r + held[c][0], i + held[c][1]
            held.append(cmul(r, i, *turn) if c < n_chip - 1 else cmul(r, i, l_ref[blk, 6:7], l_ref[blk, 7:8]))
        return held

    def end_copy(j, blk):
        return remote(e_send.at[blk], e_all.at[blk, sp], e_ssem.at[0], e_rsem.at[blk], {"sp": j})

    def scan(blk):
        cut = slice(blk * lanes, (blk + 1) * lanes)
        held = seeds(blk)
        for c in range(n_chip):
            s = jnp.dot(lower, wbuf[blk][c], preferred_element_type=F32)
            sr, si = s[:, :lanes], s[:, lanes:]
            if c:
                sr, si = sr + held[c][0], si + held[c][1]
            xr, xi = cmul(sr, si, t2r[:, cut], t2i[:, cut])
            at = slice(c * span, (c + 1) * span)
            xbuf[blk][at, :lanes] = xr.astype(BF16)
            xbuf[blk][at, lanes:] = xi.astype(BF16)

    def readout(blk):
        ch = slice(blk * LANES, (blk + 1) * LANES)
        y = jnp.dot(xbuf[blk][...], cs[blk, :, :LANES], preferred_element_type=F32)
        for c in range(n_chip):
            at = slice(c * span, (c + 1) * span)
            ylocal[blk][at] = y[at] + skip[:, ch] * source(c, blk)

    landed(urecv.at[partner], a_recv.at[0])
    for blk in range(n_blk):
        drive(chip, blk)

    def send_ends(blks, first, last):
        def go(j, c):
            for blk in blks:
                end_copy(j, blk).start()
            return c

        lax.fori_loop(first, last, go, 0)

    def finish(blk, y):
        for c in range(n_chip):
            at = slice(c * span, (c + 1) * span)
            v = ylocal[blk][at]
            if y is not None:
                v = v + y[:, c * LANES : (c + 1) * LANES]
            top, to = half_of(c)
            zst[top, blk, to] = jax.nn.gelu(v).astype(BF16)
        if y is None or blk >= n_early:
            cross(blk, zst.at[:, blk])
        elif blk:
            pl.when(core == 1)(lambda: cross(blk, zst.at[:, blk]))
        remote(
            zst.at[1 - core, blk], zbuf.at[tp, blk], load_sem.at[1], z_recv.at[0], {"tp": partner}
        ).start()

    def half_of(c):
        top = c * span // half_rows
        return top, slice(c * span - top * half_rows, (c + 1) * span - top * half_rows)

    def ahead(b):
        for c in range(n_chip):
            top, to = half_of(c)
            yst[b, top, to] = ylocal[b][c * span : (c + 1) * span].astype(BF16)
        cross(b, yst.at[b])

    def cross(blk, src):
        for k in range(1, n_chip):
            for h in (core, 1 - core):
                remote(
                    src.at[h], zbuf.at[tp, blk], load_sem.at[1], z_recv.at[1 + (k - 1) * n_blk + blk],
                    {"tp": 2 * lax.rem(chip + k, n_chip) + h},
                ).start()

    def reach(i, old, new):
        count = new - old if pair == 1 else jnp.where(sp_b == 0, new - old, (new - old) // pair)
        pl.when(count > 0)(lambda: pl.semaphore_wait(met.at[i], count))

    def take(blk):
        for k in range(1, n_chip):
            c = lax.rem(chip + k, n_chip)
            landed(urecv.at[pl.ds(2 * c, 2), blk], a_recv.at[1 + (k - 1) * n_blk + blk])
        for k in range(1, n_chip):
            drive(lax.rem(chip + k, n_chip), blk)

    close = jnp.minimum(sp + 1 + half, n_sp)

    def give(blk):
        er, ei = seeds(blk)[n_chip]
        e_send[blk] = jnp.concatenate([er, ei], axis=0).astype(BF16)

    def post(blk):
        if blk == 0:
            reach(0, sp + 1, close)
            send_ends([0], sp + 1, close)
            return
        if blk == 1:
            reach(1, close, n_sp)
        send_ends([blk], sp + 1, close)
        send_ends(range(2) if blk == 1 else [blk], close, n_sp)

    @pl.when(sp == 0)
    def _():
        for blk in range(n_blk):
            take(blk)
            give(blk)
            if blk != 1:
                post(blk)
            else:
                send_ends([1], sp + 1, close)
            scan(blk)
            readout(blk)
            finish(blk, None)
            if blk == 1:
                reach(1, close, n_sp)
                send_ends(range(2), close, n_sp)

    @pl.when(sp > 0)
    def _():
        for blk in range(n_blk + 2):
            if blk < n_blk:
                take(blk)
            if blk == n_blk - 1:
                give(blk)
                post(blk)
            if 1 <= blk <= n_blk:
                scan(blk - 1)
            if 2 <= blk:
                readout(blk - 2)
            if blk < n_blk - 1:
                give(blk)
                post(blk)
            if blk - 2 == 0:
                ahead(0)
            elif 0 < blk - 2 < n_early:
                pl.when(core == 0)(functools.partial(ahead, blk - 2))

    def after(blk):
        cut = slice(blk * lanes, (blk + 1) * lanes)
        lr, li = l_ref[blk, 0:1], l_ref[blk, 1:2]

        def join(j, held):
            e = e_all[blk, j].astype(F32)
            hr, hi = cmul(*held, lr, li)
            return hr + e[0:1], hi + e[1:2]

        for s in range(1, n_sp):
            pl.when(sp == s)(functools.partial(landed, e_all.at[blk, pl.ds(0, s)], e_rsem.at[blk]))
        nil = jnp.zeros((1, lanes), F32)
        hr, hi = lax.fori_loop(0, sp, join, (nil, nil))
        hr, hi = cmul(hr, hi, l_ref[blk, 2:3], l_ref[blk, 3:4])

        def tell_begin():
            begin[blk] = jnp.concatenate([hr, hi], axis=0).astype(BF16)
            across(
                lambda h, j: remote(
                    begin.at[blk], xbegin.at[tp * n_early + blk], load_sem.at[4], x_sem.at[2 + blk], {"tp": j}
                ).start()
            )

        if blk == 0:
            tell_begin()
        elif blk < n_early:
            pl.when(core == 0)(tell_begin)
        xr, xi = cmul(hr, hi, t2r[:, cut], t2i[:, cut])
        x = jnp.concatenate([xr.astype(BF16), xi.astype(BF16)], axis=1)
        finish(blk, jnp.dot(x, cs[blk], preferred_element_type=F32))


    @pl.when(sp > 0)
    def _():
        for blk in range(n_blk):
            after(blk)

    @pl.when(sp > 0)
    def _():
        for ref, sem in ((xct, 0), (xlam, 1)):
            landed(ref.at[pl.ds(0, (n_chip - 1) * (1 + n_early))], x_sem.at[sem])
        for k in range(1, n_chip):
            for h in range(2):
                j = 2 * lax.rem(chip + n_chip - k, n_chip) + h
                for b in range(1 if h else n_early):
                    for c in range(half_chips):
                        widen(xcs.at[slot(k, h, b)], xct[j * n_early + b, c].astype(F32), c)

    def correct(k, c2, b):
        heads = range(1 if b else 2)
        if k == 1:
            landed(xbegin.at[pl.ds(0, (n_chip - 1) * len(heads))], x_sem.at[2 + b])
        fixed = []
        for h in heads:
            j = (c2 + h) * n_early + b
            first = xbegin[j].astype(F32)
            lr, li, pr, pi = (
                jnp.broadcast_to(part[i : i + 1], (8, lanes)) for part in (xlam[j], first) for i in range(2)
            )
            row = lax.broadcasted_iota(jnp.int32, (8, lanes), 0)
            for bit in range(3):
                on = lax.rem(row // (1 << bit), 2) == 1
                ar, ai = cmul(pr, pi, lr, li)
                pr, pi = jnp.where(on, ar, pr), jnp.where(on, ai, pi)
                lr, li = cmul(lr, li, lr, li)
            pieces = [(pr, pi)]
            while len(pieces) < span // 8:
                pieces += [cmul(*p, lr, li) for p in pieces[: span // 8 - len(pieces)]]
                lr, li = cmul(lr, li, lr, li)
            x = jnp.concatenate(
                [jnp.concatenate([p[i] for p in pieces], axis=0).astype(BF16) for i in range(2)], axis=1
            )
            fixed.append(jnp.dot(x, xcs[slot(k, h, b)], preferred_element_type=F32))
        held = [zbuf[c2 + h, b].astype(F32) for h in heads]
        for h in heads:
            y = jnp.concatenate([fixed[h][:, c * LANES : (c + 1) * LANES] for c in range(half_chips)], axis=0)
            held[h] = jax.nn.gelu(held[h] + y).astype(BF16)
        for h in heads:
            zbuf[c2 + h, b] = held[h]

    loaded(5)

    def project(ref, i, j, blks):
        at = pl.ds(pl.multiple_of(j * width + blks[0] * LANES, LANES), LANES * len(blks))
        z = jnp.concatenate([ref[i, blk] for blk in blks], axis=1)
        return z, at

    def products(*parts):
        z = jnp.concatenate([p[0] for p in parts], axis=1)
        return [
            [
                jnp.dot(
                    z, jnp.concatenate([w[q, i, p[1], :] for p in parts], axis=0), preferred_element_type=F32
                )
                for i in range(2)
            ]
            for q in range(2)
        ]

    def add(new):
        for q in range(2):
            for i in range(2):
                acc[q, i] += new[q][i]

    landed(w.at[1 - core], w_sem.at[1])
    every = range(n_blk)
    new = products(project(zst, core, tp, every))
    for q in range(2):
        for i in range(2):
            acc[q, i] = new[q][i]
    landed(zbuf.at[partner], z_recv.at[0])
    add(products(project(zbuf, partner, partner, every)))
    for blk in range(n_blk):
        for k in range(1, n_chip):
            c2 = 2 * lax.rem(chip + n_chip - k, n_chip)
            landed(zbuf.at[pl.ds(c2, 2), blk], z_recv.at[1 + (k - 1) * n_blk + blk])
            if blk < n_early:
                pl.when(sp > 0)(functools.partial(correct, k, c2, blk))
            new = products(*(project(zbuf, c2 + h, c2 + h, [blk]) for h in range(2)))
            if blk < n_blk - 1 or k < n_chip - 1:
                add(new)
    part = None
    for q in range(2):
        v, g = (acc[q, i] + new[q][i] for i in range(2))
        gated = v * (0.5 + 0.5 * jnp.tanh(0.5 * g))
        both[q] = gated
        square = gated * gated
        for blk in range(n_blk):
            piece = square[:, blk * LANES : (blk + 1) * LANES]
            part = piece if part is None else part + piece
    remote(both.at[1 - core], swapped, q_sem.at[1], q_sem.at[2], {"tp": partner}).start()
    sums = jnp.sum(part, axis=1, keepdims=True)
    lane = lax.broadcasted_iota(jnp.int32, (8, LANES), 1)
    total = jnp.zeros((8, LANES), F32)
    for k in range(half_rows // 8):
        total = jnp.where(lane == k, sums[8 * k : 8 * k + 8], total)
    sq_all[tp] = total
    for k in range(1, n_tp):
        j = lax.rem(tp + n_tp - k, n_tp)
        remote(sq_all.at[tp], sq_all.at[tp], load_sem.at[5], q_sem.at[0], {"tp": j}).start()
    gone(nsend.at[pl.ds(0, n_tp - 1)], load_sem.at[0])
    gone(zbuf.at[pl.ds(0, n_tp - 1)], load_sem.at[1])
    gone(w.at[core], w_sem.at[0])

    @pl.when(sp > 0)
    def _():
        for h in range(2):

            @pl.when(core == h)
            def _(count=(n_tp - 2) * (1 if h else n_early)):
                for ref, sem in ((xct, 2), (xlam, 3), (xbegin, 4)):
                    gone(ref.at[pl.ds(0, count)], load_sem.at[sem])

    for s in range(n_sp - 1):
        pl.when(sp == s)(functools.partial(gone, e_all.at[:, pl.ds(0, n_sp - 1 - s)], e_ssem.at[0]))
    both[core] = both[core] * nout[...]
    landed(swapped, q_sem.at[2])
    swapped[...] = swapped[...] * nout[...]
    landed(sq_all.at[pl.ds(0, n_tp - 1)], q_sem.at[0])
    for h in (core, 1 - core):
        total = sq_all[h]
        for c in range(1, n_chip):
            total = total + sq_all[2 * c + h]
        scale = lax.rsqrt(total / d_model + NORM_EPS)
        column = jnp.concatenate([scale[:, i : i + 1] for i in range(half_rows // 8)], axis=0)
        gated = both[core] if h is core else swapped[...]
        at = pl.ds(pl.multiple_of(h * half_rows, half_rows), half_rows)
        out[at, :] = (gated * column).astype(BF16)

    gone(sq_all.at[pl.ds(0, n_tp - 1)], load_sem.at[5])
    gone(swapped, q_sem.at[1])


def solution(mesh):
    n_sp, n_tp = mesh.shape["sp"], mesh.shape["tp"]

    def on_device(
        tokens, norm_in, decay_log, phase, b_real, b_imag, c_real, c_imag, skip_gain, w_value, w_gate, norm_out
    ):
        mine, d_model = tokens.shape
        rows = mine * n_tp
        groups, state, group = b_real.shape
        width = groups * group
        n_blk = width // LANES
        lanes = LANES // group * state
        entries = groups * state
        n_chip = n_tp // 2
        n_early = min(2, n_blk)
        span = 2 * mine
        vmem = pl.BlockSpec(memory_space=pltpu.VMEM)
        hbm = pl.BlockSpec(memory_space=pl.ANY)
        dma = pltpu.SemaphoreType.DMA
        return pl.pallas_call(
            functools.partial(layer, n_sp, n_tp, state, group),
            out_shape=pltpu.VMEM((rows, width), BF16),
            in_specs=[hbm] * 12,
            out_specs=vmem,
            scratch_shapes=[
                pltpu.VMEM((n_tp, n_blk, mine, LANES), BF16),
                pltpu.VMEM((n_tp, n_blk, mine, LANES), BF16),
                pltpu.VMEM((8, entries), F32),
                pltpu.VMEM((8, entries), F32),
                pltpu.VMEM((span, entries), F32),
                pltpu.VMEM((span, entries), F32),
                pltpu.VMEM((span, entries), F32),
                pltpu.VMEM((span, entries), F32),
                pltpu.VMEM((n_blk, LANES, 2 * lanes), BF16),
                pltpu.VMEM((n_blk, 2 * lanes, n_chip * LANES), BF16),
                [pltpu.VMEM((n_chip, span, 2 * lanes), BF16)] * n_blk,
                [pltpu.VMEM((rows, 2 * lanes), BF16)] * n_blk,
                [pltpu.VMEM((n_chip, 2, lanes), F32)] * n_blk,
                [pltpu.VMEM((rows, LANES), F32)] * n_blk,
                pltpu.VMEM((n_blk, 2, lanes), BF16),
                pltpu.VMEM((n_blk, n_sp, 2, lanes), BF16),
                pltpu.VMEM((n_blk, 8, lanes), F32),
                pltpu.VMEM((2, n_blk, rows // 2, LANES), BF16),
                pltpu.VMEM((n_tp, n_blk, rows // 2, LANES), BF16),
                pltpu.VMEM((2, 2) + w_value.shape, BF16),
                pltpu.VMEM((2, 2, rows // 2, width), F32),
                pltpu.VMEM((2, rows // 2, width), F32),
                pltpu.VMEM((rows // 2, width), F32),
                pltpu.VMEM((n_tp, 8, LANES), F32),
                pltpu.VMEM((n_early, n_chip, 2 * state, LANES), BF16),
                pltpu.VMEM((n_tp * n_early, n_chip // 2, 2 * state, LANES), BF16),
                pltpu.VMEM(((n_chip - 1) * (1 + n_early), 2 * lanes, n_chip // 2 * LANES), BF16),
                pltpu.VMEM((n_early, 2, rows // 2, LANES), BF16),
                pltpu.VMEM((n_early, 2, lanes), F32),
                pltpu.VMEM((n_tp * n_early, 2, lanes), F32),
                pltpu.VMEM((n_early, 2, lanes), BF16),
                pltpu.VMEM((n_tp * n_early, 2, lanes), BF16),
                pltpu.VMEM((4, width, state), F32),
                pltpu.VMEM((mine, d_model), BF16),
                pltpu.VMEM((1, d_model), F32),
                pltpu.VMEM((2, groups, state), F32),
                pltpu.VMEM((2, 1, width), F32),
                dma((6,)),
                dma((1 + (n_chip - 1) * n_blk,)),
                dma((1,)),
                dma((n_blk,)),
                dma((1 + (n_chip - 1) * n_blk,)),
                dma((2,)),
                dma((3,)),
                dma((2 + n_early,)),
                pltpu.SemaphoreType.REGULAR((2,)),
            ],
            compiler_params=pltpu.CompilerParams(collective_id=0, has_side_effects=True),
        )(
            tokens,
            norm_in.reshape(1, -1),
            decay_log,
            phase,
            b_real.transpose(0, 2, 1).reshape(width, state),
            b_imag.transpose(0, 2, 1).reshape(width, state),
            c_real.reshape(width, state),
            c_imag.reshape(width, state),
            skip_gain.reshape(1, -1),
            w_value,
            w_gate,
            norm_out.reshape(1, -1),
        )

    placed = (
        P(("sp", "tp"), None),
        P(),
        P("tp", None),
        P("tp", None),
        P("tp", None, None),
        P("tp", None, None),
        P("tp", None, None),
        P("tp", None, None),
        P("tp"),
        P(None, "tp"),
        P(None, "tp"),
        P("tp"),
    )
    return jax.shard_map(
        on_device, mesh=mesh, in_specs=placed, out_specs=P("sp", "tp"), check_vma=False
    )
```

```python
import functools

import jax
import jax.numpy as jnp
from jax import lax
from jax.experimental import pallas as pl
from jax.experimental.pallas import tpu as pltpu
from jax.sharding import PartitionSpec as P

NORM_EPS = 1e-06
LANES = 128
F32 = jnp.float32
BF16 = jnp.bfloat16


def cmul(ar, ai, br, bi):
    return ar * br - ai * bi, ar * bi + ai * br


def cpow(r, i, n):
    outr, outi = None, None
    while n:
        if n % 2:
            outr, outi = (r, i) if outr is None else cmul(outr, outi, r, i)
        n //= 2
        if n:
            r, i = cmul(r, i, r, i)
    return outr, outi


def remote(src, dst, send, recv, target):
    return pltpu.make_async_remote_copy(
        src_ref=src,
        dst_ref=dst,
        send_sem=send,
        recv_sem=recv,
        device_id=target,
        device_id_type=pl.DeviceIdType.MESH,
    )


def layer(
    n_sp, n_tp, state, group,
    tok_h, nin_h, dlog_h, phase_h, bre_h, bim_h, cre_h, cim_h, skip_h, wv_h, wg_h, nout_h,
    out,
    nsend, urecv, rows_a, rows_p, t1r, t1i, t2r, t2i, bs, cs, wbuf, xbuf, wsum, ylocal,
    e_send, e_all, l_ref, zst, zbuf, w, acc, both, swapped, sq_all, ct, xct, xcs, yst, lam, xlam, begin, xbegin,
    bc, tok, nin, ap, sn,
    load_sem, a_recv, e_ssem, e_rsem, z_recv, w_sem, q_sem, x_sem, met,
):
    sp, tp = lax.axis_index("sp"), lax.axis_index("tp")
    mine, d_model = tok.shape
    rows, width = out.shape
    half_rows = rows // 2
    n_blk = width // LANES
    per = LANES // group
    lanes = per * state
    core = lax.rem(tp, 2)
    chip = tp // 2
    partner = tp + 1 - 2 * core
    n_chip = n_tp // 2
    span = 2 * mine
    pair = 2 if n_sp % 2 == 0 else 1
    sp_b = lax.rem(sp, pair)
    n_early = min(2, n_blk)
    half_chips = n_chip // 2

    parts = [pl.ds(i * width, width) for i in range(n_tp)]

    def load(i, *pairs):
        return [pltpu.make_async_copy(src, dst, load_sem.at[i]) for src, dst in pairs]

    loads = [
        load(0, *((tok_h.at[:, part], tok.at[:, part]) for part in parts)),
        load(1, (nin_h, nin)),
        load(2, (dlog_h, ap.at[0]), (phase_h, ap.at[1])),
        load(3, *((src, bc.at[i]) for i, src in enumerate((bre_h, bim_h, cre_h, cim_h)))),
        load(4, (skip_h, sn.at[0]), (nout_h, sn.at[1])),
        load(5, (wv_h, w.at[core, 0]), (wg_h, w.at[core, 1])),
    ]

    def start(*which):
        for i in which:
            for copy in loads[i]:
                copy.start()

    def loaded(*which):
        for i in which:
            dst = (tok, nin, ap, bc, sn, w.at[core])[i]
            pltpu.make_async_copy(dst, dst, load_sem.at[i]).wait()

    start(0, 1, 2)

    barrier = pltpu.get_barrier_semaphore()

    def tell(sem, axis):
        def go(j, c):
            pl.semaphore_signal(sem, inc=1, device_id={axis: j}, device_id_type=pl.DeviceIdType.MESH)
            return c

        return go

    def above(go):
        for b in range(pair):
            first = sp // pair + jnp.where(b > sp_b, 0, 1)
            go_b = lambda a, c, b=b: go(a * pair + b, c)
            lax.fori_loop(jnp.where(b >= sp_b, first, n_sp // pair), n_sp // pair, go_b, 0)

    def below(go):
        for b in range(pair):
            last = sp // pair + jnp.where(b < sp_b, 1, 0)
            lax.fori_loop(0, jnp.where(b <= sp_b, last, 0), lambda a, c, b=b: go(a * pair + b, c), 0)

    last = sp == n_sp - 1
    lax.fori_loop(jnp.where(last, tp + 1, 0), jnp.where(last, tp + 1, tp), tell(barrier, "tp"), 0)
    lax.fori_loop(tp + 1, n_tp, tell(barrier, "tp"), 0)
    above(tell(barrier, "sp"))
    start(3, 4)
    known = (sp // pair + 1) * (sp_b + 1) - 1 + jnp.where(last, tp, n_tp - 1)
    half = (n_sp // 2 + pair - 1) // pair * pair

    def enter():
        pl.when(known > 0)(lambda: pl.semaphore_wait(barrier, known))
        below(lambda j, c: tell(met.at[jnp.where(sp - j > half, 1, 0)], "sp")(j, c))
        lax.fori_loop(0, jnp.where(last, tp, 0), tell(met.at[0], "tp"), 0)

    pl.when(last)(enter)
    loaded(0, 1)

    xf = tok[...].astype(F32)
    scale = lax.rsqrt(jnp.sum(xf * xf, axis=1, keepdims=True) / d_model + NORM_EPS)
    normed = (xf * scale * nin[...]).astype(BF16)
    for j in range(n_tp):
        for blk in range(n_blk):
            at = j * width + blk * LANES
            nsend[j, blk] = normed[:, at : at + LANES]

    pl.when(jnp.logical_not(last))(enter)
    pl.when(last & (tp < n_tp - 1))(lambda: pl.semaphore_wait(met.at[0], n_tp - 1 - tp))


    def scatter(j, blk, at):
        remote(nsend.at[j, blk], urecv.at[tp, blk], load_sem.at[0], a_recv.at[at], {"tp": j}).start()

    for blk in range(n_blk):
        for k in range(1, n_chip):
            other = lax.rem(chip + n_chip - k, n_chip)
            for j in (2 * other + core, 2 * other + 1 - core):
                scatter(j, blk, 1 + (k - 1) * n_blk + blk)
        if blk == 0:
            for b in range(n_blk):
                scatter(partner, b, 0)
    start(5)
    for i, src in enumerate((wv_h, wg_h)):
        remote(src, w.at[core, i], w_sem.at[0], w_sem.at[1], {"tp": partner}).start()
    urecv[tp] = nsend[tp]

    loaded(2)
    dlog, phase, skip, nout = ap.at[0], ap.at[1], sn.at[0], sn.at[1]
    bre, bim, cre, cim = (bc.at[i] for i in range(4))
    side = LANES // state
    for i in range(width // group // side):
        cut = slice(i * LANES, (i + 1) * LANES)
        for src, dst in ((dlog, rows_a), (phase, rows_p)):
            row = jnp.concatenate([src[i * side + k : i * side + k + 1, :] for k in range(side)], axis=1)
            dst[:, cut] = jnp.broadcast_to(row, (8, LANES))

    for blk in range(n_blk):
        cut = slice(blk * lanes, (blk + 1) * lanes)
        a, p = rows_a[:, cut], rows_p[:, cut]
        mag, cos, sin = jnp.exp(a), jnp.cos(p), jnp.sin(p)
        lr, li = mag * cos, mag * sin
        inv = jnp.exp(-a)
        nr, ni = inv * cos, -inv * sin
        mod = a * a + p * p
        cr = ((lr - 1.0) * a + li * p) / mod
        ci = (li * a - (lr - 1.0) * p) / mod
        one, zero = jnp.ones_like(a), jnp.zeros_like(a)
        pr, pi, mr, mi = one, zero, cr, ci
        sr, si, qr, qi = lr, li, nr, ni
        row = lax.broadcasted_iota(jnp.int32, a.shape, 0)
        for bit in range(3):
            on = lax.rem(row // (1 << bit), 2) == 1
            ar, ai = cmul(pr, pi, sr, si)
            pr, pi = jnp.where(on, ar, pr), jnp.where(on, ai, pi)
            ar, ai = cmul(mr, mi, qr, qi)
            mr, mi = jnp.where(on, ar, mr), jnp.where(on, ai, mi)
            sr, si = cmul(sr, si, sr, si)
            qr, qi = cmul(qr, qi, qr, qi)
        t2r[0:8, cut], t2i[0:8, cut], t1r[0:8, cut], t1i[0:8, cut] = pr, pi, mr, mi
        done = 8
        while done < span:
            more = min(done, span - done)
            for off in range(0, more, 8):
                src, dst = slice(off, off + 8), slice(done + off, done + off + 8)
                t2r[dst, cut], t2i[dst, cut] = cmul(t2r[src, cut], t2i[src, cut], sr, si)
                t1r[dst, cut], t1i[dst, cut] = cmul(t1r[src, cut], t1i[src, cut], qr, qi)
            sr, si = cmul(sr, si, sr, si)
            qr, qi = cmul(qr, qi, qr, qi)
            done += more
        endr, endi = t2r[span - 1 : span, cut], t2i[span - 1 : span, cut]
        wholer, wholei = cmul(endr, endi, lr[0:1], li[0:1])
        allr, alli = cpow(wholer, wholei, n_chip)
        for k, value in enumerate((allr, alli, lr[0:1], li[0:1], wholer, wholei, endr, endi)):
            l_ref[blk, k : k + 1, :] = value

    loaded(3, 4)
    keep_b = (
        lax.broadcasted_iota(jnp.int32, (LANES, lanes), 0) // group
        == lax.broadcasted_iota(jnp.int32, (LANES, lanes), 1) // state
    )
    of_col = lax.broadcasted_iota(jnp.int32, (state, LANES), 1) // group
    a, p = dlog[...], phase[...]
    mag = jnp.exp(a)
    stepr, stepi = cpow(mag * jnp.cos(p), mag * jnp.sin(p), span)

    def widen(dst, turned, c):
        for part in range(2):
            piece = turned[part * state : (part + 1) * state]
            for g in range(per):
                at = part * lanes + g * state
                dst[at : at + state, c * LANES : (c + 1) * LANES] = jnp.where(of_col == g, piece, 0.0).astype(BF16)

    for blk in range(n_blk):
        ch = slice(blk * LANES, (blk + 1) * LANES)
        for part, in_ref in ((0, bre), (1, bim)):
            b = in_ref[ch, :]
            b = jnp.concatenate([b] * side, axis=1)
            wide = jnp.where(keep_b, jnp.concatenate([b] * (lanes // LANES), axis=1), 0.0)
            bs[blk, :, part * lanes : (part + 1) * lanes] = wide.astype(BF16)
        c_r, c_i = cre[ch, :], cim[ch, :]
        if n_chip > 1:
            spread = [
                jnp.concatenate(
                    [jnp.broadcast_to(s[g : g + 1], (group, state)) for g in range(blk * per, (blk + 1) * per)],
                    axis=0,
                )
                for s in (stepr, stepi)
            ]
        for c in range(n_chip):
            if c:
                c_r, c_i = cmul(c_r, c_i, *spread)
            turned = jnp.concatenate([c_r, -c_i], axis=1).T
            if blk < n_early:
                ct[blk, c] = turned.astype(BF16)
            widen(cs.at[blk], turned, c)
    def across(start):
        for k in range(1, n_chip):
            for h in range(2):
                start(h, 2 * lax.rem(chip + k, n_chip) + h)

    def slot(k, h, b):
        return (k - 1) * (1 + n_early) + (n_early if h else b)

    def share(b):
        lam[b] = l_ref[b, 2:4]
        across(
            lambda h, j: remote(
                ct.at[b, pl.ds(h * half_chips, half_chips)], xct.at[tp * n_early + b], load_sem.at[2], x_sem.at[0],
                {"tp": j},
            ).start()
        )
        across(
            lambda h, j: remote(
                lam.at[b], xlam.at[tp * n_early + b], load_sem.at[3], x_sem.at[1], {"tp": j}
            ).start()
        )

    @pl.when(sp > 0)
    def _():
        share(0)
        for b in range(1, n_early):
            pl.when(core == 0)(functools.partial(share, b))

    lower = (
        lax.broadcasted_iota(jnp.int32, (span, span), 0)
        >= lax.broadcasted_iota(jnp.int32, (span, span), 1)
    ).astype(BF16)

    def landed(ref, sem):
        remote(ref, ref, load_sem.at[0], sem, {"tp": partner}).wait_recv()

    def gone(ref, sem):
        remote(ref, ref, sem, a_recv.at[0], {"tp": partner}).wait_send()

    def source(c, blk):
        return jnp.concatenate([urecv[2 * c + s, blk].astype(F32) for s in range(2)], axis=0)

    def drive(c, blk):
        cut = slice(blk * lanes, (blk + 1) * lanes)
        d = jnp.dot(source(c, blk).astype(BF16), bs[blk], preferred_element_type=F32)
        wr, wi = cmul(d[:, :lanes], d[:, lanes:], t1r[:, cut], t1i[:, cut])
        wbuf[blk][c, :, :lanes] = wr.astype(BF16)
        wbuf[blk][c, :, lanes:] = wi.astype(BF16)
        wsum[blk][c, 0:1, :] = jnp.sum(wr, axis=0, keepdims=True)
        wsum[blk][c, 1:2, :] = jnp.sum(wi, axis=0, keepdims=True)

    def seeds(blk):
        turn = l_ref[blk, 4:5], l_ref[blk, 5:6]
        held = [None]
        for c in range(n_chip):
            r, i = wsum[blk][c, 0:1], wsum[blk][c, 1:2]
            if c:
                r, i = r + held[c][0], i + held[c][1]
            held.append(cmul(r, i, *turn) if c < n_chip - 1 else cmul(r, i, l_ref[blk, 6:7], l_ref[blk, 7:8]))
        return held

    def end_copy(j, blk):
        return remote(e_send.at[blk], e_all.at[blk, sp], e_ssem.at[0], e_rsem.at[blk], {"sp": j})

    def scan(blk):
        cut = slice(blk * lanes, (blk + 1) * lanes)
        held = seeds(blk)
        for c in range(n_chip):
            s = jnp.dot(lower, wbuf[blk][c], preferred_element_type=F32)
            sr, si = s[:, :lanes], s[:, lanes:]
            if c:
                sr, si = sr + held[c][0], si + held[c][1]
            xr, xi = cmul(sr, si, t2r[:, cut], t2i[:, cut])
            at = slice(c * span, (c + 1) * span)
            xbuf[blk][at, :lanes] = xr.astype(BF16)
            xbuf[blk][at, lanes:] = xi.astype(BF16)

    def readout(blk):
        ch = slice(blk * LANES, (blk + 1) * LANES)
        y = jnp.dot(xbuf[blk][...], cs[blk, :, :LANES], preferred_element_type=F32)
        for c in range(n_chip):
            at = slice(c * span, (c + 1) * span)
            ylocal[blk][at] = y[at] + skip[:, ch] * source(c, blk)

    landed(urecv.at[partner], a_recv.at[0])
    for blk in range(n_blk):
        drive(chip, blk)

    def send_ends(blks, first, last):
        def go(j, c):
            for blk in blks:
                end_copy(j, blk).start()
            return c

        lax.fori_loop(first, last, go, 0)

    def finish(blk, y):
        for c in range(n_chip):
            at = slice(c * span, (c + 1) * span)
            v = ylocal[blk][at]
            if y is not None:
                v = v + y[:, c * LANES : (c + 1) * LANES]
            top, to = half_of(c)
            zst[top, blk, to] = jax.nn.gelu(v).astype(BF16)
        if y is None:
            for h, b in [(0, blk)] + [(1, b) for b in (blk - 1, blk) if 0 <= b and (b < blk or blk == n_blk - 1)]:
                cross(b, zst.at[:, b], (h,))
        elif blk >= n_early:
            cross(blk, zst.at[:, blk])
        elif blk:
            pl.when(core == 1)(lambda: cross(blk, zst.at[:, blk]))
        remote(
            zst.at[1 - core, blk], zbuf.at[tp, blk], load_sem.at[1], z_recv.at[0], {"tp": partner}
        ).start()

    def half_of(c):
        top = c * span // half_rows
        return top, slice(c * span - top * half_rows, (c + 1) * span - top * half_rows)

    def ahead(b):
        for c in range(n_chip):
            top, to = half_of(c)
            yst[b, top, to] = ylocal[b][c * span : (c + 1) * span].astype(BF16)
        cross(b, yst.at[b])

    def cross(blk, src, heads=(core, 1 - core)):
        for k in range(1, n_chip):
            for h in heads:
                remote(
                    src.at[h], zbuf.at[tp, blk], load_sem.at[1], z_recv.at[1 + (k - 1) * n_blk + blk],
                    {"tp": 2 * lax.rem(chip + k, n_chip) + h},
                ).start()

    def reach(i, old, new):
        count = new - old if pair == 1 else jnp.where(sp_b == 0, new - old, (new - old) // pair)
        pl.when(count > 0)(lambda: pl.semaphore_wait(met.at[i], count))

    def take(blk):
        for k in range(1, n_chip):
            c = lax.rem(chip + k, n_chip)
            landed(urecv.at[pl.ds(2 * c, 2), blk], a_recv.at[1 + (k - 1) * n_blk + blk])
        for k in range(1, n_chip):
            drive(lax.rem(chip + k, n_chip), blk)

    close = jnp.minimum(sp + 1 + half, n_sp)

    def give(blk):
        er, ei = seeds(blk)[n_chip]
        e_send[blk] = jnp.concatenate([er, ei], axis=0).astype(BF16)

    def post(blk):
        if blk == 0:
            reach(0, sp + 1, close)
            send_ends([0], sp + 1, close)
            return
        if blk == 1:
            reach(1, close, n_sp)
        send_ends([blk], sp + 1, close)
        send_ends(range(2) if blk == 1 else [blk], close, n_sp)

    @pl.when(sp == 0)
    def _():
        for blk in range(n_blk):
            take(blk)
            give(blk)
            if blk != 1:
                post(blk)
            else:
                send_ends([1], sp + 1, close)
            scan(blk)
            readout(blk)
            finish(blk, None)
            if blk == 1:
                reach(1, close, n_sp)
                send_ends(range(2), close, n_sp)

    @pl.when(sp > 0)
    def _():
        for blk in range(n_blk + 2):
            def region(soon, blk=blk):
                if blk < n_blk:
                    take(blk)
                if soon:
                    give(blk)
                    post(blk)
                if 1 <= blk <= n_blk:
                    scan(blk - 1)
                if 2 <= blk:
                    readout(blk - 2)
                if blk < n_blk and not soon:
                    give(blk)
                    post(blk)

            if blk == n_blk - 1:
                pl.when(core == 0)(functools.partial(region, True))
                pl.when(core == 1)(functools.partial(region, False))
            else:
                region(False)
            if blk - 2 == 0:
                ahead(0)
            elif 0 < blk - 2 < n_early:
                pl.when(core == 0)(functools.partial(ahead, blk - 2))

    def after(blk):
        cut = slice(blk * lanes, (blk + 1) * lanes)
        lr, li = l_ref[blk, 0:1], l_ref[blk, 1:2]

        def join(j, held):
            e = e_all[blk, j].astype(F32)
            hr, hi = cmul(*held, lr, li)
            return hr + e[0:1], hi + e[1:2]

        for s in range(1, n_sp):
            pl.when(sp == s)(functools.partial(landed, e_all.at[blk, pl.ds(0, s)], e_rsem.at[blk]))
        nil = jnp.zeros((1, lanes), F32)
        hr, hi = lax.fori_loop(0, sp, join, (nil, nil))
        hr, hi = cmul(hr, hi, l_ref[blk, 2:3], l_ref[blk, 3:4])

        def tell_begin():
            begin[blk] = jnp.concatenate([hr, hi], axis=0).astype(BF16)
            across(
                lambda h, j: remote(
                    begin.at[blk], xbegin.at[tp * n_early + blk], load_sem.at[4], x_sem.at[2 + blk], {"tp": j}
                ).start()
            )

        if blk == 0:
            tell_begin()
        elif blk < n_early:
            pl.when(core == 0)(tell_begin)
        xr, xi = cmul(hr, hi, t2r[:, cut], t2i[:, cut])
        x = jnp.concatenate([xr.astype(BF16), xi.astype(BF16)], axis=1)
        finish(blk, jnp.dot(x, cs[blk], preferred_element_type=F32))


    @pl.when(sp > 0)
    def _():
        for blk in range(n_blk):
            after(blk)

    @pl.when(sp > 0)
    def _():
        for ref, sem in ((xct, 0), (xlam, 1)):
            landed(ref.at[pl.ds(0, (n_chip - 1) * (1 + n_early))], x_sem.at[sem])
        for k in range(1, n_chip):
            for h in range(2):
                j = 2 * lax.rem(chip + n_chip - k, n_chip) + h
                for b in range(1 if h else n_early):
                    for c in range(half_chips):
                        widen(xcs.at[slot(k, h, b)], xct[j * n_early + b, c].astype(F32), c)

    def correct(k, c2, b):
        heads = range(1 if b else 2)
        if k == 1:
            landed(xbegin.at[pl.ds(0, (n_chip - 1) * len(heads))], x_sem.at[2 + b])
        fixed = []
        for h in heads:
            j = (c2 + h) * n_early + b
            first = xbegin[j].astype(F32)
            lr, li, pr, pi = (
                jnp.broadcast_to(part[i : i + 1], (8, lanes)) for part in (xlam[j], first) for i in range(2)
            )
            row = lax.broadcasted_iota(jnp.int32, (8, lanes), 0)
            for bit in range(3):
                on = lax.rem(row // (1 << bit), 2) == 1
                ar, ai = cmul(pr, pi, lr, li)
                pr, pi = jnp.where(on, ar, pr), jnp.where(on, ai, pi)
                lr, li = cmul(lr, li, lr, li)
            pieces = [(pr, pi)]
            while len(pieces) < span // 8:
                pieces += [cmul(*p, lr, li) for p in pieces[: span // 8 - len(pieces)]]
                lr, li = cmul(lr, li, lr, li)
            x = jnp.concatenate(
                [jnp.concatenate([p[i] for p in pieces], axis=0).astype(BF16) for i in range(2)], axis=1
            )
            fixed.append(jnp.dot(x, xcs[slot(k, h, b)], preferred_element_type=F32))
        held = [zbuf[c2 + h, b].astype(F32) for h in heads]
        for h in heads:
            y = jnp.concatenate([fixed[h][:, c * LANES : (c + 1) * LANES] for c in range(half_chips)], axis=0)
            held[h] = jax.nn.gelu(held[h] + y).astype(BF16)
        for h in heads:
            zbuf[c2 + h, b] = held[h]

    loaded(5)

    def project(ref, i, j, blks):
        at = pl.ds(pl.multiple_of(j * width + blks[0] * LANES, LANES), LANES * len(blks))
        z = jnp.concatenate([ref[i, blk] for blk in blks], axis=1)
        return z, at

    def products(*parts):
        z = jnp.concatenate([p[0] for p in parts], axis=1)
        return [
            [
                jnp.dot(
                    z, jnp.concatenate([w[q, i, p[1], :] for p in parts], axis=0), preferred_element_type=F32
                )
                for i in range(2)
            ]
            for q in range(2)
        ]

    def add(new):
        for q in range(2):
            for i in range(2):
                acc[q, i] += new[q][i]

    landed(w.at[1 - core], w_sem.at[1])
    every = range(n_blk)
    new = products(project(zst, core, tp, every))
    for q in range(2):
        for i in range(2):
            acc[q, i] = new[q][i]
    landed(zbuf.at[partner], z_recv.at[0])
    add(products(project(zbuf, partner, partner, every)))
    for blk in range(n_blk):
        for k in range(1, n_chip):
            c2 = 2 * lax.rem(chip + n_chip - k, n_chip)
            landed(zbuf.at[pl.ds(c2, 2), blk], z_recv.at[1 + (k - 1) * n_blk + blk])
            if blk < n_early:
                pl.when(sp > 0)(functools.partial(correct, k, c2, blk))
            new = products(*(project(zbuf, c2 + h, c2 + h, [blk]) for h in range(2)))
            if blk < n_blk - 1 or k < n_chip - 1:
                add(new)
    part = None
    for q in range(2):
        v, g = (acc[q, i] + new[q][i] for i in range(2))
        gated = v * (0.5 + 0.5 * jnp.tanh(0.5 * g))
        both[q] = gated
        square = gated * gated
        for blk in range(n_blk):
            piece = square[:, blk * LANES : (blk + 1) * LANES]
            part = piece if part is None else part + piece
    remote(both.at[1 - core], swapped, q_sem.at[1], q_sem.at[2], {"tp": partner}).start()
    sums = jnp.sum(part, axis=1, keepdims=True)
    lane = lax.broadcasted_iota(jnp.int32, (8, LANES), 1)
    total = jnp.zeros((8, LANES), F32)
    for k in range(half_rows // 8):
        total = jnp.where(lane == k, sums[8 * k : 8 * k + 8], total)
    sq_all[tp] = total
    for k in range(1, n_tp):
        j = lax.rem(tp + n_tp - k, n_tp)
        remote(sq_all.at[tp], sq_all.at[tp], load_sem.at[5], q_sem.at[0], {"tp": j}).start()
    gone(nsend.at[pl.ds(0, n_tp - 1)], load_sem.at[0])
    gone(zbuf.at[pl.ds(0, n_tp - 1)], load_sem.at[1])
    gone(w.at[core], w_sem.at[0])

    @pl.when(sp > 0)
    def _():
        for h in range(2):

            @pl.when(core == h)
            def _(count=(n_tp - 2) * (1 if h else n_early)):
                for ref, sem in ((xct, 2), (xlam, 3), (xbegin, 4)):
                    gone(ref.at[pl.ds(0, count)], load_sem.at[sem])

    for s in range(n_sp - 1):
        pl.when(sp == s)(functools.partial(gone, e_all.at[:, pl.ds(0, n_sp - 1 - s)], e_ssem.at[0]))
    both[core] = both[core] * nout[...]
    landed(swapped, q_sem.at[2])
    swapped[...] = swapped[...] * nout[...]
    landed(sq_all.at[pl.ds(0, n_tp - 1)], q_sem.at[0])
    for h in (core, 1 - core):
        total = sq_all[h]
        for c in range(1, n_chip):
            total = total + sq_all[2 * c + h]
        scale = lax.rsqrt(total / d_model + NORM_EPS)
        column = jnp.concatenate([scale[:, i : i + 1] for i in range(half_rows // 8)], axis=0)
        gated = both[core] if h is core else swapped[...]
        at = pl.ds(pl.multiple_of(h * half_rows, half_rows), half_rows)
        out[at, :] = (gated * column).astype(BF16)

    gone(sq_all.at[pl.ds(0, n_tp - 1)], load_sem.at[5])
    gone(swapped, q_sem.at[1])


def solution(mesh):
    n_sp, n_tp = mesh.shape["sp"], mesh.shape["tp"]

    def on_device(
        tokens, norm_in, decay_log, phase, b_real, b_imag, c_real, c_imag, skip_gain, w_value, w_gate, norm_out
    ):
        mine, d_model = tokens.shape
        rows = mine * n_tp
        groups, state, group = b_real.shape
        width = groups * group
        n_blk = width // LANES
        lanes = LANES // group * state
        entries = groups * state
        n_chip = n_tp // 2
        n_early = min(2, n_blk)
        span = 2 * mine
        vmem = pl.BlockSpec(memory_space=pltpu.VMEM)
        hbm = pl.BlockSpec(memory_space=pl.ANY)
        dma = pltpu.SemaphoreType.DMA
        return pl.pallas_call(
            functools.partial(layer, n_sp, n_tp, state, group),
            out_shape=pltpu.VMEM((rows, width), BF16),
            in_specs=[hbm] * 12,
            out_specs=vmem,
            scratch_shapes=[
                pltpu.VMEM((n_tp, n_blk, mine, LANES), BF16),
                pltpu.VMEM((n_tp, n_blk, mine, LANES), BF16),
                pltpu.VMEM((8, entries), F32),
                pltpu.VMEM((8, entries), F32),
                pltpu.VMEM((span, entries), F32),
                pltpu.VMEM((span, entries), F32),
                pltpu.VMEM((span, entries), F32),
                pltpu.VMEM((span, entries), F32),
                pltpu.VMEM((n_blk, LANES, 2 * lanes), BF16),
                pltpu.VMEM((n_blk, 2 * lanes, n_chip * LANES), BF16),
                [pltpu.VMEM((n_chip, span, 2 * lanes), BF16)] * n_blk,
                [pltpu.VMEM((rows, 2 * lanes), BF16)] * n_blk,
                [pltpu.VMEM((n_chip, 2, lanes), F32)] * n_blk,
                [pltpu.VMEM((rows, LANES), F32)] * n_blk,
                pltpu.VMEM((n_blk, 2, lanes), BF16),
                pltpu.VMEM((n_blk, n_sp, 2, lanes), BF16),
                pltpu.VMEM((n_blk, 8, lanes), F32),
                pltpu.VMEM((2, n_blk, rows // 2, LANES), BF16),
                pltpu.VMEM((n_tp, n_blk, rows // 2, LANES), BF16),
                pltpu.VMEM((2, 2) + w_value.shape, BF16),
                pltpu.VMEM((2, 2, rows // 2, width), F32),
                pltpu.VMEM((2, rows // 2, width), F32),
                pltpu.VMEM((rows // 2, width), F32),
                pltpu.VMEM((n_tp, 8, LANES), F32),
                pltpu.VMEM((n_early, n_chip, 2 * state, LANES), BF16),
                pltpu.VMEM((n_tp * n_early, n_chip // 2, 2 * state, LANES), BF16),
                pltpu.VMEM(((n_chip - 1) * (1 + n_early), 2 * lanes, n_chip // 2 * LANES), BF16),
                pltpu.VMEM((n_early, 2, rows // 2, LANES), BF16),
                pltpu.VMEM((n_early, 2, lanes), F32),
                pltpu.VMEM((n_tp * n_early, 2, lanes), F32),
                pltpu.VMEM((n_early, 2, lanes), BF16),
                pltpu.VMEM((n_tp * n_early, 2, lanes), BF16),
                pltpu.VMEM((4, width, state), F32),
                pltpu.VMEM((mine, d_model), BF16),
                pltpu.VMEM((1, d_model), F32),
                pltpu.VMEM((2, groups, state), F32),
                pltpu.VMEM((2, 1, width), F32),
                dma((6,)),
                dma((1 + (n_chip - 1) * n_blk,)),
                dma((1,)),
                dma((n_blk,)),
                dma((1 + (n_chip - 1) * n_blk,)),
                dma((2,)),
                dma((3,)),
                dma((2 + n_early,)),
                pltpu.SemaphoreType.REGULAR((2,)),
            ],
            compiler_params=pltpu.CompilerParams(collective_id=0, has_side_effects=True),
        )(
            tokens,
            norm_in.reshape(1, -1),
            decay_log,
            phase,
            b_real.transpose(0, 2, 1).reshape(width, state),
            b_imag.transpose(0, 2, 1).reshape(width, state),
            c_real.reshape(width, state),
            c_imag.reshape(width, state),
            skip_gain.reshape(1, -1),
            w_value,
            w_gate,
            norm_out.reshape(1, -1),
        )

    placed = (
        P(("sp", "tp"), None),
        P(),
        P("tp", None),
        P("tp", None),
        P("tp", None, None),
        P("tp", None, None),
        P("tp", None, None),
        P("tp", None, None),
        P("tp"),
        P(None, "tp"),
        P(None, "tp"),
        P("tp"),
    )
    return jax.shard_map(
        on_device, mesh=mesh, in_specs=placed, out_specs=P("sp", "tp"), check_vma=False
    )
```

```python
import functools

import jax
import jax.numpy as jnp
from jax import lax
from jax.experimental import pallas as pl
from jax.experimental.pallas import tpu as pltpu
from jax.sharding import PartitionSpec as P

NORM_EPS = 1e-06
LANES = 128
F32 = jnp.float32
BF16 = jnp.bfloat16


def cmul(ar, ai, br, bi):
    return ar * br - ai * bi, ar * bi + ai * br


def cpow(r, i, n):
    outr, outi = None, None
    while n:
        if n % 2:
            outr, outi = (r, i) if outr is None else cmul(outr, outi, r, i)
        n //= 2
        if n:
            r, i = cmul(r, i, r, i)
    return outr, outi


def remote(src, dst, send, recv, target):
    return pltpu.make_async_remote_copy(
        src_ref=src,
        dst_ref=dst,
        send_sem=send,
        recv_sem=recv,
        device_id=target,
        device_id_type=pl.DeviceIdType.MESH,
    )


def layer(
    n_sp, n_tp, state, group,
    tok_h, nin_h, dlog_h, phase_h, bre_h, bim_h, cre_h, cim_h, skip_h, wv_h, wg_h, nout_h,
    out,
    nsend, urecv, rows_a, rows_p, t1r, t1i, t2r, t2i, bs, cs, wbuf, xbuf, wsum, ylocal,
    e_send, e_all, l_ref, zst, zbuf, w, acc, both, swapped, sq_all, ct, xct, xcs, yst, lam, xlam, begin, xbegin,
    bc, tok, nin, ap, sn,
    load_sem, a_recv, e_ssem, e_rsem, z_recv, w_sem, q_sem, x_sem, met,
):
    sp, tp = lax.axis_index("sp"), lax.axis_index("tp")
    mine, d_model = tok.shape
    rows, width = out.shape
    half_rows = rows // 2
    n_blk = width // LANES
    per = LANES // group
    lanes = per * state
    core = lax.rem(tp, 2)
    chip = tp // 2
    partner = tp + 1 - 2 * core
    n_chip = n_tp // 2
    span = 2 * mine
    pair = 2 if n_sp % 2 == 0 else 1
    sp_b = lax.rem(sp, pair)
    n_early = min(2, n_blk)
    half_chips = n_chip // 2

    parts = [pl.ds(i, 8) for i in range(0, mine, 8)]

    def load(i, *pairs):
        return [pltpu.make_async_copy(src, dst, load_sem.at[i]) for src, dst in pairs]

    loads = [
        load(0, *((tok_h.at[part], tok.at[part]) for part in parts)),
        load(1, (nin_h, nin)),
        load(2, (dlog_h, ap.at[0]), (phase_h, ap.at[1])),
        load(3, *((src, bc.at[i]) for i, src in enumerate((bre_h, bim_h, cre_h, cim_h)))),
        load(4, (skip_h, sn.at[0]), (nout_h, sn.at[1])),
        load(5, (wv_h, w.at[core, 0]), (wg_h, w.at[core, 1])),
    ]

    def start(*which):
        for i in which:
            for copy in loads[i]:
                copy.start()

    def loaded(*which):
        for i in which:
            dst = (tok, nin, ap, bc, sn, w.at[core])[i]
            pltpu.make_async_copy(dst, dst, load_sem.at[i]).wait()

    start(0, 1, 2)

    barrier = pltpu.get_barrier_semaphore()

    def tell(sem, axis):
        def go(j, c):
            pl.semaphore_signal(sem, inc=1, device_id={axis: j}, device_id_type=pl.DeviceIdType.MESH)
            return c

        return go

    def above(go):
        for b in range(pair):
            first = sp // pair + jnp.where(b > sp_b, 0, 1)
            go_b = lambda a, c, b=b: go(a * pair + b, c)
            lax.fori_loop(jnp.where(b >= sp_b, first, n_sp // pair), n_sp // pair, go_b, 0)

    def below(go):
        for b in range(pair):
            last = sp // pair + jnp.where(b < sp_b, 1, 0)
            lax.fori_loop(0, jnp.where(b <= sp_b, last, 0), lambda a, c, b=b: go(a * pair + b, c), 0)

    last = sp == n_sp - 1
    lax.fori_loop(jnp.where(last, tp + 1, 0), jnp.where(last, tp + 1, tp), tell(barrier, "tp"), 0)
    lax.fori_loop(tp + 1, n_tp, tell(barrier, "tp"), 0)
    above(tell(barrier, "sp"))
    start(3, 4)
    known = (sp // pair + 1) * (sp_b + 1) - 1 + jnp.where(last, tp, n_tp - 1)
    half = (n_sp // 2 + pair - 1) // pair * pair

    def enter():
        pl.when(known > 0)(lambda: pl.semaphore_wait(barrier, known))
        below(lambda j, c: tell(met.at[jnp.where(sp - j > half, 1, 0)], "sp")(j, c))
        lax.fori_loop(0, jnp.where(last, tp, 0), tell(met.at[0], "tp"), 0)

    pl.when(last)(enter)
    loaded(0, 1)

    xf = tok[...].astype(F32)
    scale = lax.rsqrt(jnp.sum(xf * xf, axis=1, keepdims=True) / d_model + NORM_EPS)
    normed = (xf * scale * nin[...]).astype(BF16)
    for j in range(n_tp):
        for blk in range(n_blk):
            at = j * width + blk * LANES
            nsend[j, blk] = normed[:, at : at + LANES]

    pl.when(jnp.logical_not(last))(enter)
    pl.when(last & (tp < n_tp - 1))(lambda: pl.semaphore_wait(met.at[0], n_tp - 1 - tp))


    def scatter(j, blk, at):
        remote(nsend.at[j, blk], urecv.at[tp, blk], load_sem.at[0], a_recv.at[at], {"tp": j}).start()

    for blk in range(n_blk):
        for k in range(1, n_chip):
            other = lax.rem(chip + n_chip - k, n_chip)
            for j in (2 * other + core, 2 * other + 1 - core):
                scatter(j, blk, 1 + (k - 1) * n_blk + blk)
        if blk == 0:
            for b in range(n_blk):
                scatter(partner, b, 0)
    start(5)
    for i, src in enumerate((wv_h, wg_h)):
        remote(src, w.at[core, i], w_sem.at[0], w_sem.at[1], {"tp": partner}).start()
    urecv[tp] = nsend[tp]

    loaded(2)
    dlog, phase, skip, nout = ap.at[0], ap.at[1], sn.at[0], sn.at[1]
    bre, bim, cre, cim = (bc.at[i] for i in range(4))
    side = LANES // state
    for i in range(width // group // side):
        cut = slice(i * LANES, (i + 1) * LANES)
        for src, dst in ((dlog, rows_a), (phase, rows_p)):
            row = jnp.concatenate([src[i * side + k : i * side + k + 1, :] for k in range(side)], axis=1)
            dst[:, cut] = jnp.broadcast_to(row, (8, LANES))

    for blk in range(n_blk):
        cut = slice(blk * lanes, (blk + 1) * lanes)
        a, p = rows_a[:, cut], rows_p[:, cut]
        mag, cos, sin = jnp.exp(a), jnp.cos(p), jnp.sin(p)
        lr, li = mag * cos, mag * sin
        inv = jnp.exp(-a)
        nr, ni = inv * cos, -inv * sin
        mod = a * a + p * p
        cr = ((lr - 1.0) * a + li * p) / mod
        ci = (li * a - (lr - 1.0) * p) / mod
        one, zero = jnp.ones_like(a), jnp.zeros_like(a)
        pr, pi, mr, mi = one, zero, cr, ci
        sr, si, qr, qi = lr, li, nr, ni
        row = lax.broadcasted_iota(jnp.int32, a.shape, 0)
        for bit in range(3):
            on = lax.rem(row // (1 << bit), 2) == 1
            ar, ai = cmul(pr, pi, sr, si)
            pr, pi = jnp.where(on, ar, pr), jnp.where(on, ai, pi)
            ar, ai = cmul(mr, mi, qr, qi)
            mr, mi = jnp.where(on, ar, mr), jnp.where(on, ai, mi)
            sr, si = cmul(sr, si, sr, si)
            qr, qi = cmul(qr, qi, qr, qi)
        t2r[0:8, cut], t2i[0:8, cut], t1r[0:8, cut], t1i[0:8, cut] = pr, pi, mr, mi
        done = 8
        while done < span:
            more = min(done, span - done)
            for off in range(0, more, 8):
                src, dst = slice(off, off + 8), slice(done + off, done + off + 8)
                t2r[dst, cut], t2i[dst, cut] = cmul(t2r[src, cut], t2i[src, cut], sr, si)
                t1r[dst, cut], t1i[dst, cut] = cmul(t1r[src, cut], t1i[src, cut], qr, qi)
            sr, si = cmul(sr, si, sr, si)
            qr, qi = cmul(qr, qi, qr, qi)
            done += more
        endr, endi = t2r[span - 1 : span, cut], t2i[span - 1 : span, cut]
        wholer, wholei = cmul(endr, endi, lr[0:1], li[0:1])
        allr, alli = cpow(wholer, wholei, n_chip)
        for k, value in enumerate((allr, alli, lr[0:1], li[0:1], wholer, wholei, endr, endi)):
            l_ref[blk, k : k + 1, :] = value

    loaded(3, 4)
    keep_b = (
        lax.broadcasted_iota(jnp.int32, (LANES, lanes), 0) // group
        == lax.broadcasted_iota(jnp.int32, (LANES, lanes), 1) // state
    )
    of_col = lax.broadcasted_iota(jnp.int32, (state, LANES), 1) // group
    a, p = dlog[...], phase[...]
    mag = jnp.exp(a)
    stepr, stepi = cpow(mag * jnp.cos(p), mag * jnp.sin(p), span)

    def widen(dst, turned, c):
        for part in range(2):
            piece = turned[part * state : (part + 1) * state]
            for g in range(per):
                at = part * lanes + g * state
                dst[at : at + state, c * LANES : (c + 1) * LANES] = jnp.where(of_col == g, piece, 0.0).astype(BF16)

    for blk in range(n_blk):
        ch = slice(blk * LANES, (blk + 1) * LANES)
        for part, in_ref in ((0, bre), (1, bim)):
            b = in_ref[ch, :]
            b = jnp.concatenate([b] * side, axis=1)
            wide = jnp.where(keep_b, jnp.concatenate([b] * (lanes // LANES), axis=1), 0.0)
            bs[blk, :, part * lanes : (part + 1) * lanes] = wide.astype(BF16)
        c_r, c_i = cre[ch, :], cim[ch, :]
        if n_chip > 1:
            spread = [
                jnp.concatenate(
                    [jnp.broadcast_to(s[g : g + 1], (group, state)) for g in range(blk * per, (blk + 1) * per)],
                    axis=0,
                )
                for s in (stepr, stepi)
            ]
        for c in range(n_chip):
            if c:
                c_r, c_i = cmul(c_r, c_i, *spread)
            turned = jnp.concatenate([c_r, -c_i], axis=1).T
            if blk < n_early:
                ct[blk, c] = turned.astype(BF16)
            widen(cs.at[blk], turned, c)
    def across(start):
        for k in range(1, n_chip):
            for h in range(2):
                start(h, 2 * lax.rem(chip + k, n_chip) + h)

    def slot(k, h, b):
        return (k - 1) * (1 + n_early) + (n_early if h else b)

    def share(b):
        lam[b] = l_ref[b, 2:4]
        across(
            lambda h, j: remote(
                ct.at[b, pl.ds(h * half_chips, half_chips)], xct.at[tp * n_early + b], load_sem.at[2], x_sem.at[0],
                {"tp": j},
            ).start()
        )
        across(
            lambda h, j: remote(
                lam.at[b], xlam.at[tp * n_early + b], load_sem.at[3], x_sem.at[1], {"tp": j}
            ).start()
        )

    @pl.when(sp > 0)
    def _():
        share(0)
        for b in range(1, n_early):
            pl.when(core == 0)(functools.partial(share, b))

    lower = (
        lax.broadcasted_iota(jnp.int32, (span, span), 0)
        >= lax.broadcasted_iota(jnp.int32, (span, span), 1)
    ).astype(BF16)

    def landed(ref, sem):
        remote(ref, ref, load_sem.at[0], sem, {"tp": partner}).wait_recv()

    def gone(ref, sem):
        remote(ref, ref, sem, a_recv.at[0], {"tp": partner}).wait_send()

    def source(c, blk):
        return jnp.concatenate([urecv[2 * c + s, blk].astype(F32) for s in range(2)], axis=0)

    def drive(c, blk):
        cut = slice(blk * lanes, (blk + 1) * lanes)
        d = jnp.dot(source(c, blk).astype(BF16), bs[blk], preferred_element_type=F32)
        wr, wi = cmul(d[:, :lanes], d[:, lanes:], t1r[:, cut], t1i[:, cut])
        wbuf[blk][c, :, :lanes] = wr.astype(BF16)
        wbuf[blk][c, :, lanes:] = wi.astype(BF16)
        wsum[blk][c, 0:1, :] = jnp.sum(wr, axis=0, keepdims=True)
        wsum[blk][c, 1:2, :] = jnp.sum(wi, axis=0, keepdims=True)

    def seeds(blk):
        turn = l_ref[blk, 4:5], l_ref[blk, 5:6]
        held = [None]
        for c in range(n_chip):
            r, i = wsum[blk][c, 0:1], wsum[blk][c, 1:2]
            if c:
                r, i = r + held[c][0], i + held[c][1]
            held.append(cmul(r, i, *turn) if c < n_chip - 1 else cmul(r, i, l_ref[blk, 6:7], l_ref[blk, 7:8]))
        return held

    def end_copy(j, blk):
        return remote(e_send.at[blk], e_all.at[blk, sp], e_ssem.at[0], e_rsem.at[blk], {"sp": j})

    def scan(blk):
        cut = slice(blk * lanes, (blk + 1) * lanes)
        held = seeds(blk)
        for c in range(n_chip):
            s = jnp.dot(lower, wbuf[blk][c], preferred_element_type=F32)
            sr, si = s[:, :lanes], s[:, lanes:]
            if c:
                sr, si = sr + held[c][0], si + held[c][1]
            xr, xi = cmul(sr, si, t2r[:, cut], t2i[:, cut])
            at = slice(c * span, (c + 1) * span)
            xbuf[blk][at, :lanes] = xr.astype(BF16)
            xbuf[blk][at, lanes:] = xi.astype(BF16)

    def readout(blk):
        ch = slice(blk * LANES, (blk + 1) * LANES)
        y = jnp.dot(xbuf[blk][...], cs[blk, :, :LANES], preferred_element_type=F32)
        for c in range(n_chip):
            at = slice(c * span, (c + 1) * span)
            ylocal[blk][at] = y[at] + skip[:, ch] * source(c, blk)

    landed(urecv.at[partner], a_recv.at[0])
    for blk in range(n_blk):
        drive(chip, blk)

    def send_ends(blks, first, last):
        def go(j, c):
            for blk in blks:
                end_copy(j, blk).start()
            return c

        lax.fori_loop(first, last, go, 0)

    def finish(blk, y):
        for c in range(n_chip):
            at = slice(c * span, (c + 1) * span)
            v = ylocal[blk][at]
            if y is not None:
                v = v + y[:, c * LANES : (c + 1) * LANES]
            top, to = half_of(c)
            zst[top, blk, to] = jax.nn.gelu(v).astype(BF16)
        if y is None:
            for h, b in [(0, blk)] + [(1, b) for b in (blk - 1, blk) if 0 <= b and (b < blk or blk == n_blk - 1)]:
                cross(b, zst.at[:, b], (h,))
        elif blk >= n_early:
            cross(blk, zst.at[:, blk])
        elif blk:
            pl.when(core == 1)(lambda: cross(blk, zst.at[:, blk]))
        remote(
            zst.at[1 - core, blk], zbuf.at[tp, blk], load_sem.at[1], z_recv.at[0], {"tp": partner}
        ).start()

    def half_of(c):
        top = c * span // half_rows
        return top, slice(c * span - top * half_rows, (c + 1) * span - top * half_rows)

    def ahead(b):
        for c in range(n_chip):
            top, to = half_of(c)
            yst[b, top, to] = ylocal[b][c * span : (c + 1) * span].astype(BF16)
        cross(b, yst.at[b])

    def cross(blk, src, heads=(core, 1 - core)):
        for k in range(1, n_chip):
            for h in heads:
                remote(
                    src.at[h], zbuf.at[tp, blk], load_sem.at[1], z_recv.at[1 + (k - 1) * n_blk + blk],
                    {"tp": 2 * lax.rem(chip + k, n_chip) + h},
                ).start()

    def reach(i, old, new):
        count = new - old if pair == 1 else jnp.where(sp_b == 0, new - old, (new - old) // pair)
        pl.when(count > 0)(lambda: pl.semaphore_wait(met.at[i], count))

    def take(blk):
        for k in range(1, n_chip):
            c = lax.rem(chip + k, n_chip)
            landed(urecv.at[pl.ds(2 * c, 2), blk], a_recv.at[1 + (k - 1) * n_blk + blk])
        for k in range(1, n_chip):
            drive(lax.rem(chip + k, n_chip), blk)

    close = jnp.minimum(sp + 1 + half, n_sp)

    def give(blk):
        er, ei = seeds(blk)[n_chip]
        e_send[blk] = jnp.concatenate([er, ei], axis=0).astype(BF16)

    def post(blk):
        if blk == 0:
            reach(0, sp + 1, close)
            send_ends([0], sp + 1, close)
            return
        if blk == 1:
            reach(1, close, n_sp)
        send_ends([blk], sp + 1, close)
        send_ends(range(2) if blk == 1 else [blk], close, n_sp)

    @pl.when(sp == 0)
    def _():
        for blk in range(n_blk):
            take(blk)
            give(blk)
            if blk != 1:
                post(blk)
            else:
                send_ends([1], sp + 1, close)
            scan(blk)
            readout(blk)
            finish(blk, None)
            if blk == 1:
                reach(1, close, n_sp)
                send_ends(range(2), close, n_sp)

    @pl.when(sp > 0)
    def _():
        for blk in range(n_blk + 2):
            def region(soon, blk=blk):
                if blk < n_blk:
                    take(blk)
                if soon:
                    give(blk)
                    post(blk)
                if 1 <= blk <= n_blk:
                    scan(blk - 1)
                if 2 <= blk:
                    readout(blk - 2)
                if blk < n_blk and not soon:
                    give(blk)
                    post(blk)

            if blk == n_blk - 1:
                pl.when(core == 0)(functools.partial(region, True))
                pl.when(core == 1)(functools.partial(region, False))
            else:
                region(False)
            if blk - 2 == 0:
                ahead(0)
            elif 0 < blk - 2 < n_early:
                pl.when(core == 0)(functools.partial(ahead, blk - 2))

    def after(blk):
        cut = slice(blk * lanes, (blk + 1) * lanes)
        lr, li = l_ref[blk, 0:1], l_ref[blk, 1:2]

        def join(j, held):
            e = e_all[blk, j].astype(F32)
            hr, hi = cmul(*held, lr, li)
            return hr + e[0:1], hi + e[1:2]

        for s in range(1, n_sp):
            pl.when(sp == s)(functools.partial(landed, e_all.at[blk, pl.ds(0, s)], e_rsem.at[blk]))
        nil = jnp.zeros((1, lanes), F32)
        hr, hi = lax.fori_loop(0, sp, join, (nil, nil))
        hr, hi = cmul(hr, hi, l_ref[blk, 2:3], l_ref[blk, 3:4])

        def tell_begin():
            begin[blk] = jnp.concatenate([hr, hi], axis=0).astype(BF16)
            across(
                lambda h, j: remote(
                    begin.at[blk], xbegin.at[tp * n_early + blk], load_sem.at[4], x_sem.at[2 + blk], {"tp": j}
                ).start()
            )

        if blk == 0:
            tell_begin()
        elif blk < n_early:
            pl.when(core == 0)(tell_begin)
        xr, xi = cmul(hr, hi, t2r[:, cut], t2i[:, cut])
        x = jnp.concatenate([xr.astype(BF16), xi.astype(BF16)], axis=1)
        finish(blk, jnp.dot(x, cs[blk], preferred_element_type=F32))


    @pl.when(sp > 0)
    def _():
        for blk in range(n_blk):
            after(blk)

    @pl.when(sp > 0)
    def _():
        for ref, sem in ((xct, 0), (xlam, 1)):
            landed(ref.at[pl.ds(0, (n_chip - 1) * (1 + n_early))], x_sem.at[sem])
        for k in range(1, n_chip):
            for h in range(2):
                j = 2 * lax.rem(chip + n_chip - k, n_chip) + h
                for b in range(1 if h else n_early):
                    for c in range(half_chips):
                        widen(xcs.at[slot(k, h, b)], xct[j * n_early + b, c].astype(F32), c)

    def correct(k, c2, b):
        heads = range(1 if b else 2)
        if k == 1:
            landed(xbegin.at[pl.ds(0, (n_chip - 1) * len(heads))], x_sem.at[2 + b])
        fixed = []
        for h in heads:
            j = (c2 + h) * n_early + b
            first = xbegin[j].astype(F32)
            lr, li, pr, pi = (
                jnp.broadcast_to(part[i : i + 1], (8, lanes)) for part in (xlam[j], first) for i in range(2)
            )
            row = lax.broadcasted_iota(jnp.int32, (8, lanes), 0)
            for bit in range(3):
                on = lax.rem(row // (1 << bit), 2) == 1
                ar, ai = cmul(pr, pi, lr, li)
                pr, pi = jnp.where(on, ar, pr), jnp.where(on, ai, pi)
                lr, li = cmul(lr, li, lr, li)
            pieces = [(pr, pi)]
            while len(pieces) < span // 8:
                pieces += [cmul(*p, lr, li) for p in pieces[: span // 8 - len(pieces)]]
                lr, li = cmul(lr, li, lr, li)
            x = jnp.concatenate(
                [jnp.concatenate([p[i] for p in pieces], axis=0).astype(BF16) for i in range(2)], axis=1
            )
            fixed.append(jnp.dot(x, xcs[slot(k, h, b)], preferred_element_type=F32))
        held = [zbuf[c2 + h, b].astype(F32) for h in heads]
        for h in heads:
            y = jnp.concatenate([fixed[h][:, c * LANES : (c + 1) * LANES] for c in range(half_chips)], axis=0)
            held[h] = jax.nn.gelu(held[h] + y).astype(BF16)
        for h in heads:
            zbuf[c2 + h, b] = held[h]

    loaded(5)

    def project(ref, i, j, blks):
        at = pl.ds(pl.multiple_of(j * width + blks[0] * LANES, LANES), LANES * len(blks))
        z = jnp.concatenate([ref[i, blk] for blk in blks], axis=1)
        return z, at

    def products(*parts):
        z = jnp.concatenate([p[0] for p in parts], axis=1)
        return [
            [
                jnp.dot(
                    z, jnp.concatenate([w[q, i, p[1], :] for p in parts], axis=0), preferred_element_type=F32
                )
                for i in range(2)
            ]
            for q in range(2)
        ]

    def add(new):
        for q in range(2):
            for i in range(2):
                acc[q, i] += new[q][i]

    landed(w.at[1 - core], w_sem.at[1])
    every = range(n_blk)
    new = products(project(zst, core, tp, every))
    for q in range(2):
        for i in range(2):
            acc[q, i] = new[q][i]
    landed(zbuf.at[partner], z_recv.at[0])
    add(products(project(zbuf, partner, partner, every)))
    for blk in range(n_blk):
        for k in range(1, n_chip):
            c2 = 2 * lax.rem(chip + n_chip - k, n_chip)
            landed(zbuf.at[pl.ds(c2, 2), blk], z_recv.at[1 + (k - 1) * n_blk + blk])
            if blk < n_early:
                pl.when(sp > 0)(functools.partial(correct, k, c2, blk))
            new = products(*(project(zbuf, c2 + h, c2 + h, [blk]) for h in range(2)))
            if blk < n_blk - 1 or k < n_chip - 1:
                add(new)
    part = None
    for q in range(2):
        v, g = (acc[q, i] + new[q][i] for i in range(2))
        gated = v * (0.5 + 0.5 * jnp.tanh(0.5 * g))
        both[q] = gated
        square = gated * gated
        for blk in range(n_blk):
            piece = square[:, blk * LANES : (blk + 1) * LANES]
            part = piece if part is None else part + piece
    remote(both.at[1 - core], swapped, q_sem.at[1], q_sem.at[2], {"tp": partner}).start()
    sums = jnp.sum(part, axis=1, keepdims=True)
    lane = lax.broadcasted_iota(jnp.int32, (8, LANES), 1)
    total = jnp.zeros((8, LANES), F32)
    for k in range(half_rows // 8):
        total = jnp.where(lane == k, sums[8 * k : 8 * k + 8], total)
    sq_all[tp] = total
    for k in range(1, n_tp):
        j = lax.rem(tp + n_tp - k, n_tp)
        remote(sq_all.at[tp], sq_all.at[tp], load_sem.at[5], q_sem.at[0], {"tp": j}).start()
    gone(nsend.at[pl.ds(0, n_tp - 1)], load_sem.at[0])
    gone(zbuf.at[pl.ds(0, n_tp - 1)], load_sem.at[1])
    gone(w.at[core], w_sem.at[0])

    @pl.when(sp > 0)
    def _():
        for h in range(2):

            @pl.when(core == h)
            def _(count=(n_tp - 2) * (1 if h else n_early)):
                for ref, sem in ((xct, 2), (xlam, 3), (xbegin, 4)):
                    gone(ref.at[pl.ds(0, count)], load_sem.at[sem])

    for s in range(n_sp - 1):
        pl.when(sp == s)(functools.partial(gone, e_all.at[:, pl.ds(0, n_sp - 1 - s)], e_ssem.at[0]))
    both[core] = both[core] * nout[...]
    landed(swapped, q_sem.at[2])
    swapped[...] = swapped[...] * nout[...]
    landed(sq_all.at[pl.ds(0, n_tp - 1)], q_sem.at[0])
    for h in (core, 1 - core):
        total = sq_all[h]
        for c in range(1, n_chip):
            total = total + sq_all[2 * c + h]
        scale = lax.rsqrt(total / d_model + NORM_EPS)
        column = jnp.concatenate([scale[:, i : i + 1] for i in range(half_rows // 8)], axis=0)
        gated = both[core] if h is core else swapped[...]
        at = pl.ds(pl.multiple_of(h * half_rows, half_rows), half_rows)
        out[at, :] = (gated * column).astype(BF16)

    gone(sq_all.at[pl.ds(0, n_tp - 1)], load_sem.at[5])
    gone(swapped, q_sem.at[1])


def solution(mesh):
    n_sp, n_tp = mesh.shape["sp"], mesh.shape["tp"]

    def on_device(
        tokens, norm_in, decay_log, phase, b_real, b_imag, c_real, c_imag, skip_gain, w_value, w_gate, norm_out
    ):
        mine, d_model = tokens.shape
        rows = mine * n_tp
        groups, state, group = b_real.shape
        width = groups * group
        n_blk = width // LANES
        lanes = LANES // group * state
        entries = groups * state
        n_chip = n_tp // 2
        n_early = min(2, n_blk)
        span = 2 * mine
        vmem = pl.BlockSpec(memory_space=pltpu.VMEM)
        hbm = pl.BlockSpec(memory_space=pl.ANY)
        dma = pltpu.SemaphoreType.DMA
        return pl.pallas_call(
            functools.partial(layer, n_sp, n_tp, state, group),
            out_shape=pltpu.VMEM((rows, width), BF16),
            in_specs=[hbm] * 12,
            out_specs=vmem,
            scratch_shapes=[
                pltpu.VMEM((n_tp, n_blk, mine, LANES), BF16),
                pltpu.VMEM((n_tp, n_blk, mine, LANES), BF16),
                pltpu.VMEM((8, entries), F32),
                pltpu.VMEM((8, entries), F32),
                pltpu.VMEM((span, entries), F32),
                pltpu.VMEM((span, entries), F32),
                pltpu.VMEM((span, entries), F32),
                pltpu.VMEM((span, entries), F32),
                pltpu.VMEM((n_blk, LANES, 2 * lanes), BF16),
                pltpu.VMEM((n_blk, 2 * lanes, n_chip * LANES), BF16),
                [pltpu.VMEM((n_chip, span, 2 * lanes), BF16)] * n_blk,
                [pltpu.VMEM((rows, 2 * lanes), BF16)] * n_blk,
                [pltpu.VMEM((n_chip, 2, lanes), F32)] * n_blk,
                [pltpu.VMEM((rows, LANES), F32)] * n_blk,
                pltpu.VMEM((n_blk, 2, lanes), BF16),
                pltpu.VMEM((n_blk, n_sp, 2, lanes), BF16),
                pltpu.VMEM((n_blk, 8, lanes), F32),
                pltpu.VMEM((2, n_blk, rows // 2, LANES), BF16),
                pltpu.VMEM((n_tp, n_blk, rows // 2, LANES), BF16),
                pltpu.VMEM((2, 2) + w_value.shape, BF16),
                pltpu.VMEM((2, 2, rows // 2, width), F32),
                pltpu.VMEM((2, rows // 2, width), F32),
                pltpu.VMEM((rows // 2, width), F32),
                pltpu.VMEM((n_tp, 8, LANES), F32),
                pltpu.VMEM((n_early, n_chip, 2 * state, LANES), BF16),
                pltpu.VMEM((n_tp * n_early, n_chip // 2, 2 * state, LANES), BF16),
                pltpu.VMEM(((n_chip - 1) * (1 + n_early), 2 * lanes, n_chip // 2 * LANES), BF16),
                pltpu.VMEM((n_early, 2, rows // 2, LANES), BF16),
                pltpu.VMEM((n_early, 2, lanes), F32),
                pltpu.VMEM((n_tp * n_early, 2, lanes), F32),
                pltpu.VMEM((n_early, 2, lanes), BF16),
                pltpu.VMEM((n_tp * n_early, 2, lanes), BF16),
                pltpu.VMEM((4, width, state), F32),
                pltpu.VMEM((mine, d_model), BF16),
                pltpu.VMEM((1, d_model), F32),
                pltpu.VMEM((2, groups, state), F32),
                pltpu.VMEM((2, 1, width), F32),
                dma((6,)),
                dma((1 + (n_chip - 1) * n_blk,)),
                dma((1,)),
                dma((n_blk,)),
                dma((1 + (n_chip - 1) * n_blk,)),
                dma((2,)),
                dma((3,)),
                dma((2 + n_early,)),
                pltpu.SemaphoreType.REGULAR((2,)),
            ],
            compiler_params=pltpu.CompilerParams(collective_id=0, has_side_effects=True),
        )(
            tokens,
            norm_in.reshape(1, -1),
            decay_log,
            phase,
            b_real.transpose(0, 2, 1).reshape(width, state),
            b_imag.transpose(0, 2, 1).reshape(width, state),
            c_real.reshape(width, state),
            c_imag.reshape(width, state),
            skip_gain.reshape(1, -1),
            w_value,
            w_gate,
            norm_out.reshape(1, -1),
        )

    placed = (
        P(("sp", "tp"), None),
        P(),
        P("tp", None),
        P("tp", None),
        P("tp", None, None),
        P("tp", None, None),
        P("tp", None, None),
        P("tp", None, None),
        P("tp"),
        P(None, "tp"),
        P(None, "tp"),
        P("tp"),
    )
    return jax.shard_map(
        on_device, mesh=mesh, in_specs=placed, out_specs=P("sp", "tp"), check_vma=False
    )
```
